32 devices in a mesh: sp: 4 (over y, x), tp: 8 (over z, core).
Axes of the slice: x: 2, y: 2, z: 4, core: 2. Of those that a mesh axis runs over, the one named last changes fastest.
Arguments:
- tokens: bfloat16 [1536, 2048], P('sp', 'tp'), may hold values from -110 to 110
- documents: int32 [1536], P('sp'), may hold values from 0 to 1, never falling along the last dimension, each value on 1 to 1152 neighbouring positions
- pre_gain: float32 [3, 2048], replicated, may hold values from 0.1 to 1.9
- query_weight: bfloat16 [3, 2048, 2048], P(None, 'tp'), may hold values from -0.125 to 0.125
- key_weight: bfloat16 [3, 2048, 2048], P(None, 'tp'), may hold values from -0.125 to 0.125
- value_weight: bfloat16 [3, 2048, 2048], P(None, 'tp'), may hold values from -0.125 to 0.125
- gate_weight: bfloat16 [3, 2048, 2048], P(None, 'tp'), may hold values from -0.125 to 0.125
- out_weight: bfloat16 [3, 2048, 2048], P(None, 'tp'), may hold values from -0.70710678 to 0.70710678
- position_bias: float32 [3, 32, 257], P(None, 'tp'), may hold values from -4 to 302
- post_gain: float32 [3, 2048], replicated, may hold values from 0.1 to 1.9
Outputs:
- updated: bfloat16 [1536, 2048], P('sp', 'tp')
The draws below stay inside these ranges and needn't reach their ends.
Inputs may be any that keep to these rules, and one draw needn't show every extreme that they name: `documents`: document numbers never fall, every number from 0 to 1 is used, each document holds at most 1152 positions.
All inputs are finite; a program needn't handle non-finite values.
Results may differ from the reference program's by a relative error of at most 0.015.
Values may be sent and summed in bfloat16 or wider, within the bound.
No kernel may reach another device: no remote copies, remote signals or barrier semaphores. Data moves between devices by JAX's collectives and lax.ppermute only.
A program may use at most 64 MiB of HBM per device.

```python
import math
import jax
import jax.numpy as jnp
import numpy as np
from jax import lax

D = 2048
HEADS = 32
HD = 64
BLOCK = 64
PAST_BLOCKS = 4
LAYERS = 3
TOKENS = 1536
PAST = 256
CLIP = 128
DOCS = 2
MOST_DOC = 1152


def column_scale(key, shape):
    ramp = math.log(4.0) * jnp.arange(D, dtype=jnp.float32) / D
    return jnp.exp(ramp + jax.random.uniform(key, shape, jnp.float32, math.log(0.6), math.log(1.6)))


def draw_tokens(key, part):
    key_list = jax.random.split(key, 3)
    row_scale = jnp.exp(jax.random.uniform(key_list[0], (TOKENS, 1), jnp.float32, math.log(0.3), math.log(3.0)))
    col_scale = column_scale(key_list[1], (1, D))
    base_draw = jax.random.truncated_normal(key_list[2], -5.0, 5.0, (TOKENS, D), jnp.float32)
    return (base_draw * row_scale * col_scale).astype(jnp.bfloat16)


def draw_out_weight(key, part):
    key_list = jax.random.split(key, 2)
    ramp = math.log(4.0) * jnp.arange(D, dtype=jnp.float32)[None, :, None] / D
    row_scale = jnp.exp(ramp + jax.random.uniform(key_list[0], (LAYERS, D, 1), jnp.float32, math.log(0.6), math.log(1.6)))
    base_draw = jax.random.truncated_normal(key_list[1], -5.0, 5.0, (LAYERS, D, D), jnp.float32)
    return (base_draw * D ** (-0.5) * row_scale).astype(jnp.bfloat16)


def draw_position_bias(key, part):
    key_list = jax.random.split(key, 1)
    shape = (LAYERS, HEADS, 2 * CLIP + 1)
    base_draw = jax.random.truncated_normal(key_list[0], -4.0, 4.0, shape, jnp.float32)
    return base_draw


def shard_levels(own_key, shape, pieces, smallest, largest):
    factor_of = 1.0
    for axis_at, parts in pieces:
        heights = jax.random.uniform(jax.random.fold_in(jax.random.fold_in(own_key, 6), axis_at), (parts,), jnp.float32, smallest / len(pieces), largest / len(pieces))
        factor_of = factor_of * jnp.repeat(jnp.exp(heights), shape[axis_at] // parts).reshape((-1,) + (1,) * (len(shape) - 1 - axis_at))
    return factor_of


def profile(count, total, bound, skew):
    loads = [(1 << 20) // math.isqrt(rank ** skew) + 1 for rank in range(2, count + 1)]
    rest, holding = total - bound - (count - 1), [1] * (count - 1)
    while rest > 0:
        candidates = [i for i in range(count - 1) if holding[i] < bound]
        pool, budget = sum([loads[i] for i in candidates]), rest
        for i in candidates:
            addition = min(bound - holding[i], max(1, budget * loads[i] // pool), rest)
            holding[i] = holding[i] + addition
            rest = rest - addition
    return np.array([bound] + holding)


def uneven_parts(stream_key, amount, total, bound, slope):
    if amount == 2:
        one = jax.random.randint(stream_key, (), max(1, total - bound), min(bound, total - 1) + 1)
        return jnp.stack([one, total - one])
    lengths = jnp.asarray(profile(amount, total, bound, slope), jnp.int32)
    twos = (amount - 1) // 2
    donor, sink = lengths[1:1 + 2 * twos:2], lengths[2:2 + 2 * twos:2]
    slack = jnp.minimum(donor - 1, bound - sink)
    passed = jax.random.randint(jax.random.fold_in(stream_key, 1), (twos,), 0, 1 << 20) % (slack + 1)
    lengths = lengths.at[1:1 + 2 * twos:2].set(donor - passed).at[2:2 + 2 * twos:2].set(sink + passed)
    return lengths[jax.random.permutation(jax.random.fold_in(stream_key, 2), amount)]


def noise(rng, extent, width, bound, shards=(), kind=jnp.bfloat16):
    result = width * jax.random.normal(rng, extent, jnp.float32)
    if shards:
        result = result * shard_levels(rng, extent, shards, -0.22, 0.18)
    return jnp.clip(result, -bound, bound).astype(kind)


def setup_inputs(seed: int = 0) -> dict:
    arg_keys = jax.random.split(jax.random.key(seed), 11)
    return {
        "tokens": draw_tokens(jax.random.fold_in(arg_keys[10], 71), 0),
        "documents": jnp.searchsorted(jnp.cumsum(uneven_parts(arg_keys[1], DOCS, TOKENS, MOST_DOC, 1)), jnp.arange(TOKENS), side="right").astype(jnp.int32),
        "pre_gain": jnp.clip(1.0 + 0.18 * jax.random.normal(arg_keys[2], (LAYERS, D), jnp.float32), 0.1, 1.9),
        "query_weight": noise(arg_keys[3], (LAYERS, D, D), D ** -0.5, 0.125, ((1, 8),)),
        "key_weight": noise(arg_keys[4], (LAYERS, D, D), D ** -0.5, 0.125, ((1, 8),)),
        "value_weight": noise(arg_keys[5], (LAYERS, D, D), D ** -0.5, 0.125, ((1, 8),)),
        "gate_weight": noise(arg_keys[6], (LAYERS, D, D), D ** -0.5, 0.125, ((1, 8),)),
        "out_weight": draw_out_weight(jax.random.fold_in(arg_keys[10], 71), 0),
        "position_bias": draw_position_bias(jax.random.fold_in(arg_keys[10], 71), 0),
        "post_gain": jnp.clip(1.0 + 0.18 * jax.random.normal(arg_keys[9], (LAYERS, D), jnp.float32), 0.1, 1.9),
    }


norm_eps = 1e-06

def band_allowed():
    row_block = (jnp.arange(2 * BLOCK) // BLOCK)[:, None]
    col_block = (jnp.arange(PAST + 2 * BLOCK) // BLOCK)[None, :]
    return (col_block >= row_block) & (col_block <= row_block + PAST_BLOCKS)

def distance_index():
    rows_at = jnp.arange(2 * BLOCK)[:, None]
    cols_at = jnp.arange(PAST + 2 * BLOCK)[None, :]
    return (jnp.clip(rows_at - cols_at + PAST, -CLIP, CLIP) + CLIP).astype(jnp.int32)

def windows(extended, groups):
    shaped = extended.reshape((groups + PAST // (2 * BLOCK), 2 * BLOCK) + extended.shape[1:])
    return jnp.concatenate([shaped[offset:offset + groups] for offset in range(PAST // (2 * BLOCK) + 1)], axis=1)

def attend_head(query_head, key_head, value_head, bias_table, doc_tags):
    groups = TOKENS // (2 * BLOCK)
    zero_rows = jnp.zeros((PAST, HD), query_head.dtype)
    key_win = windows(jnp.concatenate([zero_rows, key_head]), groups).astype(jnp.float32)
    value_win = windows(jnp.concatenate([zero_rows, value_head]), groups).astype(jnp.float32)
    doc_win = windows(jnp.concatenate([jnp.zeros((PAST,), jnp.int32), doc_tags]), groups)
    query_groups = query_head.reshape(groups, 2 * BLOCK, HD).astype(jnp.float32)
    query_docs = doc_tags.reshape(groups, 2 * BLOCK)
    scores = jnp.einsum('gqd,gkd->gqk', query_groups, key_win) * HD ** (-0.5) + bias_table[distance_index()][None]
    allowed = band_allowed()[None] & (query_docs[:, :, None] == doc_win[:, None, :])
    scores = jnp.where(allowed, scores, -1e+30)
    row_max = lax.optimization_barrier(jnp.max(scores, axis=2, keepdims=True))
    lifted = jnp.exp(scores - row_max)
    weights_bf = (lifted / lax.optimization_barrier(jnp.sum(lifted, axis=2, keepdims=True))).astype(jnp.bfloat16)
    attended = jnp.einsum('gqk,gkd->gqd', weights_bf.astype(jnp.float32), value_win)
    return attended.reshape(TOKENS, HD)

def reference(tokens, documents, pre_gain, query_weight, key_weight, value_weight, gate_weight, out_weight, position_bias, post_gain):
    doc_tags = (documents + 1).astype(jnp.int32)
    residual = tokens
    for layer_index in range(LAYERS):
        resid_wide = residual.astype(jnp.float32)
        inv_in = lax.rsqrt(lax.optimization_barrier(jnp.mean(resid_wide * resid_wide, axis=1, keepdims=True)) + norm_eps)
        normed = (resid_wide * pre_gain[layer_index]).astype(jnp.bfloat16)
        projected = [(inv_in * jnp.dot(normed, weight[layer_index].T, preferred_element_type=jnp.float32)).astype(jnp.bfloat16) for weight in (query_weight, key_weight, value_weight, gate_weight)]
        heads_first = [product.reshape(TOKENS, HEADS, HD).transpose(1, 0, 2) for product in projected[:3]]

        def one_head(inputs):
            return attend_head(inputs[0], inputs[1], inputs[2], inputs[3], doc_tags)
        attended = lax.map(one_head, (heads_first[0], heads_first[1], heads_first[2], position_bias[layer_index]))
        attended = attended.transpose(1, 0, 2).reshape(TOKENS, D)
        mixed_rows = (attended * jax.nn.silu(projected[3].astype(jnp.float32))).astype(jnp.bfloat16)
        branch = jnp.dot(mixed_rows, out_weight[layer_index].T, preferred_element_type=jnp.float32).astype(jnp.bfloat16)
        branch_wide = branch.astype(jnp.float32)
        inv_out = lax.rsqrt(lax.optimization_barrier(jnp.mean(branch_wide * branch_wide, axis=1, keepdims=True)) + norm_eps)
        residual = (resid_wide + branch_wide * inv_out * post_gain[layer_index]).astype(jnp.bfloat16)
    return residual
```

```python
import functools

import jax
import jax.numpy as jnp
from jax import lax
from jax.experimental import pallas as pl
from jax.experimental.pallas import tpu as pltpu
from jax.sharding import PartitionSpec as P

D = 2048
HD = 64
BLOCK = 64
PAST_BLOCKS = 4
LAYERS = 3
PAST = 256
CLIP = 128
GROUP = 2 * BLOCK
WINDOW = PAST + GROUP
SKEW = 512
CORES = 2
FAR = -1e30

norm_eps = 1e-06
rows_by_rows = (((1,), (1,)), ((), ()))
vmem = pl.BlockSpec(memory_space=pltpu.VMEM)
smem = pl.BlockSpec(memory_space=pltpu.SMEM)
anywhere = pl.BlockSpec(memory_space=pl.ANY)
params = pltpu.CompilerParams(vmem_limit_bytes=40 * 1024 * 1024)


def bias_base(position_bias):
    layers, heads, _ = position_bias.shape
    far = position_bias[:, :, 2 * CLIP :]
    ahead = PAST - CLIP + 1
    near = position_bias[:, :, 2 * CLIP - 1 : 0 : -1]
    rest = SKEW - ahead - near.shape[2]
    return jnp.concatenate(
        [
            jnp.broadcast_to(far, (layers, heads, ahead)),
            near,
            jnp.broadcast_to(far, (layers, heads, rest)),
        ],
        axis=2,
    )


def setup_body(base_ref, row_docs_ref, col_docs_ref, band_ref, mask_ref):
    layers, heads, _ = base_ref.shape
    row_block = lax.broadcasted_iota(jnp.int32, (GROUP, WINDOW), 0) // BLOCK
    col_block = lax.broadcasted_iota(jnp.int32, (GROUP, WINDOW), 1) // BLOCK
    allowed = (col_block >= row_block) & (col_block <= row_block + PAST_BLOCKS)
    for layer in range(layers):
        for head in range(heads):
            row = base_ref[layer, head : head + 1, :]
            skewed = pltpu.roll(
                jnp.broadcast_to(row, (GROUP, SKEW)), 0, 1, stride=1, stride_axis=0
            )
            band_ref[layer, head] = jnp.where(allowed, skewed[:, :WINDOW], FAR)
    for group in range(mask_ref.shape[0]):
        start = group * GROUP
        own = col_docs_ref[start : start + GROUP, :]
        seen = row_docs_ref[:, start : start + WINDOW]
        mask_ref[group] = jnp.where(own == seen, 0.0, FAR)


def setup(base, row_docs, col_docs):
    layers, heads, _ = base.shape
    groups = col_docs.shape[0] // GROUP
    return pl.pallas_call(
        setup_body,
        out_shape=(
            jax.ShapeDtypeStruct((layers, heads, GROUP, WINDOW), jnp.float32),
            jax.ShapeDtypeStruct((groups, GROUP, WINDOW), jnp.float32),
        ),
        in_specs=[vmem, vmem, vmem],
        out_specs=(vmem, vmem),
        compiler_params=params,
        name="setup",
    )(base, row_docs, col_docs)


def block_columns(core, blocks):
    if len(blocks) == 1:
        return [(blocks[0], 0, 0)]
    width = blocks[0].shape[2]
    return [
        (ref, z, pl.multiple_of((CORES * z + (core if side == 0 else 1 - core)) * width, 128))
        for side, ref in enumerate(blocks)
        for z in range(ref.shape[0])
    ]


def proj_body(layer, first, count, *refs):
    core_ref = refs[0]
    blocks = refs[1 : 1 + count]
    rest = list(refs[1 + count :])
    if not first:
        resid_ref, post_ref = rest[:2]
        rest = rest[2:]
    pre_ref = rest[0]
    weights = rest[1:5]
    if first:
        resid_out, q_ref, kv_ref, tail_ref, gate_ref = rest[5:10]
    else:
        resid_out, q_ref, kv_ref, tail_ref, gate_ref = rest[5:10]
    weight_buf, normed_ref, inv_ref, sems = rest[10:]
    copies = [
        pltpu.make_async_copy(weight.at[layer], weight_buf.at[at], sems.at[at])
        for at, weight in enumerate(weights)
    ]
    for copy in copies:
        copy.start()
    rows = normed_ref.shape[0]
    step = BLOCK
    placed = block_columns(core_ref[0], blocks)
    width = blocks[0].shape[2]

    def lane_sum(square):
        total = square[:, :128]
        for at in range(128, square.shape[1], 128):
            total = total + square[:, at : at + 128]
        return total

    def one(index, carry):
        at = pl.ds(pl.multiple_of(index * step, step), step)
        if not first:
            total = jnp.zeros((step, 128), jnp.float32)
            for ref, z, _ in placed:
                part = ref[z, at, :].astype(jnp.float32)
                total = total + lane_sum(part * part)
            inv_out = lax.rsqrt(jnp.sum(total, axis=1, keepdims=True) / D + norm_eps)
        total = jnp.zeros((step, 128), jnp.float32)
        for ref, z, col in placed:
            cols = pl.ds(col, width)
            if first:
                new = ref[z, at, :]
            else:
                part = ref[z, at, :].astype(jnp.float32)
                old = resid_ref[at, cols].astype(jnp.float32)
                new = (old + part * inv_out * post_ref[:, cols]).astype(jnp.bfloat16)
            resid_out[at, cols] = new
            wide = new.astype(jnp.float32)
            total = total + lane_sum(wide * wide)
            normed_ref[at, cols] = (wide * pre_ref[:, cols]).astype(jnp.bfloat16)
        inv_in = lax.rsqrt(jnp.sum(total, axis=1, keepdims=True) / D + norm_eps)
        inv_ref[at, :] = jnp.broadcast_to(inv_in, (step, 128))
        return carry

    lax.fori_loop(0, rows // step, one, 0)
    own = q_ref.shape[1]
    tail_start = rows - PAST
    inv = inv_ref[:, :1]
    for at, copy in enumerate(copies):
        copy.wait()
        product = lax.dot_general(
            normed_ref[...], weight_buf[at], rows_by_rows, preferred_element_type=jnp.float32
        )
        product = (product * inv).astype(jnp.bfloat16)
        if at < 2:
            kv_ref[:, at * own : (at + 1) * own] = product
            tail_ref[:, at * own : (at + 1) * own] = product[tail_start:]
        elif at == 2:
            q_ref[...] = product * jnp.bfloat16(HD ** (-0.5))
        else:
            gate_ref[...] = product


def project(layer, core, blocks, resid, post, pre, weights):
    first = resid is None
    rows = blocks[0].shape[1]
    own = weights[0].shape[1]
    bf = jnp.bfloat16
    operands = [core, *blocks] + ([] if first else [resid, post]) + [pre, *weights]
    specs = [smem] + [vmem] * len(blocks) + ([] if first else [vmem, vmem]) + [vmem]
    specs = specs + [anywhere] * 4
    return pl.pallas_call(
        functools.partial(proj_body, layer, first, len(blocks)),
        out_shape=(
            jax.ShapeDtypeStruct((rows, D), bf),
            jax.ShapeDtypeStruct((rows, own), bf),
            jax.ShapeDtypeStruct((rows, 2 * own), bf),
            jax.ShapeDtypeStruct((PAST, 2 * own), bf),
            jax.ShapeDtypeStruct((rows, own), bf),
        ),
        in_specs=specs,
        out_specs=(vmem,) * 5,
        scratch_shapes=[
            pltpu.VMEM((4, own, D), bf),
            pltpu.VMEM((rows, D), bf),
            pltpu.VMEM((rows, 128), jnp.float32),
            pltpu.SemaphoreType.DMA((4,)),
        ],
        compiler_params=params,
        name="project",
    )(*operands)


def attend_body(q_ref, kv_ref, halo_ref, gate_ref, band_ref, mask_ref, mixed_ref, ext_ref):
    rows, own = q_ref.shape
    span = min(own, 128)
    ext_ref[:PAST, :] = halo_ref[...]
    ext_ref[PAST:, :] = kv_ref[...]
    lane = lax.broadcasted_iota(jnp.int32, (GROUP, span), 1) // HD
    for group in range(rows // GROUP):
        at = slice(group * GROUP, (group + 1) * GROUP)
        seen = slice(group * GROUP, group * GROUP + WINDOW)
        mask = mask_ref[group]
        for start in range(0, own, span):
            cols = slice(start, start + span)
            query = q_ref[at, cols]
            keys = ext_ref[seen, cols]
            values = ext_ref[seen, own + start : own + start + span]
            result = None
            for sub in range(span // HD):
                picked = jnp.where(lane == sub, query, jnp.zeros_like(query))
                scores = lax.dot_general(
                    picked, keys, rows_by_rows, preferred_element_type=jnp.float32
                )
                scores = scores + band_ref[0, start // HD + sub] + mask
                lifted = jnp.exp(scores - jnp.max(scores, axis=1, keepdims=True))
                total = jnp.sum(lifted, axis=1, keepdims=True)
                part = jnp.dot(
                    lifted.astype(jnp.bfloat16), values, preferred_element_type=jnp.float32
                )
                part = part / total
                result = part if result is None else jnp.where(lane == sub, part, result)
            gate = gate_ref[at, cols].astype(jnp.float32)
            mixed_ref[at, cols] = (result * (gate / (1.0 + jnp.exp(-gate)))).astype(jnp.bfloat16)


def attend(layer, q, kv, halo, gate, band, mask):
    rows, own = q.shape
    whole = lambda a: pl.BlockSpec(a.shape, lambda i: (0,) * a.ndim)
    picked = pl.BlockSpec((1,) + band.shape[1:], lambda i: (layer, 0, 0, 0))
    return pl.pallas_call(
        attend_body,
        grid=(1,),
        out_shape=jax.ShapeDtypeStruct((rows, own), jnp.bfloat16),
        in_specs=[whole(q), whole(kv), whole(halo), whole(gate), picked, whole(mask)],
        out_specs=whole(q),
        scratch_shapes=[pltpu.VMEM((PAST + rows, 2 * own), jnp.bfloat16)],
        compiler_params=params,
        name="attend",
    )(q, kv, halo, gate, band, mask)


def out_body(layer, count, last, *refs):
    core_ref = refs[0]
    blocks = refs[1 : 1 + count]
    weight_ref, branch_ref = refs[1 + count : 3 + count]
    rest = refs[3 + count :]
    if last:
        square_ref, rest = rest[0], rest[1:]
    weight_buf, mixed_ref, sem = rest
    copy = pltpu.make_async_copy(weight_ref.at[layer], weight_buf, sem)
    copy.start()
    width = blocks[0].shape[2]
    for ref, z, col in block_columns(core_ref[0], blocks):
        mixed_ref[:, pl.ds(col, width)] = ref[z]
    copy.wait()
    branch = lax.dot_general(
        mixed_ref[...], weight_buf[...], rows_by_rows, preferred_element_type=jnp.float32
    ).astype(jnp.bfloat16)
    branch_ref[...] = branch
    if last:
        wide = branch.astype(jnp.float32)
        total = jnp.sum(wide * wide, axis=1, keepdims=True)
        square_ref[...] = jnp.transpose(jnp.broadcast_to(total, (total.shape[0], 128)))[:8]


def out_project(layer, core, blocks, weight, last):
    rows = blocks[0].shape[1]
    own = weight.shape[1]
    shapes = [jax.ShapeDtypeStruct((rows, own), jnp.bfloat16)]
    if last:
        shapes.append(jax.ShapeDtypeStruct((8, rows), jnp.float32))
    return pl.pallas_call(
        functools.partial(out_body, layer, len(blocks), last),
        out_shape=tuple(shapes),
        in_specs=[smem] + [vmem] * len(blocks) + [anywhere],
        out_specs=(vmem,) * len(shapes),
        scratch_shapes=[
            pltpu.VMEM((own, D), jnp.bfloat16),
            pltpu.VMEM((rows, D), jnp.bfloat16),
            pltpu.SemaphoreType.DMA,
        ],
        compiler_params=params,
        name="out_project",
    )(core, *blocks, weight)


def finish_body(resid_ref, branch_ref, gain_ref, *refs):
    out_ref = refs[-1]
    total = refs[0][...]
    for ref in refs[1:-1]:
        total = total + ref[...]
    rows = out_ref.shape[0]
    column = jnp.transpose(jnp.broadcast_to(total[:1], (128, rows)))[:, :1]
    inv_out = lax.rsqrt(column / D + norm_eps)
    old = resid_ref[...].astype(jnp.float32)
    branch = branch_ref[...].astype(jnp.float32)
    out_ref[...] = (old + branch * inv_out * gain_ref[...]).astype(jnp.bfloat16)


def finish(resid_cols, branch, gain_cols, totals):
    return pl.pallas_call(
        finish_body,
        out_shape=jax.ShapeDtypeStruct(branch.shape, jnp.bfloat16),
        in_specs=[vmem] * (3 + len(totals)),
        out_specs=vmem,
        compiler_params=params,
        name="finish",
    )(resid_cols, branch, gain_cols, *totals)


def partner(x):
    size = lax.axis_size("tp")
    return lax.ppermute(x, "tp", [(i, i ^ 1) for i in range(size)])


def gather(x):
    size = lax.axis_size("tp")
    if x.shape[1] % 128 or size % CORES:
        return (lax.all_gather(x, "tp", axis=1, tiled=True)[None],)
    lines = [list(range(core, size, CORES)) for core in range(CORES)]
    own = lax.all_gather(x, "tp", axis=0, axis_index_groups=lines)
    return own, partner(own)


def total_over_features(square):
    size = lax.axis_size("tp")
    if size % CORES or size > 8:
        return (lax.psum(square, "tp"),)
    both = square + partner(square)
    return (both,) + tuple(
        lax.ppermute(both, "tp", [(i, (i + hop) % size) for i in range(size)])
        for hop in range(CORES, size, CORES)
    )


def from_behind(block):
    size = lax.axis_size("sp")
    return lax.ppermute(block, "sp", [(i, (i + 1) % size) for i in range(size)])


def local(
    tokens,
    documents,
    pre_gain,
    query_weight,
    key_weight,
    value_weight,
    gate_weight,
    out_weight,
    position_bias,
    post_gain,
):
    rows, own = tokens.shape
    tp_at = lax.axis_index("tp")
    core = jnp.reshape(tp_at % CORES, (1,)).astype(jnp.int32)
    doc_tags = documents + 1
    behind = from_behind(doc_tags[rows - PAST :])
    behind = jnp.where(lax.axis_index("sp") == 0, 0, behind)
    row_docs = jnp.concatenate([behind, doc_tags])[None, :]
    col_docs = doc_tags[:, None]
    blocks = gather(tokens)
    band, mask = setup(bias_base(position_bias), row_docs, col_docs)
    residual = None
    for layer in range(LAYERS):
        residual, q, kv, tail, gate = project(
            layer,
            core,
            blocks,
            residual,
            post_gain[layer - 1 : layer] if layer else None,
            pre_gain[layer : layer + 1],
            (key_weight, value_weight, query_weight, gate_weight),
        )
        halo = from_behind(tail)
        mixed = attend(layer, q, kv, halo, gate, band, mask)
        last = layer + 1 == LAYERS
        result = out_project(layer, core, gather(mixed), out_weight, last)
        if not last:
            blocks = gather(result[0])
    branch, square = result
    start = tp_at * own
    return finish(
        lax.dynamic_slice_in_dim(residual, start, own, 1),
        branch,
        lax.dynamic_slice_in_dim(post_gain[LAYERS - 1 :], start, own, 1),
        total_over_features(square),
    )


def solution(mesh):
    placed = (
        P("sp", "tp"),
        P("sp"),
        P(),
        P(None, "tp", None),
        P(None, "tp", None),
        P(None, "tp", None),
        P(None, "tp", None),
        P(None, "tp", None),
        P(None, "tp", None),
        P(),
    )
    return jax.shard_map(
        local, mesh=mesh, in_specs=placed, out_specs=P("sp", "tp"), check_vma=False
    )
```

```python
import functools

import jax
import jax.numpy as jnp
from jax import lax
from jax.experimental import pallas as pl
from jax.experimental.pallas import tpu as pltpu
from jax.sharding import PartitionSpec as P

D = 2048
HD = 64
BLOCK = 64
PAST_BLOCKS = 4
LAYERS = 3
PAST = 256
CLIP = 128
GROUP = 2 * BLOCK
WINDOW = PAST + GROUP
SKEW = 512
CORES = 2
FAR = -1e30

norm_eps = 1e-06
rows_by_rows = (((1,), (1,)), ((), ()))
vmem = pl.BlockSpec(memory_space=pltpu.VMEM)
smem = pl.BlockSpec(memory_space=pltpu.SMEM)
hbm = pl.BlockSpec(memory_space=pltpu.HBM)
params = pltpu.CompilerParams(vmem_limit_bytes=40 * 1024 * 1024)


def turn(vector, axis):
    size = GROUP
    diagonal = lax.broadcasted_iota(jnp.int32, (size, size), 0) == lax.broadcasted_iota(
        jnp.int32, (size, size), 1
    )
    spread = jnp.where(diagonal, jnp.broadcast_to(vector, (size, size)), jnp.zeros_like(vector))
    return jnp.sum(spread, axis=axis, keepdims=True)


def setup_body(sp_ref, bias_ref, docs_ref, behind_ref, band_ref, mask_ref):
    layers, heads, entries = bias_ref.shape
    row_block = lax.broadcasted_iota(jnp.int32, (GROUP, WINDOW), 0) // BLOCK
    col_block = lax.broadcasted_iota(jnp.int32, (GROUP, WINDOW), 1) // BLOCK
    allowed = (col_block >= row_block) & (col_block <= row_block + PAST_BLOCKS)
    shift = lax.broadcasted_iota(jnp.int32, (entries, SKEW), 1)
    entry = jnp.where(shift < WINDOW, jnp.minimum(PAST - shift, CLIP) + CLIP, 2 * CLIP)
    pick = (lax.broadcasted_iota(jnp.int32, (entries, SKEW), 0) == entry).astype(jnp.float32)
    for layer in range(layers):
        base = lax.dot_general(
            bias_ref[layer],
            pick,
            (((1,), (0,)), ((), ())),
            precision=lax.Precision.HIGHEST,
            preferred_element_type=jnp.float32,
        )
        for head in range(heads):
            row = jnp.broadcast_to(base[head : head + 1, :], (GROUP, SKEW))
            skewed = pltpu.roll(row, 0, 1, stride=1, stride_axis=0)
            band_ref[layer, head] = jnp.where(allowed, skewed[:, :WINDOW], FAR)
    behind = jnp.where(sp_ref[0] == 0, -1, behind_ref[...])
    docs = docs_ref[...]
    seen = jnp.concatenate([behind, docs], axis=1)
    for group in range(mask_ref.shape[0]):
        start = group * GROUP
        own = turn(docs[:, start : start + GROUP], 1)
        mask_ref[group] = jnp.where(own == seen[:, start : start + WINDOW], 0.0, FAR)


def setup(sp_at, position_bias, docs, behind):
    layers, heads, _ = position_bias.shape
    groups = docs.shape[1] // GROUP
    return pl.pallas_call(
        setup_body,
        out_shape=(
            jax.ShapeDtypeStruct((layers, heads, GROUP, WINDOW), jnp.float32),
            jax.ShapeDtypeStruct((groups, GROUP, WINDOW), jnp.float32),
        ),
        in_specs=[smem, vmem, vmem, vmem],
        out_specs=(vmem, vmem),
        compiler_params=params,
        name="setup",
    )(sp_at, position_bias, docs, behind)


def block_columns(core, blocks):
    if len(blocks) == 1:
        return [(blocks[0], 0, 0)]
    width = blocks[0].shape[2]
    return [
        (ref, z, pl.multiple_of((CORES * z + (core if side == 0 else 1 - core)) * width, 128))
        for side, ref in enumerate(blocks)
        for z in range(ref.shape[0])
    ]


def lane_sum(square):
    total = square[:, :128]
    for at in range(128, square.shape[1], 128):
        total = total + square[:, at : at + 128]
    return total


def update_rows(core, blocks, offset, resid_ref, post_ref, pre_ref, resid_out, normed_ref, inv_ref):
    step = BLOCK
    placed = block_columns(core, blocks)
    width = blocks[0].shape[2]

    def one(index, carry):
        at = pl.ds(pl.multiple_of(index * step, step), step)
        source = pl.ds(pl.multiple_of(offset + index * step, step), step)
        if resid_ref is not None:
            total = jnp.zeros((step, 128), jnp.float32)
            for ref, z, _ in placed:
                part = ref[z, source, :].astype(jnp.float32)
                total = total + lane_sum(part * part)
            inv_out = lax.rsqrt(jnp.sum(total, axis=1, keepdims=True) / D + norm_eps)
        total = jnp.zeros((step, 128), jnp.float32)
        for ref, z, col in placed:
            cols = pl.ds(col, width)
            if resid_ref is None:
                new = ref[z, source, :]
            else:
                part = ref[z, source, :].astype(jnp.float32)
                old = resid_ref[at, cols].astype(jnp.float32)
                new = (old + part * inv_out * post_ref[:, cols]).astype(jnp.bfloat16)
            resid_out[at, cols] = new
            wide = new.astype(jnp.float32)
            total = total + lane_sum(wide * wide)
            normed_ref[at, cols] = (wide * pre_ref[:, cols]).astype(jnp.bfloat16)
        inv_in = lax.rsqrt(jnp.sum(total, axis=1, keepdims=True) / D + norm_eps)
        inv_ref[at, :] = jnp.broadcast_to(inv_in, (step, 128))
        return carry

    lax.fori_loop(0, resid_out.shape[0] // step, one, 0)


def scaled_product(normed_ref, inv_ref, weight):
    product = lax.dot_general(
        normed_ref[...], weight, rows_by_rows, preferred_element_type=jnp.float32
    )
    return (product * inv_ref[:, :1]).astype(jnp.bfloat16)


def fetch(layer, weights, weight_buf, sems):
    copies = [
        pltpu.make_async_copy(weight.at[layer], weight_buf.at[at], sems.at[at])
        for at, weight in enumerate(weights)
    ]
    for copy in copies:
        copy.start()
    return copies


def tail_body(layer, first, count, offset, *refs):
    core_ref, refs = refs[0], refs[1:]
    blocks, refs = refs[:count], refs[count:]
    resid_ref = post_ref = None
    if not first:
        (resid_ref, post_ref), refs = refs[:2], refs[2:]
    pre_ref, weights = refs[0], refs[1:3]
    resid_out, normed_ref, inv_ref, tail_ref, weight_buf, sems = refs[3:]
    copies = fetch(layer, weights, weight_buf, sems)
    update_rows(
        core_ref[0], blocks, offset, resid_ref, post_ref, pre_ref, resid_out, normed_ref, inv_ref
    )
    own = weight_buf.shape[1]
    for at, copy in enumerate(copies):
        copy.wait()
        tail_ref[:, at * own : (at + 1) * own] = scaled_product(
            normed_ref, inv_ref, weight_buf[at]
        )


def project_tail(layer, core, blocks, resid, post, pre, weights):
    first = resid is None
    rows = blocks[0].shape[1]
    own = weights[0].shape[1]
    bf = jnp.bfloat16
    operands = [core, *blocks] + ([] if first else [resid, post]) + [pre, *weights]
    specs = [smem] + [vmem] * (len(operands) - 3) + [hbm] * 2
    return pl.pallas_call(
        functools.partial(tail_body, layer, first, len(blocks), rows - PAST),
        out_shape=(
            jax.ShapeDtypeStruct((PAST, D), bf),
            jax.ShapeDtypeStruct((PAST, D), bf),
            jax.ShapeDtypeStruct((PAST, 128), jnp.float32),
            jax.ShapeDtypeStruct((PAST, 2 * own), bf),
        ),
        in_specs=specs,
        out_specs=(vmem,) * 4,
        scratch_shapes=[pltpu.VMEM((2, own, D), bf), pltpu.SemaphoreType.DMA((2,))],
        compiler_params=params,
        name="project_tail",
    )(*operands)


def attend_group(query, gate, ext_ref, seen, band_ref, mask, own):
    span = min(own, 128)
    lane = lax.broadcasted_iota(jnp.int32, (GROUP, span), 1) // HD
    results = []
    for start in range(0, own, span):
        cols = slice(start, start + span)
        keys = ext_ref[seen, cols]
        values = ext_ref[seen, own + start : own + start + span]
        result = None
        for sub in range(span // HD):
            picked = jnp.where(lane == sub, query[:, cols], jnp.zeros((), query.dtype))
            scores = lax.dot_general(
                picked, keys, rows_by_rows, preferred_element_type=jnp.float32
            )
            scores = scores + band_ref[0, start // HD + sub] + mask
            lifted = jnp.exp(scores - jnp.max(scores, axis=1, keepdims=True))
            total = jnp.sum(lifted, axis=1, keepdims=True)
            part = jnp.dot(lifted.astype(jnp.bfloat16), values, preferred_element_type=jnp.float32)
            part = part / total
            result = part if result is None else jnp.where(lane == sub, part, result)
        wide = gate[:, cols].astype(jnp.float32)
        results.append((result * (wide / (1.0 + jnp.exp(-wide)))).astype(jnp.bfloat16))
    return results


def store_group(mixed_ref, at, results):
    start = 0
    for result in results:
        mixed_ref[at, start : start + result.shape[1]] = result
        start = start + result.shape[1]


def local_body(layer, first, count, *refs):
    core_ref, refs = refs[0], refs[1:]
    blocks, refs = refs[:count], refs[count:]
    resid_ref = post_ref = None
    if not first:
        (resid_ref, post_ref), refs = refs[:2], refs[2:]
    pre_ref, tail_normed_ref, tail_inv_ref, tail_ref, band_ref, mask_ref = refs[:6]
    weights = refs[6:10]
    resid_out, head_ref, query_out, gate_out, mixed_ref = refs[10:15]
    weight_buf, sems, normed_ref, inv_ref, ext_ref = refs[15:]
    copies = fetch(layer, weights, weight_buf, sems)
    head_rows = resid_out.shape[0]
    update_rows(
        core_ref[0], blocks, 0, resid_ref, post_ref, pre_ref, resid_out, normed_ref, inv_ref
    )
    own = weight_buf.shape[1]
    rest = query_out.shape[0]
    cut = rest - head_rows
    pieces = []
    for at, copy in enumerate(copies):
        copy.wait()
        head = scaled_product(normed_ref, inv_ref, weight_buf[at])
        if at < 2:
            head_ref[:, at * own : (at + 1) * own] = head
            continue
        tail = scaled_product(tail_normed_ref, tail_inv_ref, weight_buf[at])
        if at == 2:
            head = head * jnp.bfloat16(HD ** (-0.5))
            tail = tail * jnp.bfloat16(HD ** (-0.5))
        target = query_out if at == 2 else gate_out
        target[:head_rows] = head
        target[head_rows:] = tail[:cut]
        pieces.append(tail[cut:])
    ext_ref[:head_rows] = head_ref[...]
    ext_ref[head_rows:] = tail_ref[...]
    groups = mask_ref.shape[0]
    for index, group in enumerate(range(rest // GROUP, groups)):
        at = slice(index * GROUP, (index + 1) * GROUP)
        seen = slice(group * GROUP - PAST, group * GROUP - PAST + WINDOW)
        store_group(
            mixed_ref,
            at,
            attend_group(
                pieces[0][at], pieces[1][at], ext_ref, seen, band_ref, mask_ref[group], own
            ),
        )


def layer_of(band, layer):
    return pl.BlockSpec((1,) + band.shape[1:], lambda i: (layer, 0, 0, 0))


def whole_of(shape):
    return pl.BlockSpec(shape, lambda i: (0,) * len(shape))


def project_local(layer, core, blocks, resid, post, pre, tail_parts, band, mask, weights):
    first = resid is None
    rows = blocks[0].shape[1]
    own = weights[0].shape[1]
    head_rows = rows - PAST
    bf = jnp.bfloat16
    moved = [*blocks] + ([] if first else [resid, post]) + [pre, *tail_parts]
    operands = [core, *moved, band, mask, *weights]
    specs = [smem] + [whole_of(a.shape) for a in moved] + [layer_of(band, layer)]
    specs = specs + [whole_of(mask.shape)] + [hbm] * 4
    shapes = [
        ((head_rows, D), bf),
        ((head_rows, 2 * own), bf),
        ((PAST, own), bf),
        ((PAST, own), bf),
        ((rows - PAST, own), bf),
    ]
    return pl.pallas_call(
        functools.partial(local_body, layer, first, len(blocks)),
        grid=(1,),
        out_shape=tuple(jax.ShapeDtypeStruct(shape, kind) for shape, kind in shapes),
        in_specs=specs,
        out_specs=tuple(whole_of(shape) for shape, _ in shapes),
        scratch_shapes=[
            pltpu.VMEM((4, own, D), bf),
            pltpu.SemaphoreType.DMA((4,)),
            pltpu.VMEM((head_rows, D), bf),
            pltpu.VMEM((head_rows, 128), jnp.float32),
            pltpu.VMEM((rows, 2 * own), bf),
        ],
        compiler_params=params,
        name="project_local",
    )(*operands)


def attend_body(
    query_ref, gate_ref, head_ref, tail_ref, halo_ref, local_ref, band_ref, mask_ref, mixed_ref, ext_ref
):
    head_rows, own = head_ref.shape[0], query_ref.shape[1]
    rest = query_ref.shape[0]
    ext_ref[:PAST] = halo_ref[...]
    ext_ref[PAST : PAST + head_rows] = head_ref[...]
    ext_ref[PAST + head_rows :] = tail_ref[...]
    mixed_ref[rest:] = local_ref[...]
    for group in range(rest // GROUP):
        at = slice(group * GROUP, (group + 1) * GROUP)
        seen = slice(group * GROUP, group * GROUP + WINDOW)
        store_group(
            mixed_ref,
            at,
            attend_group(
                query_ref[at], gate_ref[at], ext_ref, seen, band_ref, mask_ref[group], own
            ),
        )


def attend(layer, query, gate, head, tail, halo, local_mixed, band, mask):
    own = query.shape[1]
    rows = head.shape[0] + tail.shape[0]
    moved = [query, gate, head, tail, halo, local_mixed]
    return pl.pallas_call(
        attend_body,
        grid=(1,),
        out_shape=jax.ShapeDtypeStruct((rows, own), jnp.bfloat16),
        in_specs=[whole_of(a.shape) for a in moved]
        + [layer_of(band, layer), whole_of(mask.shape)],
        out_specs=whole_of((rows, own)),
        scratch_shapes=[pltpu.VMEM((PAST + rows, 2 * own), jnp.bfloat16)],
        compiler_params=params,
        name="attend",
    )(*moved, band, mask)


def out_body(layer, count, last, *refs):
    core_ref = refs[0]
    blocks = refs[1 : 1 + count]
    weight_ref, branch_ref = refs[1 + count : 3 + count]
    rest = refs[3 + count :]
    if last:
        square_ref, rest = rest[0], rest[1:]
    weight_buf, mixed_ref, sem = rest
    copy = pltpu.make_async_copy(weight_ref.at[layer], weight_buf, sem)
    copy.start()
    width = blocks[0].shape[2]
    for ref, z, col in block_columns(core_ref[0], blocks):
        mixed_ref[:, pl.ds(col, width)] = ref[z]
    copy.wait()
    branch = lax.dot_general(
        mixed_ref[...], weight_buf[...], rows_by_rows, preferred_element_type=jnp.float32
    ).astype(jnp.bfloat16)
    branch_ref[...] = branch
    if last:
        wide = branch.astype(jnp.float32)
        total = jnp.sum(wide * wide, axis=1, keepdims=True)
        for start in range(0, total.shape[0], GROUP):
            square_ref[:, start : start + GROUP] = turn(total[start : start + GROUP], 0)


def out_project(layer, core, blocks, weight, last):
    rows = blocks[0].shape[1]
    own = weight.shape[1]
    shapes = [jax.ShapeDtypeStruct((rows, own), jnp.bfloat16)]
    if last:
        shapes.append(jax.ShapeDtypeStruct((1, rows), jnp.float32))
    return pl.pallas_call(
        functools.partial(out_body, layer, len(blocks), last),
        out_shape=tuple(shapes),
        in_specs=[smem] + [vmem] * len(blocks) + [hbm],
        out_specs=(vmem,) * len(shapes),
        scratch_shapes=[
            pltpu.VMEM((own, D), jnp.bfloat16),
            pltpu.VMEM((rows, D), jnp.bfloat16),
            pltpu.SemaphoreType.DMA,
        ],
        compiler_params=params,
        name="out_project",
    )(core, *blocks, weight)


def finish_body(resid_ref, branch_ref, gain_ref, *refs):
    out_ref = refs[-1]
    total = refs[0][...]
    for ref in refs[1:-1]:
        total = total + ref[...]
    for start in range(0, out_ref.shape[0], GROUP):
        at = slice(start, start + GROUP)
        inv_out = lax.rsqrt(turn(total[:, at], 1) / D + norm_eps)
        old = resid_ref[at].astype(jnp.float32)
        branch = branch_ref[at].astype(jnp.float32)
        out_ref[at] = (old + branch * inv_out * gain_ref[...]).astype(jnp.bfloat16)


def finish(resid_cols, branch, gain_cols, totals):
    return pl.pallas_call(
        finish_body,
        out_shape=jax.ShapeDtypeStruct(branch.shape, jnp.bfloat16),
        in_specs=[vmem] * (3 + len(totals)),
        out_specs=vmem,
        compiler_params=params,
        name="finish",
    )(resid_cols, branch, gain_cols, *totals)


def partner(x):
    size = lax.axis_size("tp")
    return lax.ppermute(x, "tp", [(i, i ^ 1) for i in range(size)])


def gather(x):
    size = lax.axis_size("tp")
    if x.shape[1] % 128 or size % CORES:
        return (lax.all_gather(x, "tp", axis=1, tiled=True)[None],)
    lines = [list(range(core, size, CORES)) for core in range(CORES)]
    own = lax.all_gather(x, "tp", axis=0, axis_index_groups=lines)
    return own, partner(own)


def total_over_features(square):
    size = lax.axis_size("tp")
    if size % CORES or size > 8:
        return (lax.psum(square, "tp"),)
    both = square + partner(square)
    return (both,) + tuple(
        lax.ppermute(both, "tp", [(i, (i + hop) % size) for i in range(size)])
        for hop in range(CORES, size, CORES)
    )


def from_behind(block):
    size = lax.axis_size("sp")
    return lax.ppermute(block, "sp", [(i, (i + 1) % size) for i in range(size)])


def local(
    tokens,
    documents,
    pre_gain,
    query_weight,
    key_weight,
    value_weight,
    gate_weight,
    out_weight,
    position_bias,
    post_gain,
):
    rows, own = tokens.shape
    tp_at = lax.axis_index("tp")
    core = jnp.reshape(tp_at % CORES, (1,)).astype(jnp.int32)
    sp_at = jnp.reshape(lax.axis_index("sp"), (1,)).astype(jnp.int32)
    docs = documents[None, :]
    behind = from_behind(docs[:, rows - PAST :])
    blocks = gather(tokens)
    band, mask = setup(sp_at, position_bias, docs, behind)
    tail_resid = head_resid = None
    for layer in range(LAYERS):
        post = post_gain[layer - 1 : layer] if layer else None
        pre = pre_gain[layer : layer + 1]
        tail_resid, normed, inv, tail = project_tail(
            layer, core, blocks, tail_resid, post, pre, (key_weight, value_weight)
        )
        halo = from_behind(tail)
        head_resid, head, query, gate, local_mixed = project_local(
            layer,
            core,
            blocks,
            head_resid,
            post,
            pre,
            (normed, inv, tail),
            band,
            mask,
            (key_weight, value_weight, query_weight, gate_weight),
        )
        mixed = attend(layer, query, gate, head, tail, halo, local_mixed, band, mask)
        last = layer + 1 == LAYERS
        result = out_project(layer, core, gather(mixed), out_weight, last)
        if not last:
            blocks = gather(result[0])
    branch, square = result
    start = tp_at * own
    resid_cols = jnp.concatenate(
        [lax.dynamic_slice_in_dim(part, start, own, 1) for part in (head_resid, tail_resid)]
    )
    return finish(
        resid_cols,
        branch,
        lax.dynamic_slice_in_dim(post_gain[LAYERS - 1 :], start, own, 1),
        total_over_features(square),
    )


def solution(mesh):
    placed = (
        P("sp", "tp"),
        P("sp"),
        P(),
        P(None, "tp", None),
        P(None, "tp", None),
        P(None, "tp", None),
        P(None, "tp", None),
        P(None, "tp", None),
        P(None, "tp", None),
        P(),
    )
    return jax.shard_map(
        local, mesh=mesh, in_specs=placed, out_specs=P("sp", "tp"), check_vma=False
    )
```

```python
import functools

import jax
import jax.numpy as jnp
from jax import lax
from jax.experimental import pallas as pl
from jax.experimental.pallas import tpu as pltpu
from jax.sharding import PartitionSpec as P

D = 2048
HD = 64
BLOCK = 64
PAST_BLOCKS = 4
LAYERS = 3
PAST = 256
CLIP = 128
GROUP = 2 * BLOCK
WINDOW = PAST + GROUP
SKEW = 512
CORES = 2
FAR = -1e30

norm_eps = 1e-06
rows_by_rows = (((1,), (1,)), ((), ()))
vmem = pl.BlockSpec(memory_space=pltpu.VMEM)
hbm = pl.BlockSpec(memory_space=pltpu.HBM)
params = pltpu.CompilerParams(vmem_limit_bytes=16 * 1024 * 1024)


def turn(vector, axis):
    size = GROUP
    diagonal = lax.broadcasted_iota(jnp.int32, (size, size), 0) == lax.broadcasted_iota(
        jnp.int32, (size, size), 1
    )
    spread = jnp.where(diagonal, jnp.broadcast_to(vector, (size, size)), jnp.zeros_like(vector))
    return jnp.sum(spread, axis=axis, keepdims=True)


def setup_body(bias_ref, docs_ref, *outs):
    bands, mask_ref = outs[:-1], outs[-1]
    layers, heads, entries = bias_ref.shape
    row_block = lax.broadcasted_iota(jnp.int32, (GROUP, WINDOW), 0) // BLOCK
    col_block = lax.broadcasted_iota(jnp.int32, (GROUP, WINDOW), 1) // BLOCK
    allowed = (col_block >= row_block) & (col_block <= row_block + PAST_BLOCKS)
    shift = lax.broadcasted_iota(jnp.int32, (entries, SKEW), 1)
    entry = jnp.where(shift < WINDOW, jnp.minimum(PAST - shift, CLIP) + CLIP, 2 * CLIP)
    pick = (lax.broadcasted_iota(jnp.int32, (entries, SKEW), 0) == entry).astype(jnp.float32)
    for layer in range(layers):
        base = lax.dot_general(
            bias_ref[layer],
            pick,
            (((1,), (0,)), ((), ())),
            precision=lax.Precision.HIGHEST,
            preferred_element_type=jnp.float32,
        )
        for head in range(heads):
            row = jnp.broadcast_to(base[head : head + 1, :], (GROUP, SKEW))
            skewed = pltpu.roll(row, 0, 1, stride=1, stride_axis=0)
            bands[layer][head] = jnp.where(allowed, skewed[:, :WINDOW], FAR)
    docs = docs_ref[...]
    for index in range(mask_ref.shape[0]):
        start = PAST + index * GROUP
        mask_ref[index] = doc_mask(docs[:, start : start + GROUP], docs[:, start - PAST : start + GROUP])


def doc_mask(own, seen):
    return jnp.where(turn(own, 1) == seen, 0.0, FAR)


def setup(position_bias, docs):
    layers, heads, _ = position_bias.shape
    groups = (docs.shape[1] - PAST) // GROUP
    return pl.pallas_call(
        setup_body,
        out_shape=(
            *[jax.ShapeDtypeStruct((heads, GROUP, WINDOW), jnp.float32) for _ in range(layers)],
            jax.ShapeDtypeStruct((groups, GROUP, WINDOW), jnp.float32),
        ),
        in_specs=[vmem, vmem],
        out_specs=(vmem,) * (layers + 1),
        compiler_params=params,
        name="setup",
    )(position_bias, docs)


def block_columns(blocks):
    if len(blocks) == 1:
        return [(blocks[0], 0, 0)]
    core = lax.rem(lax.axis_index("tp"), CORES)
    width = blocks[0].shape[2]
    return [
        (ref, z, pl.multiple_of((CORES * z + (core if side == 0 else 1 - core)) * width, 128))
        for side, ref in enumerate(blocks)
        for z in range(ref.shape[0])
    ]


def lane_sum(square):
    total = square[:, :128]
    for at in range(128, square.shape[1], 128):
        total = total + square[:, at : at + 128]
    return total


def update_rows(layer, blocks, offset, resid_ref, post_ref, pre_ref, resid_out, normed_ref, inv_ref):
    step = BLOCK
    placed = block_columns(blocks)
    width = blocks[0].shape[2]

    def one(index, carry):
        at = pl.ds(pl.multiple_of(index * step, step), step)
        source = pl.ds(pl.multiple_of(offset + index * step, step), step)
        if resid_ref is not None:
            total = jnp.zeros((step, 128), jnp.float32)
            for ref, z, _ in placed:
                part = ref[z, source, :].astype(jnp.float32)
                total = total + lane_sum(part * part)
            inv_out = lax.rsqrt(jnp.sum(total, axis=1, keepdims=True) / D + norm_eps)
        total = jnp.zeros((step, 128), jnp.float32)
        for ref, z, col in placed:
            cols = pl.ds(col, width)
            if resid_ref is None:
                new = ref[z, source, :]
            else:
                part = ref[z, source, :].astype(jnp.float32)
                old = resid_ref[at, cols].astype(jnp.float32)
                new = (old + part * inv_out * post_ref[layer - 1 : layer, cols]).astype(jnp.bfloat16)
            resid_out[at, cols] = new
            wide = new.astype(jnp.float32)
            total = total + lane_sum(wide * wide)
            normed_ref[at, cols] = (wide * pre_ref[layer : layer + 1, cols]).astype(jnp.bfloat16)
        inv_in = lax.rsqrt(jnp.sum(total, axis=1, keepdims=True) / D + norm_eps)
        inv_ref[at, :] = jnp.broadcast_to(inv_in, (step, 128))
        return carry

    lax.fori_loop(0, resid_out.shape[0] // step, one, 0)


def scaled_product(normed_ref, inv_ref, weight):
    product = lax.dot_general(
        normed_ref[...], weight, rows_by_rows, preferred_element_type=jnp.float32
    )
    return (product * inv_ref[:, :1]).astype(jnp.bfloat16)


def fetch(layer, weights, weight_buf, sems):
    copies = [
        pltpu.make_async_copy(weight.at[layer], weight_buf.at[at], sems.at[at])
        for at, weight in enumerate(weights)
    ]
    for copy in copies:
        copy.start()
    return copies


def tail_body(layer, first, count, offset, *refs):
    blocks, refs = refs[:count], refs[count:]
    resid_ref = post_ref = None
    if not first:
        (resid_ref, post_ref), refs = refs[:2], refs[2:]
    pre_ref, weights = refs[0], refs[1:3]
    resid_out, normed_ref, inv_ref, tail_ref, weight_buf, sems = refs[3:]
    copies = fetch(layer, weights, weight_buf, sems)
    update_rows(
        layer, blocks, offset, resid_ref, post_ref, pre_ref, resid_out, normed_ref, inv_ref
    )
    own = weight_buf.shape[1]
    for at, copy in enumerate(copies):
        copy.wait()
        tail_ref[:, at * own : (at + 1) * own] = scaled_product(
            normed_ref, inv_ref, weight_buf[at]
        )


def project_tail(layer, blocks, resid, post, pre, weights):
    first = resid is None
    rows = blocks[0].shape[1]
    own = weights[0].shape[1]
    bf = jnp.bfloat16
    operands = [*blocks] + ([] if first else [resid, post]) + [pre, *weights]
    specs = [vmem] * (len(operands) - 2) + [hbm] * 2
    return pl.pallas_call(
        functools.partial(tail_body, layer, first, len(blocks), rows - PAST),
        out_shape=(
            jax.ShapeDtypeStruct((PAST, D), bf),
            jax.ShapeDtypeStruct((PAST, D), bf),
            jax.ShapeDtypeStruct((PAST, 128), jnp.float32),
            jax.ShapeDtypeStruct((PAST, 2 * own), bf),
        ),
        in_specs=specs,
        out_specs=(vmem,) * 4,
        scratch_shapes=[pltpu.VMEM((2, own, D), bf), pltpu.SemaphoreType.DMA((2,))],
        compiler_params=params,
        name="project_tail",
    )(*operands)


def attend_group(query, gate, ext_ref, seen, band_ref, mask, own):
    span = min(own, 128)
    lane = lax.broadcasted_iota(jnp.int32, (GROUP, span), 1) // HD
    results = []
    for start in range(0, own, span):
        cols = slice(start, start + span)
        keys = ext_ref[seen, cols]
        values = ext_ref[seen, own + start : own + start + span]
        result = None
        for sub in range(span // HD):
            picked = jnp.where(lane == sub, query[:, cols], jnp.zeros((), query.dtype))
            scores = lax.dot_general(
                picked, keys, rows_by_rows, preferred_element_type=jnp.float32
            )
            scores = scores + band_ref[start // HD + sub] + mask
            lifted = jnp.exp(scores - jnp.max(scores, axis=1, keepdims=True))
            total = jnp.sum(lifted, axis=1, keepdims=True)
            part = jnp.dot(lifted.astype(jnp.bfloat16), values, preferred_element_type=jnp.float32)
            part = part / total
            result = part if result is None else jnp.where(lane == sub, part, result)
        wide = gate[:, cols].astype(jnp.float32)
        results.append((result * (wide / (1.0 + jnp.exp(-wide)))).astype(jnp.bfloat16))
    return results


def store_group(mixed_ref, at, results):
    start = 0
    for result in results:
        mixed_ref[at, start : start + result.shape[1]] = result
        start = start + result.shape[1]


def local_body(layer, first, count, *refs):
    blocks, refs = refs[:count], refs[count:]
    resid_ref = post_ref = None
    if not first:
        (resid_ref, post_ref), refs = refs[:2], refs[2:]
    pre_ref, tail_normed_ref, tail_inv_ref, tail_ref, band_ref, mask_ref = refs[:6]
    weights = refs[6:10]
    resid_out, head_ref, query_out, gate_out, mixed_ref = refs[10:15]
    weight_buf, sems, normed_ref, inv_ref, ext_ref = refs[15:]
    copies = fetch(layer, weights, weight_buf, sems)
    head_rows = resid_out.shape[0]
    update_rows(
        layer, blocks, 0, resid_ref, post_ref, pre_ref, resid_out, normed_ref, inv_ref
    )
    own = weight_buf.shape[1]
    rest = query_out.shape[0]
    cut = rest - head_rows
    pieces = []
    for at, copy in enumerate(copies):
        copy.wait()
        head = scaled_product(normed_ref, inv_ref, weight_buf[at])
        if at < 2:
            head_ref[:, at * own : (at + 1) * own] = head
            continue
        tail = scaled_product(tail_normed_ref, tail_inv_ref, weight_buf[at])
        if at == 2:
            head = head * jnp.bfloat16(HD ** (-0.5))
            tail = tail * jnp.bfloat16(HD ** (-0.5))
        target = query_out if at == 2 else gate_out
        target[:head_rows] = head
        target[head_rows:] = tail[:cut]
        pieces.append(tail[cut:])
    ext_ref[:head_rows] = head_ref[...]
    ext_ref[head_rows:] = tail_ref[...]
    for index in range(mask_ref.shape[0]):
        at = slice(index * GROUP, (index + 1) * GROUP)
        seen = slice(index * GROUP, index * GROUP + WINDOW)
        store_group(
            mixed_ref,
            at,
            attend_group(
                pieces[0][at], pieces[1][at], ext_ref, seen, band_ref, mask_ref[index], own
            ),
        )


def project_local(layer, blocks, resid, post, pre, tail_parts, band, mask, weights):
    first = resid is None
    rows = blocks[0].shape[1]
    own = weights[0].shape[1]
    head_rows = rows - PAST
    bf = jnp.bfloat16
    moved = [*blocks] + ([] if first else [resid, post]) + [pre, *tail_parts]
    operands = [*moved, band, mask, *weights]
    specs = [vmem] * (len(moved) + 2) + [hbm] * 4
    shapes = [
        ((head_rows, D), bf),
        ((head_rows, 2 * own), bf),
        ((PAST, own), bf),
        ((PAST, own), bf),
        ((rows - PAST, own), bf),
    ]
    return pl.pallas_call(
        functools.partial(local_body, layer, first, len(blocks)),
        out_shape=tuple(jax.ShapeDtypeStruct(shape, kind) for shape, kind in shapes),
        in_specs=specs,
        out_specs=(vmem,) * len(shapes),
        scratch_shapes=[
            pltpu.VMEM((4, own, D), bf),
            pltpu.SemaphoreType.DMA((4,)),
            pltpu.VMEM((head_rows, D), bf),
            pltpu.VMEM((head_rows, 128), jnp.float32),
            pltpu.VMEM((rows, 2 * own), bf),
        ],
        compiler_params=params,
        name="project_local",
    )(*operands)


def attend_body(
    query_ref,
    gate_ref,
    head_ref,
    tail_ref,
    halo_ref,
    local_ref,
    band_ref,
    docs_ref,
    behind_ref,
    mixed_ref,
    ext_ref,
):
    head_rows, own = head_ref.shape[0], query_ref.shape[1]
    rest = query_ref.shape[0]
    ext_ref[:PAST] = halo_ref[...]
    ext_ref[PAST : PAST + head_rows] = head_ref[...]
    ext_ref[PAST + head_rows :] = tail_ref[...]
    mixed_ref[rest:] = local_ref[...]
    docs = docs_ref[...]
    behind = jnp.where(lax.axis_index("sp") == 0, -1, behind_ref[...])
    docs_seen = jnp.concatenate([behind, docs], axis=1)
    for group in range(rest // GROUP):
        at = slice(group * GROUP, (group + 1) * GROUP)
        seen = slice(group * GROUP, group * GROUP + WINDOW)
        mask = doc_mask(docs[:, at], docs_seen[:, seen])
        store_group(
            mixed_ref,
            at,
            attend_group(query_ref[at], gate_ref[at], ext_ref, seen, band_ref, mask, own),
        )


def attend(layer, query, gate, head, tail, halo, local_mixed, band, docs, behind):
    own = query.shape[1]
    rows = head.shape[0] + tail.shape[0]
    operands = (query, gate, head, tail, halo, local_mixed, band, docs, behind)
    return pl.pallas_call(
        attend_body,
        out_shape=jax.ShapeDtypeStruct((rows, own), jnp.bfloat16),
        in_specs=[vmem] * len(operands),
        out_specs=vmem,
        scratch_shapes=[pltpu.VMEM((PAST + rows, 2 * own), jnp.bfloat16)],
        compiler_params=params,
        name="attend",
    )(*operands)


def out_body(layer, count, last, *refs):
    blocks = refs[:count]
    weight_ref, branch_ref = refs[count : 2 + count]
    rest = refs[2 + count :]
    if last:
        square_ref, rest = rest[0], rest[1:]
    weight_buf, mixed_ref, sem = rest
    copy = pltpu.make_async_copy(weight_ref.at[layer], weight_buf, sem)
    copy.start()
    width = blocks[0].shape[2]
    for ref, z, col in block_columns(blocks):
        mixed_ref[:, pl.ds(col, width)] = ref[z]
    copy.wait()
    branch = lax.dot_general(
        mixed_ref[...], weight_buf[...], rows_by_rows, preferred_element_type=jnp.float32
    ).astype(jnp.bfloat16)
    branch_ref[...] = branch
    if last:
        for start in range(0, branch.shape[0], GROUP):
            at = slice(start, start + GROUP)
            wide = branch_ref[at].astype(jnp.float32)
            square_ref[:, at] = turn(jnp.sum(wide * wide, axis=1, keepdims=True), 0)


def out_project(layer, blocks, weight, last):
    rows = blocks[0].shape[1]
    own = weight.shape[1]
    shapes = [jax.ShapeDtypeStruct((rows, own), jnp.bfloat16)]
    if last:
        shapes.append(jax.ShapeDtypeStruct((1, rows), jnp.float32))
    return pl.pallas_call(
        functools.partial(out_body, layer, len(blocks), last),
        out_shape=tuple(shapes),
        in_specs=[vmem] * len(blocks) + [hbm],
        out_specs=(vmem,) * len(shapes),
        scratch_shapes=[
            pltpu.VMEM((own, D), jnp.bfloat16),
            pltpu.VMEM((rows, D), jnp.bfloat16),
            pltpu.SemaphoreType.DMA,
        ],
        compiler_params=params,
        name="out_project",
    )(*blocks, weight)


def finish_body(head_ref, tail_ref, branch_ref, gain_ref, *refs):
    out_ref = refs[-1]
    total = refs[0][...]
    for ref in refs[1:-1]:
        total = total + ref[...]
    own = out_ref.shape[1]
    cols = slice(None)
    if head_ref.shape[1] != own:
        cols = pl.ds(pl.multiple_of(lax.axis_index("tp") * own, 128), own)
    gain = gain_ref[gain_ref.shape[0] - 1 :, cols]
    head_rows = head_ref.shape[0]
    for start in range(0, out_ref.shape[0], GROUP):
        at = slice(start, start + GROUP)
        inv_out = lax.rsqrt(turn(total[:, at], 1) / D + norm_eps)
        if start < head_rows:
            old = head_ref[at, cols]
        else:
            old = tail_ref[start - head_rows : start - head_rows + GROUP, cols]
        branch = branch_ref[at].astype(jnp.float32)
        out_ref[at] = (old.astype(jnp.float32) + branch * inv_out * gain).astype(jnp.bfloat16)


def finish(head, tail, branch, gain, totals):
    own = branch.shape[1]
    if own % 128:
        start = lax.axis_index("tp") * own
        head, tail, gain = [
            lax.dynamic_slice_in_dim(part, start, own, 1) for part in (head, tail, gain)
        ]
    operands = (head, tail, branch, gain, *totals)
    return pl.pallas_call(
        finish_body,
        out_shape=jax.ShapeDtypeStruct(branch.shape, jnp.bfloat16),
        in_specs=[vmem] * len(operands),
        out_specs=vmem,
        compiler_params=params,
        name="finish",
    )(*operands)


def partner(x):
    size = lax.axis_size("tp")
    return lax.ppermute(x, "tp", [(i, i ^ 1) for i in range(size)])


def gather(x):
    size = lax.axis_size("tp")
    if x.shape[1] % 128 or size % CORES:
        return (lax.all_gather(x, "tp", axis=1, tiled=True)[None],)
    lines = [list(range(core, size, CORES)) for core in range(CORES)]
    own = lax.all_gather(x, "tp", axis=0, axis_index_groups=lines)
    return own, partner(own)


def total_over_features(square):
    size = lax.axis_size("tp")
    if size % CORES or size > 8:
        return (lax.psum(square, "tp"),)
    both = square + partner(square)
    return (both,) + tuple(
        lax.ppermute(both, "tp", [(i, (i + hop) % size) for i in range(size)])
        for hop in range(CORES, size, CORES)
    )


def from_behind(block):
    size = lax.axis_size("sp")
    return lax.ppermute(block, "sp", [(i, (i + 1) % size) for i in range(size)])


def local(
    tokens,
    documents,
    pre_gain,
    query_weight,
    key_weight,
    value_weight,
    gate_weight,
    out_weight,
    position_bias,
    post_gain,
):
    rows = tokens.shape[0]
    docs = documents[None, :]
    *bands, mask = setup(position_bias, docs)
    blocks = gather(tokens)
    tail_resid = head_resid = behind = None
    for layer in range(LAYERS):
        tail_resid, normed, inv, tail = project_tail(
            layer, blocks, tail_resid, post_gain, pre_gain, (key_weight, value_weight)
        )
        if behind is None:
            tail, docs_tail = lax.optimization_barrier((tail, docs[:, rows - PAST :]))
            behind = from_behind(docs_tail)
        halo = from_behind(tail)
        head_resid, head, query, gate, local_mixed = project_local(
            layer,
            blocks,
            head_resid,
            post_gain,
            pre_gain,
            (normed, inv, tail),
            bands[layer],
            mask,
            (key_weight, value_weight, query_weight, gate_weight),
        )
        mixed = attend(
            layer, query, gate, head, tail, halo, local_mixed, bands[layer], docs, behind
        )
        last = layer + 1 == LAYERS
        result = out_project(layer, gather(mixed), out_weight, last)
        if not last:
            blocks = gather(result[0])
    branch, square = result
    return finish(head_resid, tail_resid, branch, post_gain, total_over_features(square))


def solution(mesh):
    placed = (
        P("sp", "tp"),
        P("sp"),
        P(),
        P(None, "tp", None),
        P(None, "tp", None),
        P(None, "tp", None),
        P(None, "tp", None),
        P(None, "tp", None),
        P(None, "tp", None),
        P(),
    )
    return jax.shard_map(
        local, mesh=mesh, in_specs=placed, out_specs=P("sp", "tp"), check_vma=False
    )
```

```python
import functools

import jax
import jax.numpy as jnp
from jax import lax
from jax.experimental import pallas as pl
from jax.experimental.pallas import tpu as pltpu
from jax.sharding import PartitionSpec as P

D = 2048
HD = 64
BLOCK = 64
PAST_BLOCKS = 4
LAYERS = 3
PAST = 256
CLIP = 128
GROUP = 2 * BLOCK
WINDOW = PAST + GROUP
SKEW = 512
CORES = 2
DOC_ROWS = 16
FAR = -1e30

norm_eps = 1e-06
rows_by_rows = (((1,), (1,)), ((), ()))
vmem = pl.BlockSpec(memory_space=pltpu.VMEM)
hbm = pl.BlockSpec(memory_space=pltpu.HBM)
params = pltpu.CompilerParams(vmem_limit_bytes=16 * 1024 * 1024)


def turn(vector, axis):
    size = GROUP
    diagonal = lax.broadcasted_iota(jnp.int32, (size, size), 0) == lax.broadcasted_iota(
        jnp.int32, (size, size), 1
    )
    spread = jnp.where(diagonal, jnp.broadcast_to(vector, (size, size)), jnp.zeros_like(vector))
    return jnp.sum(spread, axis=axis, keepdims=True)


def setup_body(bias_hbm, docs_ref, *refs):
    sources, refs = refs[:6], refs[6:]
    stage_ref, pre_ref, post_ref, docs_out, mask_ref, *bands = refs[:-2]
    bias_ref, sems = refs[-2:]
    bias_copy = pltpu.make_async_copy(bias_hbm, bias_ref, sems.at[6])
    bias_copy.start()
    targets = [stage_ref.at[at] for at in range(4)] + [pre_ref, post_ref]
    copies = [
        pltpu.make_async_copy(source.at[0] if at < 4 else source, target, sems.at[at])
        for at, (source, target) in enumerate(zip(sources, targets))
    ]
    for copy in copies:
        copy.start()
    docs = docs_ref[...].reshape(1, docs_ref.shape[0])
    docs_out[...] = docs
    for index in range(mask_ref.shape[0]):
        start = PAST + index * GROUP
        mask_ref[index] = doc_mask(
            docs[:, start : start + GROUP], docs[:, start - PAST : start + GROUP]
        )
    layers, heads, entries = bias_ref.shape
    row_block = lax.broadcasted_iota(jnp.int32, (GROUP, WINDOW), 0) // BLOCK
    col_block = lax.broadcasted_iota(jnp.int32, (GROUP, WINDOW), 1) // BLOCK
    allowed = (col_block >= row_block) & (col_block <= row_block + PAST_BLOCKS)
    shift = lax.broadcasted_iota(jnp.int32, (entries, SKEW), 1)
    entry = jnp.where(shift < WINDOW, jnp.minimum(PAST - shift, CLIP) + CLIP, 2 * CLIP)
    pick = (lax.broadcasted_iota(jnp.int32, (entries, SKEW), 0) == entry).astype(jnp.float32)
    bias_copy.wait()
    for layer in range(layers):
        base = lax.dot_general(
            bias_ref[layer],
            pick,
            (((1,), (0,)), ((), ())),
            precision=lax.Precision.HIGHEST,
            preferred_element_type=jnp.float32,
        )
        for head in range(heads):
            row = jnp.broadcast_to(base[head : head + 1, :], (GROUP, SKEW))
            skewed = pltpu.roll(row, 0, 1, stride=1, stride_axis=0)
            bands[layer][head] = jnp.where(allowed, skewed[:, :WINDOW], FAR)
    for copy in copies:
        copy.wait()


def doc_mask(own, seen):
    return jnp.where(turn(own, 1) == seen, 0.0, FAR)


def setup(position_bias, docs, weights, pre_gain, post_gain):
    layers, heads, _ = position_bias.shape
    rows = docs.shape[0]
    groups = (rows - PAST) // GROUP
    own = weights[0].shape[1]
    shapes = [
        jax.ShapeDtypeStruct((4, own, D), jnp.bfloat16),
        jax.ShapeDtypeStruct(pre_gain.shape, jnp.float32),
        jax.ShapeDtypeStruct(post_gain.shape, jnp.float32),
        jax.ShapeDtypeStruct((1, rows), jnp.int32),
        jax.ShapeDtypeStruct((groups, GROUP, WINDOW), jnp.float32),
        *[jax.ShapeDtypeStruct((heads, GROUP, WINDOW), jnp.float32) for _ in range(layers)],
    ]
    far = [
        pltpu.with_memory_space_constraint(a, pltpu.HBM)
        for a in (position_bias, *weights, pre_gain, post_gain)
    ]
    return pl.pallas_call(
        setup_body,
        out_shape=tuple(shapes),
        in_specs=[hbm, vmem] + [hbm] * 6,
        out_specs=(vmem,) * len(shapes),
        scratch_shapes=[
            pltpu.VMEM(position_bias.shape, jnp.float32),
            pltpu.SemaphoreType.DMA((7,)),
        ],
        compiler_params=params,
        name="setup",
    )(far[0], docs, *far[1:])


def ring_order(count):
    return [0, *range(1, count, 2), *reversed(range(2, count, 2))]


def block_columns(blocks):
    if len(blocks) == 1:
        return [(blocks[0], 0, 0)]
    core = lax.rem(lax.axis_index("tp"), CORES)
    width = blocks[0].shape[2]
    return [
        (ref, slot, pl.multiple_of((CORES * z + (core if side == 0 else 1 - core)) * width, 128))
        for side, ref in enumerate(blocks)
        for slot, z in enumerate(ring_order(ref.shape[0]))
    ]


def lane_sum(square):
    total = square[:, :128]
    for at in range(128, square.shape[1], 128):
        total = total + square[:, at : at + 128]
    return total


def update_rows(layer, blocks, offset, resid_ref, post_ref, pre_ref, resid_out, normed_ref, inv_ref):
    step = BLOCK
    placed = block_columns(blocks)
    width = blocks[0].shape[2]

    def one(index, carry):
        at = pl.ds(pl.multiple_of(index * step, step), step)
        source = pl.ds(pl.multiple_of(offset + index * step, step), step)
        if resid_ref is not None:
            total = jnp.zeros((step, 128), jnp.float32)
            for ref, z, _ in placed:
                part = ref[z, source, :].astype(jnp.float32)
                total = total + lane_sum(part * part)
            inv_out = lax.rsqrt(jnp.sum(total, axis=1, keepdims=True) / D + norm_eps)
        total = jnp.zeros((step, 128), jnp.float32)
        for ref, z, col in placed:
            cols = pl.ds(col, width)
            if resid_ref is None:
                new = ref[z, source, :]
            else:
                part = ref[z, source, :].astype(jnp.float32)
                old = resid_ref[at, cols].astype(jnp.float32)
                new = (old + part * inv_out * post_ref[layer - 1 : layer, cols]).astype(jnp.bfloat16)
            resid_out[at, cols] = new
            wide = new.astype(jnp.float32)
            total = total + lane_sum(wide * wide)
            normed_ref[at, cols] = (wide * pre_ref[layer : layer + 1, cols]).astype(jnp.bfloat16)
        inv_in = lax.rsqrt(jnp.sum(total, axis=1, keepdims=True) / D + norm_eps)
        inv_ref[at, :] = jnp.broadcast_to(inv_in, (step, 128))
        return carry

    lax.fori_loop(0, resid_out.shape[0] // step, one, 0)


def scaled_product(normed_ref, inv_ref, weight):
    product = lax.dot_general(
        normed_ref[...], weight, rows_by_rows, preferred_element_type=jnp.float32
    )
    return (product * inv_ref[:, :1]).astype(jnp.bfloat16)


def weight_of(layer, weights, at):
    return weights[0][at] if layer == 0 else weights[at][layer]


def piece_body(layer, count, offset, *refs):
    blocks, refs = refs[:count], refs[count:]
    resid_ref = post_ref = docs_ref = None
    if layer:
        (resid_ref, post_ref), refs = refs[:2], refs[2:]
    else:
        docs_ref, refs = refs[0], refs[1:]
    pre_ref, weights = refs[0], refs[1:-4]
    resid_out, normed_ref, inv_ref, kv_ref = refs[-4:]
    update_rows(
        layer, blocks, offset, resid_ref, post_ref, pre_ref, resid_out, normed_ref, inv_ref
    )
    own = kv_ref.shape[1] // 2
    for at in range(2):
        kv_ref[:GROUP, at * own : (at + 1) * own] = scaled_product(
            normed_ref, inv_ref, weight_of(layer, weights, at)
        )
    if layer == 0:
        docs = docs_ref[:, offset : offset + GROUP].astype(jnp.float32)
        kv_ref[GROUP:, :GROUP] = jnp.broadcast_to(docs, (DOC_ROWS, GROUP)).astype(jnp.bfloat16)


def project_piece(layer, blocks, offset, resid, docs, post, pre, weights):
    own = weights[0].shape[1]
    bf = jnp.bfloat16
    extra = [resid, post] if layer else [docs]
    operands = [*blocks, *extra, pre, *weights]
    kv_rows = GROUP if layer else GROUP + DOC_ROWS
    return pl.pallas_call(
        functools.partial(piece_body, layer, len(blocks), offset),
        out_shape=(
            jax.ShapeDtypeStruct((GROUP, D), bf),
            jax.ShapeDtypeStruct((GROUP, D), bf),
            jax.ShapeDtypeStruct((GROUP, 128), jnp.float32),
            jax.ShapeDtypeStruct((kv_rows, 2 * own), bf),
        ),
        in_specs=[vmem] * len(operands),
        out_specs=(vmem,) * 4,
        compiler_params=params,
        name="project_piece",
    )(*operands)


def attend_group(query, gate, ext_ref, seen, band_ref, mask, own):
    span = min(own, 128)
    lane = lax.broadcasted_iota(jnp.int32, (GROUP, span), 1) // HD
    results = []
    for start in range(0, own, span):
        cols = slice(start, start + span)
        keys = ext_ref[seen, cols]
        values = ext_ref[seen, own + start : own + start + span]
        result = None
        for sub in range(span // HD):
            picked = jnp.where(lane == sub, query[:, cols], jnp.zeros((), query.dtype))
            scores = lax.dot_general(
                picked, keys, rows_by_rows, preferred_element_type=jnp.float32
            )
            scores = scores + band_ref[start // HD + sub] + mask
            lifted = jnp.exp(scores - jnp.max(scores, axis=1, keepdims=True))
            total = jnp.sum(lifted, axis=1, keepdims=True)
            part = jnp.dot(lifted.astype(jnp.bfloat16), values, preferred_element_type=jnp.float32)
            part = part / total
            result = part if result is None else jnp.where(lane == sub, part, result)
        wide = gate[:, cols].astype(jnp.float32)
        results.append((result * (wide / (1.0 + jnp.exp(-wide)))).astype(jnp.bfloat16))
    return results


def store_group(mixed_ref, at, results):
    start = 0
    for result in results:
        mixed_ref[at, start : start + result.shape[1]] = result
        start = start + result.shape[1]


def local_body(layer, count, *refs):
    blocks, refs = refs[:count], refs[count:]
    resid_ref = post_ref = None
    if layer:
        (resid_ref, post_ref), refs = refs[:2], refs[2:]
    pieces = PAST // GROUP
    pre_ref, refs = refs[0], refs[1:]
    piece_normed, piece_inv, piece_kv = [refs[at * pieces : (at + 1) * pieces] for at in range(3)]
    refs = refs[3 * pieces :]
    band_ref, mask_ref, weights = refs[0], refs[1], refs[2:-8]
    resid_out, head_ref, query_out, gate_out, mixed_ref = refs[-8:-3]
    normed_ref, inv_ref, ext_ref = refs[-3:]
    head_rows = resid_out.shape[0]
    head_at = pl.ds(0, head_rows)
    for index in range(pieces):
        at = pl.ds(head_rows + index * GROUP, GROUP)
        normed_ref[at] = piece_normed[index][...]
        inv_ref[at] = piece_inv[index][...]
        ext_ref[at] = piece_kv[index][:GROUP]
    update_rows(
        layer,
        blocks,
        0,
        resid_ref,
        post_ref,
        pre_ref,
        resid_out,
        normed_ref.at[head_at],
        inv_ref.at[head_at],
    )
    rest, own = query_out.shape
    local = []
    for at in range(4):
        weight = weight_of(layer, weights, at)
        if at < 2:
            head = scaled_product(normed_ref.at[head_at], inv_ref.at[head_at], weight)
            head_ref[:, at * own : (at + 1) * own] = head
            continue
        product = scaled_product(normed_ref, inv_ref, weight)
        if at == 2:
            product = product * jnp.bfloat16(HD ** (-0.5))
        target = query_out if at == 2 else gate_out
        target[...] = product[:rest]
        local.append(product[rest:])
    ext_ref[head_at] = head_ref[...]
    for index in range(mask_ref.shape[0]):
        at = slice(index * GROUP, (index + 1) * GROUP)
        seen = slice(index * GROUP, index * GROUP + WINDOW)
        results = attend_group(
            local[0][at], local[1][at], ext_ref, seen, band_ref, mask_ref[index], own
        )
        store_group(mixed_ref, at, results)


def project_local(layer, blocks, resid, post, pre, pieces, band, mask, weights):
    rows = blocks[0].shape[1]
    own = weights[0].shape[1]
    head_rows = rows - PAST
    bf = jnp.bfloat16
    moved = [*blocks] + ([resid, post] if layer else []) + [pre, *pieces, band, mask]
    shapes = [
        (head_rows, D),
        (head_rows, 2 * own),
        (PAST, own),
        (PAST, own),
        (rows - PAST, own),
    ]
    return pl.pallas_call(
        functools.partial(local_body, layer, len(blocks)),
        out_shape=tuple(jax.ShapeDtypeStruct(shape, bf) for shape in shapes),
        in_specs=[vmem] * (len(moved) + len(weights)),
        out_specs=(vmem,) * len(shapes),
        scratch_shapes=[
            pltpu.VMEM((rows, D), bf),
            pltpu.VMEM((rows, 128), jnp.float32),
            pltpu.VMEM((rows, 2 * own), bf),
        ],
        compiler_params=params,
        name="project_local",
    )(*moved, *weights)


def attend_body(layer, *refs):
    pieces = PAST // GROUP
    piece_refs, halo_refs, refs = refs[:pieces], refs[pieces : 2 * pieces], refs[2 * pieces :]
    query_ref, gate_ref, head_ref, local_ref, band_ref, docs_ref = refs[:6]
    if layer:
        behind_ref, mixed_ref, ext_ref = refs[6:]
    else:
        mixed_ref, behind_ref, ext_ref = refs[6:]
        first = lax.axis_index("sp") == 0
        for index in range(pieces):
            told = halo_refs[index][GROUP : GROUP + DOC_ROWS, :GROUP].astype(jnp.float32)[:1]
            behind_ref[:, index * GROUP : (index + 1) * GROUP] = jnp.where(
                first, -1, told.astype(jnp.int32)
            )
    head_rows, own = head_ref.shape[0], query_ref.shape[1]
    rest = query_ref.shape[0]
    for index in range(pieces):
        ext_ref[index * GROUP : (index + 1) * GROUP] = halo_refs[index][:GROUP]
        start = PAST + head_rows + index * GROUP
        ext_ref[start : start + GROUP] = piece_refs[index][:GROUP]
    ext_ref[PAST : PAST + head_rows] = head_ref[...]
    mixed_ref[rest:] = local_ref[...]
    docs = docs_ref[...]
    docs_seen = jnp.concatenate([behind_ref[...], docs], axis=1)
    for group in range(rest // GROUP):
        at = slice(group * GROUP, (group + 1) * GROUP)
        seen = slice(group * GROUP, group * GROUP + WINDOW)
        mask = doc_mask(docs[:, at], docs_seen[:, seen])
        store_group(
            mixed_ref,
            at,
            attend_group(query_ref[at], gate_ref[at], ext_ref, seen, band_ref, mask, own),
        )


def attend(layer, pieces, halos, query, gate, head, local_mixed, band, docs, behind):
    own = query.shape[1]
    rows = head.shape[0] + PAST
    operands = [*pieces, *halos, query, gate, head, local_mixed, band, docs]
    shapes = [jax.ShapeDtypeStruct((rows, own), jnp.bfloat16)]
    if layer:
        operands.append(behind)
    else:
        shapes.append(jax.ShapeDtypeStruct((1, PAST), jnp.int32))
    return pl.pallas_call(
        functools.partial(attend_body, layer),
        out_shape=tuple(shapes),
        in_specs=[vmem] * len(operands),
        out_specs=(vmem,) * len(shapes),
        scratch_shapes=[pltpu.VMEM((PAST + rows, 2 * own), jnp.bfloat16)],
        compiler_params=params,
        name="attend",
    )(*operands)


def out_body(layer, count, last, *refs):
    blocks = refs[:count]
    weight_ref, branch_ref = refs[count : 2 + count]
    rest = refs[2 + count :]
    if last:
        square_ref, rest = rest[0], rest[1:]
    width = blocks[0].shape[2]
    mixed_ref = rest[0]
    for ref, z, col in block_columns(blocks):
        mixed_ref[:, pl.ds(col, width)] = ref[z]
    branch = lax.dot_general(
        mixed_ref[...], weight_ref[layer], rows_by_rows, preferred_element_type=jnp.float32
    ).astype(jnp.bfloat16)
    branch_ref[...] = branch
    if last:
        for start in range(0, branch.shape[0], GROUP):
            at = slice(start, start + GROUP)
            wide = branch_ref[at].astype(jnp.float32)
            square_ref[:, at] = turn(jnp.sum(wide * wide, axis=1, keepdims=True), 0)


def out_project(layer, blocks, weight, last):
    rows = blocks[0].shape[1]
    own = weight.shape[1]
    shapes = [jax.ShapeDtypeStruct((rows, own), jnp.bfloat16)]
    if last:
        shapes.append(jax.ShapeDtypeStruct((1, rows), jnp.float32))
    return pl.pallas_call(
        functools.partial(out_body, layer, len(blocks), last),
        out_shape=tuple(shapes),
        in_specs=[vmem] * (len(blocks) + 1),
        out_specs=(vmem,) * len(shapes),
        scratch_shapes=[pltpu.VMEM((rows, D), jnp.bfloat16)],
        compiler_params=params,
        name="out_project",
    )(*blocks, weight)


def finish_body(count, *refs):
    resid_refs, (branch_ref, gain_ref), refs = refs[:count], refs[count : count + 2], refs[count + 2 :]
    out_ref = refs[-1]
    total = refs[0][...]
    for ref in refs[1:-1]:
        total = total + ref[...]
    own = out_ref.shape[1]
    cols = slice(None)
    if gain_ref.shape[1] != own:
        cols = pl.ds(pl.multiple_of(lax.axis_index("tp") * own, 128), own)
    gain = gain_ref[gain_ref.shape[0] - 1 :, cols]
    start = 0
    for ref in resid_refs:
        for base in range(0, ref.shape[0], GROUP):
            at = slice(start, start + GROUP)
            inv_out = lax.rsqrt(turn(total[:, at], 1) / D + norm_eps)
            old = ref[base : base + GROUP, cols].astype(jnp.float32)
            branch = branch_ref[at].astype(jnp.float32)
            out_ref[at] = (old + branch * inv_out * gain).astype(jnp.bfloat16)
            start = start + GROUP


def finish(resids, branch, gain, totals):
    own = branch.shape[1]
    if own % 128:
        start = lax.axis_index("tp") * own
        *resids, gain = [
            lax.dynamic_slice_in_dim(part, start, own, 1) for part in (*resids, gain)
        ]
    operands = (*resids, branch, gain, *totals)
    return pl.pallas_call(
        functools.partial(finish_body, len(resids)),
        out_shape=jax.ShapeDtypeStruct(branch.shape, jnp.bfloat16),
        in_specs=[vmem] * len(operands),
        out_specs=vmem,
        compiler_params=params,
        name="finish",
    )(*operands)


def partner(x):
    size = lax.axis_size("tp")
    return lax.ppermute(x, "tp", [(i, i ^ 1) for i in range(size)])


def gather(x):
    size = lax.axis_size("tp")
    if x.shape[1] % 128 or size % CORES:
        return lax.all_gather(x, "tp", axis=1, tiled=True)[None]
    order = ring_order(size // CORES)
    lines = [[CORES * z + core for z in order] for core in range(CORES)]
    return lax.all_gather(x, "tp", axis=0, axis_index_groups=lines)


def swapped(own):
    return (own, partner(own)) if own.shape[2] < D else (own,)


def total_over_features(square):
    size = lax.axis_size("tp")
    if size % CORES or size > 8:
        return (lax.psum(square, "tp"),)
    both = square + partner(square)
    return (both,) + tuple(
        lax.ppermute(both, "tp", [(i, (i + hop) % size) for i in range(size)])
        for hop in range(CORES, size, CORES)
    )


def from_behind(block):
    size = lax.axis_size("sp")
    return lax.ppermute(block, "sp", [(i, (i + 1) % size) for i in range(size)])


def local(
    tokens,
    documents,
    pre_gain,
    query_weight,
    key_weight,
    value_weight,
    gate_weight,
    out_weight,
    position_bias,
    post_gain,
):
    rows = tokens.shape[0]
    starts = range(rows - PAST, rows, GROUP)
    weights = (key_weight, value_weight, query_weight, gate_weight)
    gathered, documents = lax.optimization_barrier((gather(tokens), documents))
    blocks = swapped(gathered)
    stage, pre, post, docs, mask, *bands = setup(
        position_bias, documents, weights, pre_gain, post_gain
    )
    resids = [None] * len(starts)
    head_resid = behind = None
    for layer in range(LAYERS):
        used = weights if layer else (stage,)
        made = [None] * len(starts)
        halos = [None] * len(starts)
        for index in reversed(range(len(starts))):
            made[index] = project_piece(
                layer,
                blocks,
                starts[index],
                resids[index],
                docs,
                post,
                pre,
                used[:2],
            )
            halos[index] = from_behind(made[index][3])
        resids, normed, inv, pieces = [list(part) for part in zip(*made)]
        head_resid, head, query, gate, local_mixed = project_local(
            layer,
            blocks,
            head_resid,
            post,
            pre,
            (*normed, *inv, *pieces),
            bands[layer],
            mask,
            used,
        )
        mixed, *told = attend(
            layer, pieces, halos, query, gate, head, local_mixed, bands[layer], docs, behind
        )
        behind = told[0] if told else behind
        last = layer + 1 == LAYERS
        result = out_project(layer, swapped(gather(mixed)), out_weight, last)
        if not last:
            blocks = swapped(gather(result[0]))
    branch, square = result
    return finish((head_resid, *resids), branch, post, total_over_features(square))


def solution(mesh):
    placed = (
        P("sp", "tp"),
        P("sp"),
        P(),
        P(None, "tp", None),
        P(None, "tp", None),
        P(None, "tp", None),
        P(None, "tp", None),
        P(None, "tp", None),
        P(None, "tp", None),
        P(),
    )
    return jax.shard_map(
        local, mesh=mesh, in_specs=placed, out_specs=P("sp", "tp"), check_vma=False
    )
```

```python
import functools

import jax
import jax.numpy as jnp
from jax import lax
from jax.experimental import pallas as pl
from jax.experimental.pallas import tpu as pltpu
from jax.sharding import PartitionSpec as P

D = 2048
HD = 64
BLOCK = 64
PAST_BLOCKS = 4
LAYERS = 3
PAST = 256
CLIP = 128
GROUP = 2 * BLOCK
WINDOW = PAST + GROUP
SKEW = 512
CORES = 2
DOC_ROWS = 16
HALF = GROUP // CORES
FAR = -1e30

norm_eps = 1e-06
rows_by_rows = (((1,), (1,)), ((), ()))
vmem = pl.BlockSpec(memory_space=pltpu.VMEM)
hbm = pl.BlockSpec(memory_space=pltpu.HBM)
params = pltpu.CompilerParams(vmem_limit_bytes=16 * 1024 * 1024)


def turn(vector, axis):
    size = max(vector.shape)
    diagonal = lax.broadcasted_iota(jnp.int32, (size, size), 0) == lax.broadcasted_iota(
        jnp.int32, (size, size), 1
    )
    spread = jnp.where(diagonal, jnp.broadcast_to(vector, (size, size)), jnp.zeros_like(vector))
    return jnp.sum(spread, axis=axis, keepdims=True)


def setup_body(bias_hbm, docs_hbm, *refs):
    sources, refs = refs[:6], refs[6:]
    stage_ref, pre_ref, post_ref, docs_out, mask_ref, *bands = refs[:-3]
    bias_ref, docs_ref, sems = refs[-3:]
    bias_copy = pltpu.make_async_copy(bias_hbm, bias_ref, sems.at[6])
    bias_copy.start()
    docs_copy = pltpu.make_async_copy(docs_hbm, docs_ref, sems.at[7])
    docs_copy.start()
    targets = [stage_ref.at[at] for at in range(4)] + [pre_ref, post_ref]
    copies = [
        pltpu.make_async_copy(source.at[0] if at < 4 else source, target, sems.at[at])
        for at, (source, target) in enumerate(zip(sources, targets))
    ]
    for copy in copies:
        copy.start()
    docs_copy.wait()
    docs = docs_ref[...].reshape(1, docs_ref.shape[0])
    docs_out[...] = docs
    for index in range(mask_ref.shape[0]):
        start = PAST + index * GROUP
        mask_ref[index] = doc_mask(
            docs[:, start : start + GROUP], docs[:, start - PAST : start + GROUP]
        )
    layers, heads, entries = bias_ref.shape
    row_block = lax.broadcasted_iota(jnp.int32, (GROUP, WINDOW), 0) // BLOCK
    col_block = lax.broadcasted_iota(jnp.int32, (GROUP, WINDOW), 1) // BLOCK
    allowed = (col_block >= row_block) & (col_block <= row_block + PAST_BLOCKS)
    shift = lax.broadcasted_iota(jnp.int32, (entries, SKEW), 1)
    entry = jnp.where(shift < WINDOW, jnp.minimum(PAST - shift, CLIP) + CLIP, 2 * CLIP)
    pick = (lax.broadcasted_iota(jnp.int32, (entries, SKEW), 0) == entry).astype(jnp.float32)
    bias_copy.wait()
    for layer in range(layers):
        base = lax.dot_general(
            bias_ref[layer],
            pick,
            (((1,), (0,)), ((), ())),
            precision=lax.Precision.HIGHEST,
            preferred_element_type=jnp.float32,
        )
        for head in range(heads):
            row = jnp.broadcast_to(base[head : head + 1, :], (GROUP, SKEW))
            skewed = pltpu.roll(row, 0, 1, stride=1, stride_axis=0)
            bands[layer][head] = jnp.where(allowed, skewed[:, :WINDOW], FAR)
    for copy in copies:
        copy.wait()


def doc_mask(own, seen):
    return jnp.where(turn(own, 1) == seen, 0.0, FAR)


def setup(position_bias, docs, weights, pre_gain, post_gain):
    layers, heads, _ = position_bias.shape
    rows = docs.shape[0]
    groups = (rows - PAST) // GROUP
    own = weights[0].shape[1]
    shapes = [
        jax.ShapeDtypeStruct((4, own, D), jnp.bfloat16),
        jax.ShapeDtypeStruct(pre_gain.shape, jnp.float32),
        jax.ShapeDtypeStruct(post_gain.shape, jnp.float32),
        jax.ShapeDtypeStruct((1, rows), jnp.int32),
        jax.ShapeDtypeStruct((groups, GROUP, WINDOW), jnp.float32),
        *[jax.ShapeDtypeStruct((heads, GROUP, WINDOW), jnp.float32) for _ in range(layers)],
    ]
    far = [
        pltpu.with_memory_space_constraint(a, pltpu.HBM)
        for a in (position_bias, docs, *weights, pre_gain, post_gain)
    ]
    return pl.pallas_call(
        setup_body,
        out_shape=tuple(shapes),
        in_specs=[hbm] * 8,
        out_specs=(vmem,) * len(shapes),
        scratch_shapes=[
            pltpu.VMEM(position_bias.shape, jnp.float32),
            pltpu.VMEM(docs.shape, jnp.int32),
            pltpu.SemaphoreType.DMA((8,)),
        ],
        compiler_params=params,
        name="setup",
    )(*far)


def ring_order(count):
    return [0, *range(1, count, 2), *reversed(range(2, count, 2))]


def block_columns(blocks):
    if len(blocks) == 1:
        return [(blocks[0], 0, 0)]
    core = lax.rem(lax.axis_index("tp"), CORES)
    width = blocks[0].shape[2]
    return [
        (ref, slot, pl.multiple_of((CORES * z + (core if side == 0 else 1 - core)) * width, 128))
        for side, ref in enumerate(blocks)
        for slot, z in enumerate(ring_order(ref.shape[0]))
    ]


def lane_sum(square):
    total = square[:, :128]
    for at in range(128, square.shape[1], 128):
        total = total + square[:, at : at + 128]
    return total


def core_at():
    return lax.rem(lax.axis_index("tp"), CORES)


def half_rows(mine):
    at = core_at() if mine else 1 - core_at()
    return pl.ds(pl.multiple_of(at * HALF, HALF), HALF)


def update_half(layer, placed, source, resid_ref, post_ref, pre_ref, resid_out, normed_out):
    if layer:
        total = jnp.zeros((HALF, 128), jnp.float32)
        for ref, slot, _ in placed:
            part = ref[slot, source, :].astype(jnp.float32)
            total = total + lane_sum(part * part)
        inv_out = lax.rsqrt(jnp.sum(total, axis=1, keepdims=True) / D + norm_eps)
    total = jnp.zeros((HALF, 128), jnp.float32)
    for ref, slot, col in placed:
        cols = pl.ds(col, ref.shape[2])
        new = ref[slot, source, :]
        if layer:
            part = new.astype(jnp.float32)
            old = resid_ref[:, cols].astype(jnp.float32)
            new = (old + part * inv_out * post_ref[layer - 1 : layer, cols]).astype(jnp.bfloat16)
        resid_out[:, cols] = new
        wide = new.astype(jnp.float32)
        total = total + lane_sum(wide * wide)
    inv_in = lax.rsqrt(jnp.sum(total, axis=1, keepdims=True) / D + norm_eps)
    for ref, _, col in placed:
        cols = pl.ds(col, ref.shape[2])
        wide = resid_out[:, cols].astype(jnp.float32)
        normed_out[:, cols] = (wide * inv_in * pre_ref[layer : layer + 1, cols]).astype(jnp.bfloat16)


def norm_group(blocks, offset, pre_ref, resid_half, rows_ref, normed_ref):
    placed = block_columns(blocks)
    for half in range(CORES):
        at = pl.ds(half * HALF, HALF)
        update_half(
            0,
            placed,
            pl.ds(offset + half * HALF, HALF),
            None,
            None,
            pre_ref,
            rows_ref.at[at],
            normed_ref.at[at],
        )
    resid_half[...] = rows_ref[half_rows(True), :]


def chip_columns(ref):
    width = ref.shape[2]
    return [(ref, slot, z * width) for slot, z in enumerate(ring_order(ref.shape[0]))]


def update_body(layer, groups, blocks_ref, post_ref, pre_ref, *refs):
    count = len(groups)
    olds, news, normed = [refs[at * count : (at + 1) * count] for at in range(3)]
    placed = chip_columns(blocks_ref)
    for index, group in enumerate(groups):
        update_half(
            layer,
            placed,
            pl.ds(group * HALF, HALF),
            olds[index],
            post_ref,
            pre_ref,
            news[index],
            normed[index],
        )


def update(layer, groups, blocks, post, pre, olds):
    shape = jax.ShapeDtypeStruct((HALF, D), jnp.bfloat16)
    operands = (blocks, post, pre, *olds)
    made = pl.pallas_call(
        functools.partial(update_body, layer, groups),
        out_shape=(shape,) * (2 * len(groups)),
        in_specs=[vmem] * len(operands),
        out_specs=(vmem,) * (2 * len(groups)),
        compiler_params=params,
        name="update",
    )(*operands)
    return made[: len(groups)], made[len(groups) :]


def product(rows_ref, weight):
    return lax.dot_general(
        rows_ref[...], weight, rows_by_rows, preferred_element_type=jnp.float32
    ).astype(jnp.bfloat16)


def weight_of(layer, weights, at):
    return weights[0][at] if layer == 0 else weights[at][layer]


def first_piece_body(offset, count, *refs):
    blocks, (docs_ref, pre_ref, weights_ref) = refs[:count], refs[count : count + 3]
    resid_half, normed_ref, kv_ref, rows_ref = refs[count + 3 :]
    norm_group(blocks, offset, pre_ref, resid_half, rows_ref, normed_ref)
    own = kv_ref.shape[1] // 2
    for at in range(2):
        kv_ref[:GROUP, at * own : (at + 1) * own] = product(normed_ref, weights_ref[at])
    docs = docs_ref[:, offset : offset + GROUP].astype(jnp.float32)
    kv_ref[GROUP:, :GROUP] = jnp.broadcast_to(docs, (DOC_ROWS, GROUP)).astype(jnp.bfloat16)


def first_piece(blocks, offset, docs, pre, stage):
    own = stage.shape[1]
    bf = jnp.bfloat16
    operands = (*blocks, docs, pre, stage)
    return pl.pallas_call(
        functools.partial(first_piece_body, offset, len(blocks)),
        out_shape=(
            jax.ShapeDtypeStruct((HALF, D), bf),
            jax.ShapeDtypeStruct((GROUP, D), bf),
            jax.ShapeDtypeStruct((GROUP + DOC_ROWS, 2 * own), bf),
        ),
        in_specs=[vmem] * len(operands),
        out_specs=(vmem,) * 3,
        scratch_shapes=[pltpu.VMEM((GROUP, D), bf)],
        compiler_params=params,
        name="first_piece",
    )(*operands)


def piece_body(layer, mine_ref, other_ref, key_ref, value_ref, kv_ref, rows_ref):
    rows_ref[half_rows(True), :] = mine_ref[...]
    rows_ref[half_rows(False), :] = other_ref[...]
    own = kv_ref.shape[1] // 2
    kv_ref[:, :own] = product(rows_ref, key_ref[layer])
    kv_ref[:, own:] = product(rows_ref, value_ref[layer])


def project_piece(layer, mine, other, key_weight, value_weight):
    own = key_weight.shape[1]
    return pl.pallas_call(
        functools.partial(piece_body, layer),
        out_shape=jax.ShapeDtypeStruct((GROUP, 2 * own), jnp.bfloat16),
        in_specs=[vmem] * 4,
        out_specs=vmem,
        scratch_shapes=[pltpu.VMEM((GROUP, D), jnp.bfloat16)],
        compiler_params=params,
        name="project_piece",
    )(mine, other, key_weight, value_weight)


def attend_group(query, gate, ext_ref, seen, band_ref, mask, own):
    span = min(own, 128)
    lane = lax.broadcasted_iota(jnp.int32, (GROUP, span), 1) // HD
    results = []
    for start in range(0, own, span):
        cols = slice(start, start + span)
        keys = ext_ref[seen, cols]
        values = ext_ref[seen, own + start : own + start + span]
        result = None
        for sub in range(span // HD):
            picked = jnp.where(lane == sub, query[:, cols], jnp.zeros((), query.dtype))
            scores = lax.dot_general(
                picked, keys, rows_by_rows, preferred_element_type=jnp.float32
            )
            scores = scores + band_ref[start // HD + sub] + mask
            lifted = jnp.exp(scores - jnp.max(scores, axis=1, keepdims=True))
            total = jnp.sum(lifted, axis=1, keepdims=True)
            part = jnp.dot(lifted.astype(jnp.bfloat16), values, preferred_element_type=jnp.float32)
            part = part / total
            result = part if result is None else jnp.where(lane == sub, part, result)
        wide = gate[:, cols].astype(jnp.float32)
        results.append((result * (wide / (1.0 + jnp.exp(-wide)))).astype(jnp.bfloat16))
    return results


def store_group(mixed_ref, at, results):
    start = 0
    for result in results:
        mixed_ref[at, start : start + result.shape[1]] = result
        start = start + result.shape[1]


def local_body(layer, count, *refs):
    pieces = PAST // GROUP
    if layer == 0:
        blocks, pre_ref, refs = refs[:count], refs[count], refs[count + 1 :]
        piece_normed, refs = refs[:pieces], refs[pieces:]
    else:
        mine, other, refs = refs[:count], refs[count : 2 * count], refs[2 * count :]
    piece_kv, refs = refs[:pieces], refs[pieces:]
    band_ref, mask_ref, refs = refs[0], refs[1], refs[2:]
    if layer == 0:
        weights, refs = refs[:1], refs[1:]
        resid_half, refs = refs[0], refs[1:]
    else:
        weights, refs = refs[:4], refs[4:]
    head_ref, query_out, gate_out, mixed_ref, normed_ref, ext_ref = refs[:6]
    head_rows = head_ref.shape[0]
    head_at = pl.ds(0, head_rows)
    for index in range(pieces):
        at = pl.ds(head_rows + index * GROUP, GROUP)
        ext_ref[at] = piece_kv[index][:GROUP]
        if layer == 0:
            normed_ref[at] = piece_normed[index][...]
    if layer == 0:
        norm_group(blocks, 0, pre_ref, resid_half, refs[6], normed_ref.at[head_at])
    else:
        for group in range(count):
            rows_ref = normed_ref.at[pl.ds(group * GROUP, GROUP)]
            rows_ref[half_rows(True), :] = mine[group][...]
            rows_ref[half_rows(False), :] = other[group][...]
    rest, own = query_out.shape
    local = []
    for at in range(4):
        weight = weight_of(layer, weights, at)
        if at < 2:
            head_ref[:, at * own : (at + 1) * own] = product(normed_ref.at[head_at], weight)
            continue
        result = product(normed_ref, weight)
        if at == 2:
            result = result * jnp.bfloat16(HD ** (-0.5))
        target = query_out if at == 2 else gate_out
        target[...] = result[:rest]
        local.append(result[rest:])
    ext_ref[head_at] = head_ref[...]
    for index in range(mask_ref.shape[0]):
        at = slice(index * GROUP, (index + 1) * GROUP)
        seen = slice(index * GROUP, index * GROUP + WINDOW)
        results = attend_group(
            local[0][at], local[1][at], ext_ref, seen, band_ref, mask_ref[index], own
        )
        store_group(mixed_ref, at, results)


def project_local(layer, rows, sources, pieces, band, mask, weights):
    own = weights[0].shape[1]
    head_rows = rows - PAST
    bf = jnp.bfloat16
    operands = [*sources, *pieces, band, mask, *weights]
    count = len(sources) // 2 if layer else len(sources) - 1 - len(pieces)
    shapes = [] if layer else [(HALF, D)]
    shapes = shapes + [
        (head_rows, 2 * own),
        (PAST, own),
        (PAST, own),
        (rows - PAST, own),
    ]
    scratch = [pltpu.VMEM((rows, D), bf), pltpu.VMEM((rows, 2 * own), bf)]
    if layer == 0:
        scratch.append(pltpu.VMEM((head_rows, D), bf))
    return pl.pallas_call(
        functools.partial(local_body, layer, count),
        out_shape=tuple(jax.ShapeDtypeStruct(shape, bf) for shape in shapes),
        in_specs=[vmem] * len(operands),
        out_specs=(vmem,) * len(shapes),
        scratch_shapes=scratch,
        compiler_params=params,
        name="project_local",
    )(*operands)


def attend_body(layer, group, done, *refs):
    halo_count = PAST // GROUP - group
    chunks, refs = refs[: WINDOW // GROUP], refs[WINDOW // GROUP :]
    query_ref, gate_ref, band_ref, docs_ref, refs = *refs[:4], refs[4:]
    known = halo_count if layer else halo_count - 1
    told_refs, refs = refs[:known], refs[known:]
    done_refs, refs = refs[:done], refs[done:]
    keep_ref = give_ref = None
    if group == 0:
        (keep_ref, give_ref), refs = refs[:2], refs[2:]
    else:
        mixed_ref, refs = refs[0], refs[1:]
    told = [ref[...] for ref in told_refs]
    if layer == 0:
        arrived = chunks[0][GROUP : GROUP + DOC_ROWS, :GROUP].astype(jnp.float32)[:1]
        arrived = jnp.where(lax.axis_index("sp") == 0, -1, arrived.astype(jnp.int32))
        refs[0][...] = arrived
        told = [arrived, *told]
        refs = refs[1:]
    ext_ref = refs[0]
    if group == 0:
        mixed_ref = refs[1]
    for index, chunk in enumerate(chunks):
        ext_ref[index * GROUP : (index + 1) * GROUP] = chunk[:GROUP]
    at = slice(group * GROUP, (group + 1) * GROUP)
    docs = docs_ref[...]
    mask = doc_mask(docs[:, at], jnp.concatenate([*told, docs[:, : at.stop]], axis=1))
    own = query_ref.shape[1]
    results = attend_group(
        query_ref[at], gate_ref[at], ext_ref, slice(None), band_ref, mask, own
    )
    store_group(mixed_ref, slice(None), results)
    if group == 0:
        for index, ref in enumerate((mixed_ref, *done_refs)):
            at = slice(index * HALF, (index + 1) * HALF)
            keep_ref[at] = ref[half_rows(True), :]
            give_ref[at] = ref[half_rows(False), :]


def attend(layer, group, chunks, query, gate, band, docs, told, done):
    own = query.shape[1]
    bf = jnp.bfloat16
    operands = (*chunks, query, gate, band, docs, *told, *done)
    shapes = [jax.ShapeDtypeStruct((GROUP, own), bf)]
    scratch = [pltpu.VMEM((WINDOW, 2 * own), bf)]
    if group == 0:
        shapes = [jax.ShapeDtypeStruct(((1 + len(done)) * HALF, own), bf)] * CORES
        scratch.append(pltpu.VMEM((GROUP, own), bf))
    if layer == 0:
        shapes.append(jax.ShapeDtypeStruct((1, GROUP), jnp.int32))
    return pl.pallas_call(
        functools.partial(attend_body, layer, group, len(done)),
        out_shape=tuple(shapes),
        in_specs=[vmem] * len(operands),
        out_specs=(vmem,) * len(shapes),
        scratch_shapes=scratch,
        compiler_params=params,
        name="attend",
    )(*operands)


def by_core(action):
    for core in range(CORES):
        pl.when(core_at() == core)(functools.partial(action, core))


def join_body(keep_ref, got_ref, out_ref):
    own = keep_ref.shape[1]

    def place(core):
        out_ref[:, core * own : (core + 1) * own] = keep_ref[...]
        out_ref[:, (1 - core) * own : (2 - core) * own] = got_ref[...]

    by_core(place)


def join(keep, got):
    rows, own = keep.shape
    return pl.pallas_call(
        join_body,
        out_shape=jax.ShapeDtypeStruct((rows, CORES * own), keep.dtype),
        in_specs=[vmem] * 2,
        out_specs=vmem,
        compiler_params=params,
        name="join",
    )(keep, got)


def out_body(layer, last, blocks_ref, mine_ref, other_ref, branch_ref, *rest):
    mixed_ref = rest[-1]
    width = blocks_ref.shape[2]
    own = width // CORES
    for ref, slot, col in chip_columns(blocks_ref):
        mixed_ref[:, col : col + width] = ref[slot]
    mine = product(mixed_ref, mine_ref[layer])
    other = product(mixed_ref, other_ref[layer])

    def place(core):
        branch_ref[:, core * own : (core + 1) * own] = mine
        branch_ref[:, (1 - core) * own : (2 - core) * own] = other

    by_core(place)
    if last:
        square_ref = rest[0]
        wide = mine.astype(jnp.float32)
        total = jnp.sum(wide * wide, axis=1, keepdims=True)
        wide = other.astype(jnp.float32)
        total = total + jnp.sum(wide * wide, axis=1, keepdims=True)
        for start in range(0, total.shape[0], HALF):
            at = slice(start, start + HALF)
            square_ref[:, at] = turn(total[at], 0)


def out_project(layer, blocks, mine, other, last):
    rows, width = blocks.shape[1:]
    shapes = [jax.ShapeDtypeStruct((rows, width), jnp.bfloat16)]
    if last:
        shapes.append(jax.ShapeDtypeStruct((1, rows), jnp.float32))
    return pl.pallas_call(
        functools.partial(out_body, layer, last),
        out_shape=tuple(shapes),
        in_specs=[vmem] * 3,
        out_specs=(vmem,) * len(shapes),
        scratch_shapes=[pltpu.VMEM((rows, D), jnp.bfloat16)],
        compiler_params=params,
        name="out_project",
    )(blocks, mine, other)


def finish_body(groups, *refs):
    resid_refs, (branch_ref, gain_ref), refs = refs[:groups], refs[groups : groups + 2], refs[groups + 2 :]
    keep_ref, give_ref = refs[-2:]
    total = refs[0][...]
    for ref in refs[1:-2]:
        total = total + ref[...]
    width = branch_ref.shape[1]
    own = width // CORES
    chip = lax.div(lax.axis_index("tp"), CORES)
    cols = pl.ds(pl.multiple_of(chip * width, 128), width)
    gain = gain_ref[gain_ref.shape[0] - 1 :, cols]
    for group, ref in enumerate(resid_refs):
        at = slice(group * HALF, (group + 1) * HALF)
        inv_out = lax.rsqrt(turn(total[:, at], 1) / D + norm_eps)
        old = ref[:, cols].astype(jnp.float32)
        branch = branch_ref[at].astype(jnp.float32)
        new = (old + branch * inv_out * gain).astype(jnp.bfloat16)

        def place(core):
            keep_ref[at] = new[:, core * own : (core + 1) * own]
            give_ref[at] = new[:, (1 - core) * own : (2 - core) * own]

        by_core(place)


def finish(resids, branch, gain, totals):
    rows, width = branch.shape
    operands = (*resids, branch, gain, *totals)
    return pl.pallas_call(
        functools.partial(finish_body, len(resids)),
        out_shape=(jax.ShapeDtypeStruct((rows, width // CORES), jnp.bfloat16),) * 2,
        in_specs=[vmem] * len(operands),
        out_specs=(vmem,) * 2,
        compiler_params=params,
        name="finish",
    )(*operands)


def merge_body(keep_ref, got_ref, out_ref):
    for group in range(out_ref.shape[0] // GROUP):
        at = slice(group * HALF, (group + 1) * HALF)
        rows_ref = out_ref.at[pl.ds(group * GROUP, GROUP)]
        rows_ref[half_rows(True), :] = keep_ref[at]
        rows_ref[half_rows(False), :] = got_ref[at]


def merge(keep, got):
    rows, own = keep.shape
    return pl.pallas_call(
        merge_body,
        out_shape=jax.ShapeDtypeStruct((CORES * rows, own), keep.dtype),
        in_specs=[vmem] * 2,
        out_specs=vmem,
        compiler_params=params,
        name="merge",
    )(keep, got)


def partner(x):
    size = lax.axis_size("tp")
    return lax.ppermute(x, "tp", [(i, i ^ 1) for i in range(size)])


def gather_chips(x):
    order = ring_order(lax.axis_size("tp") // CORES)
    lines = [[CORES * z + core for z in order] for core in range(CORES)]
    return lax.all_gather(x, "tp", axis=0, axis_index_groups=lines)


def gather_tokens(x):
    if x.shape[1] % 128:
        return lax.all_gather(x, "tp", axis=1, tiled=True)[None]
    return gather_chips(x)


def swapped(own):
    return (own, partner(own)) if own.shape[2] < D else (own,)


def total_over_chips(square):
    size = lax.axis_size("tp")
    if size > 8:
        lines = [list(range(core, size, CORES)) for core in range(CORES)]
        return (lax.psum(square, "tp", axis_index_groups=lines),)
    return (square,) + tuple(
        lax.ppermute(square, "tp", [(i, (i + hop) % size) for i in range(size)])
        for hop in range(CORES, size, CORES)
    )


def from_behind(block):
    size = lax.axis_size("sp")
    return lax.ppermute(block, "sp", [(i, (i + 1) % size) for i in range(size)])


def local(
    tokens,
    documents,
    pre_gain,
    query_weight,
    key_weight,
    value_weight,
    gate_weight,
    out_weight,
    position_bias,
    post_gain,
):
    rows = tokens.shape[0]
    groups = rows // GROUP
    first = (rows - PAST) // GROUP
    weights = (key_weight, value_weight, query_weight, gate_weight)
    other_out = partner(out_weight)
    gathered, documents = lax.optimization_barrier((gather_tokens(tokens), documents))
    blocks = swapped(gathered)
    stage, pre, post, docs, mask, *bands = setup(
        position_bias, documents, weights, pre_gain, post_gain
    )
    halves, normed, other, pieces, halos = [[None] * groups for _ in range(5)]
    behind = [None] * (PAST // GROUP)
    for layer in range(LAYERS):
        if layer:
            late = tuple(range(groups - 1))
            for batch in ((groups - 1,), late[::-1]):
                made = update(layer, batch, blocks, post, pre, [halves[at] for at in batch])
                for at, half, row in zip(batch, *made):
                    halves[at], normed[at], other[at] = half, row, partner(row)
        for group in reversed(range(first, groups)):
            if layer:
                pieces[group] = project_piece(layer, normed[group], other[group], *weights[:2])
            else:
                halves[group], normed[group], pieces[group] = first_piece(
                    blocks, group * GROUP, docs, pre, stage
                )
            halos[group] = from_behind(pieces[group])
        sources = (*normed, *other) if layer else (*blocks, pre, *normed[first:])
        *half, head, query, gate, local_mixed = project_local(
            layer, rows, sources, pieces[first:], bands[layer], mask, weights if layer else (stage,)
        )
        if half:
            halves[0] = half[0]
        done = [local_mixed]
        known = [*halos[first:], head, *pieces[first:]]
        for group in reversed(range(PAST // GROUP)):
            chunks = known[group : group + WINDOW // GROUP]
            told = behind[group if layer else group + 1 :]
            made = attend(
                layer, group, chunks, query, gate, bands[layer], docs, told, done if group == 0 else []
            )
            if layer == 0:
                *made, behind[group] = made
            if group:
                done = [made[0], *done]
        keep, give = made
        last = layer + 1 == LAYERS
        mixed = gather_chips(join(keep, partner(give)))
        result = out_project(layer, mixed, out_weight, other_out, last)
        if not last:
            blocks = gather_chips(result[0])
    branch, square = result
    keep, give = finish(halves, branch, post, total_over_chips(square))
    return merge(keep, partner(give))


def solution(mesh):
    placed = (
        P("sp", "tp"),
        P("sp"),
        P(),
        P(None, "tp", None),
        P(None, "tp", None),
        P(None, "tp", None),
        P(None, "tp", None),
        P(None, "tp", None),
        P(None, "tp", None),
        P(),
    )
    return jax.shard_map(
        local, mesh=mesh, in_specs=placed, out_specs=P("sp", "tp"), check_vma=False
    )
```

```python
import functools

import jax
import jax.numpy as jnp
from jax import lax
from jax.experimental import pallas as pl
from jax.experimental.pallas import tpu as pltpu
from jax.sharding import PartitionSpec as P

D = 2048
HD = 64
BLOCK = 64
PAST_BLOCKS = 4
LAYERS = 3
PAST = 256
CLIP = 128
GROUP = 2 * BLOCK
WINDOW = PAST + GROUP
SKEW = 512
CORES = 2
DOC_ROWS = 16
HALF = GROUP // CORES
FAR = -1e30

norm_eps = 1e-06
rows_by_rows = (((1,), (1,)), ((), ()))
vmem = pl.BlockSpec(memory_space=pltpu.VMEM)
hbm = pl.BlockSpec(memory_space=pltpu.HBM)
params = pltpu.CompilerParams(vmem_limit_bytes=16 * 1024 * 1024)


def turn(vector, axis):
    size = max(vector.shape)
    diagonal = lax.broadcasted_iota(jnp.int32, (size, size), 0) == lax.broadcasted_iota(
        jnp.int32, (size, size), 1
    )
    spread = jnp.where(diagonal, jnp.broadcast_to(vector, (size, size)), jnp.zeros_like(vector))
    return jnp.sum(spread, axis=axis, keepdims=True)


def setup_body(bias_hbm, docs_hbm, *refs):
    sources, refs = refs[:6], refs[6:]
    stage_ref, pre_ref, post_ref, docs_out, mask_ref, *bands = refs[:-3]
    bias_ref, docs_ref, sems = refs[-3:]
    bias_copy = pltpu.make_async_copy(bias_hbm, bias_ref, sems.at[6])
    bias_copy.start()
    docs_copy = pltpu.make_async_copy(docs_hbm, docs_ref, sems.at[7])
    docs_copy.start()
    targets = [stage_ref.at[at] for at in range(4)] + [pre_ref, post_ref]
    copies = [
        pltpu.make_async_copy(source.at[0] if at < 4 else source, target, sems.at[at])
        for at, (source, target) in enumerate(zip(sources, targets))
    ]
    for copy in copies:
        copy.start()
    docs_copy.wait()
    docs = docs_ref[...].reshape(1, docs_ref.shape[0])
    docs_out[...] = docs
    for index in range(mask_ref.shape[0]):
        start = PAST + index * GROUP
        mask_ref[index] = doc_mask(
            docs[:, start : start + GROUP], docs[:, start - PAST : start + GROUP]
        )
    layers, heads, entries = bias_ref.shape
    row_block = lax.broadcasted_iota(jnp.int32, (GROUP, WINDOW), 0) // BLOCK
    col_block = lax.broadcasted_iota(jnp.int32, (GROUP, WINDOW), 1) // BLOCK
    allowed = (col_block >= row_block) & (col_block <= row_block + PAST_BLOCKS)
    shift = lax.broadcasted_iota(jnp.int32, (entries, SKEW), 1)
    entry = jnp.where(shift < WINDOW, jnp.minimum(PAST - shift, CLIP) + CLIP, 2 * CLIP)
    pick = (lax.broadcasted_iota(jnp.int32, (entries, SKEW), 0) == entry).astype(jnp.float32)
    bias_copy.wait()
    for layer in range(layers):
        base = lax.dot_general(
            bias_ref[layer],
            pick,
            (((1,), (0,)), ((), ())),
            precision=lax.Precision.HIGHEST,
            preferred_element_type=jnp.float32,
        )
        for head in range(heads):
            row = jnp.broadcast_to(base[head : head + 1, :], (GROUP, SKEW))
            skewed = pltpu.roll(row, 0, 1, stride=1, stride_axis=0)
            bands[layer][head] = jnp.where(allowed, skewed[:, :WINDOW], FAR)
    for copy in copies:
        copy.wait()


def doc_mask(own, seen):
    return jnp.where(turn(own, 1) == seen, 0.0, FAR)


def setup(position_bias, docs, weights, pre_gain, post_gain):
    layers, heads, _ = position_bias.shape
    rows = docs.shape[0]
    groups = (rows - PAST) // GROUP
    own = weights[0].shape[1]
    shapes = [
        jax.ShapeDtypeStruct((4, own, D), jnp.bfloat16),
        jax.ShapeDtypeStruct(pre_gain.shape, jnp.float32),
        jax.ShapeDtypeStruct(post_gain.shape, jnp.float32),
        jax.ShapeDtypeStruct((1, rows), jnp.int32),
        jax.ShapeDtypeStruct((groups, GROUP, WINDOW), jnp.float32),
        *[jax.ShapeDtypeStruct((heads, GROUP, WINDOW), jnp.float32) for _ in range(layers)],
    ]
    far = [
        pltpu.with_memory_space_constraint(a, pltpu.HBM)
        for a in (position_bias, docs, *weights, pre_gain, post_gain)
    ]
    return pl.pallas_call(
        setup_body,
        out_shape=tuple(shapes),
        in_specs=[hbm] * 8,
        out_specs=(vmem,) * len(shapes),
        scratch_shapes=[
            pltpu.VMEM(position_bias.shape, jnp.float32),
            pltpu.VMEM(docs.shape, jnp.int32),
            pltpu.SemaphoreType.DMA((8,)),
        ],
        compiler_params=params,
        name="setup",
    )(*far)


def ring_order(count):
    return [0, *range(1, count, 2), *reversed(range(2, count, 2))]


def block_columns(blocks):
    if len(blocks) == 1:
        return [(blocks[0], 0, 0)]
    core = lax.rem(lax.axis_index("tp"), CORES)
    width = blocks[0].shape[2]
    return [
        (ref, slot, pl.multiple_of((CORES * z + (core if side == 0 else 1 - core)) * width, 128))
        for side, ref in enumerate(blocks)
        for slot, z in enumerate(ring_order(ref.shape[0]))
    ]


def lane_sum(square):
    total = square[:, :128]
    for at in range(128, square.shape[1], 128):
        total = total + square[:, at : at + 128]
    return total


def core_at():
    return lax.rem(lax.axis_index("tp"), CORES)


def half_rows(mine):
    at = core_at() if mine else 1 - core_at()
    return pl.ds(pl.multiple_of(at * HALF, HALF), HALF)


def update_half(layer, placed, source, resid_ref, post_ref, pre_ref, resid_out, normed_out):
    if layer:
        total = jnp.zeros((HALF, 128), jnp.float32)
        for ref, slot, _ in placed:
            part = ref[slot, source, :].astype(jnp.float32)
            total = total + lane_sum(part * part)
        inv_out = lax.rsqrt(jnp.sum(total, axis=1, keepdims=True) / D + norm_eps)
    total = jnp.zeros((HALF, 128), jnp.float32)
    for ref, slot, col in placed:
        cols = pl.ds(col, ref.shape[2])
        new = ref[slot, source, :]
        if layer:
            part = new.astype(jnp.float32)
            old = resid_ref[:, cols].astype(jnp.float32)
            new = (old + part * inv_out * post_ref[layer - 1 : layer, cols]).astype(jnp.bfloat16)
        resid_out[:, cols] = new
        wide = new.astype(jnp.float32)
        total = total + lane_sum(wide * wide)
    inv_in = lax.rsqrt(jnp.sum(total, axis=1, keepdims=True) / D + norm_eps)
    for ref, _, col in placed:
        cols = pl.ds(col, ref.shape[2])
        wide = resid_out[:, cols].astype(jnp.float32)
        normed_out[:, cols] = (wide * inv_in * pre_ref[layer : layer + 1, cols]).astype(jnp.bfloat16)


def norm_group(blocks, offset, pre_ref, resid_half, rows_ref, normed_ref):
    placed = block_columns(blocks)
    for half in range(CORES):
        at = pl.ds(half * HALF, HALF)
        update_half(
            0,
            placed,
            pl.ds(offset + half * HALF, HALF),
            None,
            None,
            pre_ref,
            rows_ref.at[at],
            normed_ref.at[at],
        )
    resid_half[...] = rows_ref[half_rows(True), :]


def chip_columns(ref):
    width = ref.shape[2]
    return [(ref, slot, z * width) for slot, z in enumerate(ring_order(ref.shape[0]))]


def update_body(layer, groups, blocks_ref, post_ref, pre_ref, *refs):
    count = len(groups)
    olds, news, normed = [refs[at * count : (at + 1) * count] for at in range(3)]
    placed = chip_columns(blocks_ref)
    for index, group in enumerate(groups):
        update_half(
            layer,
            placed,
            pl.ds(group * HALF, HALF),
            olds[index],
            post_ref,
            pre_ref,
            news[index],
            normed[index],
        )


def update(layer, groups, blocks, post, pre, olds):
    shape = jax.ShapeDtypeStruct((HALF, D), jnp.bfloat16)
    operands = (blocks, post, pre, *olds)
    made = pl.pallas_call(
        functools.partial(update_body, layer, groups),
        out_shape=(shape,) * (2 * len(groups)),
        in_specs=[vmem] * len(operands),
        out_specs=(vmem,) * (2 * len(groups)),
        compiler_params=params,
        name="update",
    )(*operands)
    return made[: len(groups)], made[len(groups) :]


def product(rows_ref, weight):
    return lax.dot_general(
        rows_ref[...], weight, rows_by_rows, preferred_element_type=jnp.float32
    ).astype(jnp.bfloat16)


def weight_of(layer, weights, at):
    return weights[0][at] if layer == 0 else weights[at][layer]


def first_piece_body(offset, count, *refs):
    blocks, (docs_ref, pre_ref, weights_ref) = refs[:count], refs[count : count + 3]
    resid_half, normed_ref, kv_ref, rows_ref = refs[count + 3 :]
    norm_group(blocks, offset, pre_ref, resid_half, rows_ref, normed_ref)
    own = kv_ref.shape[1] // 2
    for at in range(2):
        kv_ref[:GROUP, at * own : (at + 1) * own] = product(normed_ref, weights_ref[at])
    docs = docs_ref[:, offset : offset + GROUP].astype(jnp.float32)
    kv_ref[GROUP:, :GROUP] = jnp.broadcast_to(docs, (DOC_ROWS, GROUP)).astype(jnp.bfloat16)


def first_piece(blocks, offset, docs, pre, stage):
    own = stage.shape[1]
    bf = jnp.bfloat16
    operands = (*blocks, docs, pre, stage)
    return pl.pallas_call(
        functools.partial(first_piece_body, offset, len(blocks)),
        out_shape=(
            jax.ShapeDtypeStruct((HALF, D), bf),
            jax.ShapeDtypeStruct((GROUP, D), bf),
            jax.ShapeDtypeStruct((GROUP + DOC_ROWS, 2 * own), bf),
        ),
        in_specs=[vmem] * len(operands),
        out_specs=(vmem,) * 3,
        scratch_shapes=[pltpu.VMEM((GROUP, D), bf)],
        compiler_params=params,
        name="first_piece",
    )(*operands)


def piece_body(layer, mine_ref, other_ref, key_ref, value_ref, kv_ref, rows_ref):
    rows_ref[half_rows(True), :] = mine_ref[...]
    rows_ref[half_rows(False), :] = other_ref[...]
    own = kv_ref.shape[1] // 2
    kv_ref[:, :own] = product(rows_ref, key_ref[layer])
    kv_ref[:, own:] = product(rows_ref, value_ref[layer])


def project_piece(layer, mine, other, key_weight, value_weight):
    own = key_weight.shape[1]
    return pl.pallas_call(
        functools.partial(piece_body, layer),
        out_shape=jax.ShapeDtypeStruct((GROUP, 2 * own), jnp.bfloat16),
        in_specs=[vmem] * 4,
        out_specs=vmem,
        scratch_shapes=[pltpu.VMEM((GROUP, D), jnp.bfloat16)],
        compiler_params=params,
        name="project_piece",
    )(mine, other, key_weight, value_weight)


def attend_group(query, gate, ext_ref, seen, band_ref, mask, own):
    span = min(own, 128)
    subs = span // HD
    lane = lax.broadcasted_iota(jnp.int32, (GROUP, span), 1) // HD
    zero = jnp.zeros((), query.dtype)
    heads = [
        (start // HD + sub, slice(start, start + span), sub)
        for start in range(0, own, span)
        for sub in range(subs)
    ]
    scores = [
        lax.dot_general(
            jnp.where(lane == sub, query[:, cols], zero),
            ext_ref[seen, cols],
            rows_by_rows,
            preferred_element_type=jnp.float32,
        )
        for _, cols, sub in heads
    ]
    scores = [part + band_ref[head] + mask for (head, _, _), part in zip(heads, scores)]
    tops = [jnp.max(part, axis=1, keepdims=True) for part in scores]
    lifted = [jnp.exp(part - top) for part, top in zip(scores, tops)]
    totals = [jnp.sum(part, axis=1, keepdims=True) for part in lifted]
    parts = [
        jnp.dot(
            part.astype(jnp.bfloat16),
            ext_ref[seen, own + cols.start : own + cols.stop],
            preferred_element_type=jnp.float32,
        )
        for (_, cols, _), part in zip(heads, lifted)
    ]
    parts = [part / total for part, total in zip(parts, totals)]
    results = []
    for at in range(0, len(parts), subs):
        result = parts[at]
        for sub in range(1, subs):
            result = jnp.where(lane == sub, parts[at + sub], result)
        wide = gate[:, heads[at][1]].astype(jnp.float32)
        results.append((result * (wide / (1.0 + jnp.exp(-wide)))).astype(jnp.bfloat16))
    return results


def store_group(mixed_ref, at, results):
    start = 0
    for result in results:
        mixed_ref[at, start : start + result.shape[1]] = result
        start = start + result.shape[1]


def local_body(layer, count, *refs):
    pieces = PAST // GROUP
    if layer == 0:
        blocks, pre_ref, refs = refs[:count], refs[count], refs[count + 1 :]
        piece_normed, refs = refs[:pieces], refs[pieces:]
    else:
        mine, other, refs = refs[:count], refs[count : 2 * count], refs[2 * count :]
    piece_kv, refs = refs[:pieces], refs[pieces:]
    band_ref, mask_ref, refs = refs[0], refs[1], refs[2:]
    if layer == 0:
        weights, refs = refs[:1], refs[1:]
        resid_half, refs = refs[0], refs[1:]
    else:
        weights, refs = refs[:4], refs[4:]
    head_ref, query_out, gate_out, mixed_ref, normed_ref, ext_ref = refs[:6]
    head_rows = head_ref.shape[0]
    head_at = pl.ds(0, head_rows)
    for index in range(pieces):
        at = pl.ds(head_rows + index * GROUP, GROUP)
        ext_ref[at] = piece_kv[index][:GROUP]
        if layer == 0:
            normed_ref[at] = piece_normed[index][...]
    if layer == 0:
        norm_group(blocks, 0, pre_ref, resid_half, refs[6], normed_ref.at[head_at])
    else:
        for group in range(count):
            rows_ref = normed_ref.at[pl.ds(group * GROUP, GROUP)]
            rows_ref[half_rows(True), :] = mine[group][...]
            rows_ref[half_rows(False), :] = other[group][...]
    rest, own = query_out.shape
    local = []
    for at in range(4):
        weight = weight_of(layer, weights, at)
        if at < 2:
            head_ref[:, at * own : (at + 1) * own] = product(normed_ref.at[head_at], weight)
            continue
        result = product(normed_ref, weight)
        if at == 2:
            result = result * jnp.bfloat16(HD ** (-0.5))
        target = query_out if at == 2 else gate_out
        target[...] = result[:rest]
        local.append(result[rest:])
    ext_ref[head_at] = head_ref[...]
    for index in range(mask_ref.shape[0]):
        at = slice(index * GROUP, (index + 1) * GROUP)
        seen = slice(index * GROUP, index * GROUP + WINDOW)
        results = attend_group(
            local[0][at], local[1][at], ext_ref, seen, band_ref, mask_ref[index], own
        )
        store_group(mixed_ref, at, results)


def project_local(layer, rows, sources, pieces, band, mask, weights):
    own = weights[0].shape[1]
    head_rows = rows - PAST
    bf = jnp.bfloat16
    operands = [*sources, *pieces, band, mask, *weights]
    count = len(sources) // 2 if layer else len(sources) - 1 - len(pieces)
    shapes = [] if layer else [(HALF, D)]
    shapes = shapes + [
        (head_rows, 2 * own),
        (PAST, own),
        (PAST, own),
        (rows - PAST, own),
    ]
    scratch = [pltpu.VMEM((rows, D), bf), pltpu.VMEM((rows, 2 * own), bf)]
    if layer == 0:
        scratch.append(pltpu.VMEM((head_rows, D), bf))
    return pl.pallas_call(
        functools.partial(local_body, layer, count),
        out_shape=tuple(jax.ShapeDtypeStruct(shape, bf) for shape in shapes),
        in_specs=[vmem] * len(operands),
        out_specs=(vmem,) * len(shapes),
        scratch_shapes=scratch,
        compiler_params=params,
        name="project_local",
    )(*operands)


def attend_body(layer, group, done, *refs):
    halo_count = PAST // GROUP - group
    chunks, refs = refs[: WINDOW // GROUP], refs[WINDOW // GROUP :]
    query_ref, gate_ref, band_ref, docs_ref, refs = *refs[:4], refs[4:]
    known = halo_count if layer else halo_count - 1
    told_refs, refs = refs[:known], refs[known:]
    done_refs, refs = refs[:done], refs[done:]
    keep_ref = give_ref = None
    if group == 0:
        (keep_ref, give_ref), refs = refs[:2], refs[2:]
    else:
        mixed_ref, refs = refs[0], refs[1:]
    told = [ref[...] for ref in told_refs]
    if layer == 0:
        arrived = chunks[0][GROUP : GROUP + DOC_ROWS, :GROUP].astype(jnp.float32)[:1]
        arrived = jnp.where(lax.axis_index("sp") == 0, -1, arrived.astype(jnp.int32))
        refs[0][...] = arrived
        told = [arrived, *told]
        refs = refs[1:]
    ext_ref = refs[0]
    if group == 0:
        mixed_ref = refs[1]
    for index, chunk in enumerate(chunks):
        ext_ref[index * GROUP : (index + 1) * GROUP] = chunk[:GROUP]
    at = slice(group * GROUP, (group + 1) * GROUP)
    docs = docs_ref[...]
    mask = doc_mask(docs[:, at], jnp.concatenate([*told, docs[:, : at.stop]], axis=1))
    own = query_ref.shape[1]
    results = attend_group(
        query_ref[at], gate_ref[at], ext_ref, slice(None), band_ref, mask, own
    )
    store_group(mixed_ref, slice(None), results)
    if group == 0:
        for index, ref in enumerate((mixed_ref, *done_refs)):
            at = slice(index * HALF, (index + 1) * HALF)
            keep_ref[at] = ref[half_rows(True), :]
            give_ref[at] = ref[half_rows(False), :]


def attend(layer, group, chunks, query, gate, band, docs, told, done):
    own = query.shape[1]
    bf = jnp.bfloat16
    operands = (*chunks, query, gate, band, docs, *told, *done)
    shapes = [jax.ShapeDtypeStruct((GROUP, own), bf)]
    scratch = [pltpu.VMEM((WINDOW, 2 * own), bf)]
    if group == 0:
        shapes = [jax.ShapeDtypeStruct(((1 + len(done)) * HALF, own), bf)] * CORES
        scratch.append(pltpu.VMEM((GROUP, own), bf))
    if layer == 0:
        shapes.append(jax.ShapeDtypeStruct((1, GROUP), jnp.int32))
    return pl.pallas_call(
        functools.partial(attend_body, layer, group, len(done)),
        out_shape=tuple(shapes),
        in_specs=[vmem] * len(operands),
        out_specs=(vmem,) * len(shapes),
        scratch_shapes=scratch,
        compiler_params=params,
        name="attend",
    )(*operands)


def by_core(action):
    for core in range(CORES):
        pl.when(core_at() == core)(functools.partial(action, core))


def join_body(keep_ref, got_ref, out_ref):
    own = keep_ref.shape[1]

    def place(core):
        out_ref[:, core * own : (core + 1) * own] = keep_ref[...]
        out_ref[:, (1 - core) * own : (2 - core) * own] = got_ref[...]

    by_core(place)


def join(keep, got):
    rows, own = keep.shape
    return pl.pallas_call(
        join_body,
        out_shape=jax.ShapeDtypeStruct((rows, CORES * own), keep.dtype),
        in_specs=[vmem] * 2,
        out_specs=vmem,
        compiler_params=params,
        name="join",
    )(keep, got)


def out_body(layer, last, blocks_ref, mine_ref, other_ref, branch_ref, *rest):
    mixed_ref = rest[-1]
    width = blocks_ref.shape[2]
    own = width // CORES
    for ref, slot, col in chip_columns(blocks_ref):
        mixed_ref[:, col : col + width] = ref[slot]
    mine = product(mixed_ref, mine_ref[layer])
    other = product(mixed_ref, other_ref[layer])

    def place(core):
        branch_ref[:, core * own : (core + 1) * own] = mine
        branch_ref[:, (1 - core) * own : (2 - core) * own] = other

    by_core(place)
    if last:
        square_ref = rest[0]
        wide = mine.astype(jnp.float32)
        total = jnp.sum(wide * wide, axis=1, keepdims=True)
        wide = other.astype(jnp.float32)
        total = total + jnp.sum(wide * wide, axis=1, keepdims=True)
        for start in range(0, total.shape[0], HALF):
            at = slice(start, start + HALF)
            square_ref[:, at] = turn(total[at], 0)


def out_project(layer, blocks, mine, other, last):
    rows, width = blocks.shape[1:]
    shapes = [jax.ShapeDtypeStruct((rows, width), jnp.bfloat16)]
    if last:
        shapes.append(jax.ShapeDtypeStruct((1, rows), jnp.float32))
    return pl.pallas_call(
        functools.partial(out_body, layer, last),
        out_shape=tuple(shapes),
        in_specs=[vmem] * 3,
        out_specs=(vmem,) * len(shapes),
        scratch_shapes=[pltpu.VMEM((rows, D), jnp.bfloat16)],
        compiler_params=params,
        name="out_project",
    )(blocks, mine, other)


def finish_body(groups, *refs):
    resid_refs, (branch_ref, gain_ref), refs = refs[:groups], refs[groups : groups + 2], refs[groups + 2 :]
    keep_ref, give_ref = refs[-2:]
    total = refs[0][...]
    for ref in refs[1:-2]:
        total = total + ref[...]
    width = branch_ref.shape[1]
    own = width // CORES
    chip = lax.div(lax.axis_index("tp"), CORES)
    cols = pl.ds(pl.multiple_of(chip * width, 128), width)
    gain = gain_ref[gain_ref.shape[0] - 1 :, cols]
    for group, ref in enumerate(resid_refs):
        at = slice(group * HALF, (group + 1) * HALF)
        inv_out = lax.rsqrt(turn(total[:, at], 1) / D + norm_eps)
        old = ref[:, cols].astype(jnp.float32)
        branch = branch_ref[at].astype(jnp.float32)
        new = (old + branch * inv_out * gain).astype(jnp.bfloat16)

        def place(core):
            keep_ref[at] = new[:, core * own : (core + 1) * own]
            give_ref[at] = new[:, (1 - core) * own : (2 - core) * own]

        by_core(place)


def finish(resids, branch, gain, totals):
    rows, width = branch.shape
    operands = (*resids, branch, gain, *totals)
    return pl.pallas_call(
        functools.partial(finish_body, len(resids)),
        out_shape=(jax.ShapeDtypeStruct((rows, width // CORES), jnp.bfloat16),) * 2,
        in_specs=[vmem] * len(operands),
        out_specs=(vmem,) * 2,
        compiler_params=params,
        name="finish",
    )(*operands)


def merge_body(keep_ref, got_ref, out_ref):
    for group in range(out_ref.shape[0] // GROUP):
        at = slice(group * HALF, (group + 1) * HALF)
        rows_ref = out_ref.at[pl.ds(group * GROUP, GROUP)]
        rows_ref[half_rows(True), :] = keep_ref[at]
        rows_ref[half_rows(False), :] = got_ref[at]


def merge(keep, got):
    rows, own = keep.shape
    return pl.pallas_call(
        merge_body,
        out_shape=jax.ShapeDtypeStruct((CORES * rows, own), keep.dtype),
        in_specs=[vmem] * 2,
        out_specs=vmem,
        compiler_params=params,
        name="merge",
    )(keep, got)


def partner(x):
    size = lax.axis_size("tp")
    return lax.ppermute(x, "tp", [(i, i ^ 1) for i in range(size)])


def gather_chips(x):
    order = ring_order(lax.axis_size("tp") // CORES)
    lines = [[CORES * z + core for z in order] for core in range(CORES)]
    return lax.all_gather(x, "tp", axis=0, axis_index_groups=lines)


def gather_tokens(x):
    if x.shape[1] % 128:
        return lax.all_gather(x, "tp", axis=1, tiled=True)[None]
    return gather_chips(x)


def swapped(own):
    return (own, partner(own)) if own.shape[2] < D else (own,)


def total_over_chips(square):
    size = lax.axis_size("tp")
    if size > 8:
        lines = [list(range(core, size, CORES)) for core in range(CORES)]
        return (lax.psum(square, "tp", axis_index_groups=lines),)
    return (square,) + tuple(
        lax.ppermute(square, "tp", [(i, (i + hop) % size) for i in range(size)])
        for hop in range(CORES, size, CORES)
    )


def from_behind(block):
    size = lax.axis_size("sp")
    return lax.ppermute(block, "sp", [(i, (i + 1) % size) for i in range(size)])


def local(
    tokens,
    documents,
    pre_gain,
    query_weight,
    key_weight,
    value_weight,
    gate_weight,
    out_weight,
    position_bias,
    post_gain,
):
    rows = tokens.shape[0]
    groups = rows // GROUP
    first = (rows - PAST) // GROUP
    weights = (key_weight, value_weight, query_weight, gate_weight)
    other_out = partner(out_weight)
    gathered, documents = lax.optimization_barrier((gather_tokens(tokens), documents))
    blocks = swapped(gathered)
    stage, pre, post, docs, mask, *bands = setup(
        position_bias, documents, weights, pre_gain, post_gain
    )
    halves, normed, other, pieces, halos = [[None] * groups for _ in range(5)]
    behind = [None] * (PAST // GROUP)
    for layer in range(LAYERS):
        if layer:
            late = tuple(range(groups - 1))
            for batch in ((groups - 1,), late[::-1]):
                made = update(layer, batch, blocks, post, pre, [halves[at] for at in batch])
                for at, half, row in zip(batch, *made):
                    halves[at], normed[at], other[at] = half, row, partner(row)
        for group in reversed(range(first, groups)):
            if layer:
                pieces[group] = project_piece(layer, normed[group], other[group], *weights[:2])
            else:
                halves[group], normed[group], pieces[group] = first_piece(
                    blocks, group * GROUP, docs, pre, stage
                )
            halos[group] = from_behind(pieces[group])
        sources = (*normed, *other) if layer else (*blocks, pre, *normed[first:])
        *half, head, query, gate, local_mixed = project_local(
            layer, rows, sources, pieces[first:], bands[layer], mask, weights if layer else (stage,)
        )
        if half:
            halves[0] = half[0]
        done = [local_mixed]
        known = [*halos[first:], head, *pieces[first:]]
        for group in reversed(range(PAST // GROUP)):
            chunks = known[group : group + WINDOW // GROUP]
            told = behind[group if layer else group + 1 :]
            made = attend(
                layer, group, chunks, query, gate, bands[layer], docs, told, done if group == 0 else []
            )
            if layer == 0:
                *made, behind[group] = made
            if group:
                done = [made[0], *done]
        keep, give = made
        last = layer + 1 == LAYERS
        mixed = gather_chips(join(keep, partner(give)))
        result = out_project(layer, mixed, out_weight, other_out, last)
        if not last:
            blocks = gather_chips(result[0])
    branch, square = result
    keep, give = finish(halves, branch, post, total_over_chips(square))
    return merge(keep, partner(give))


def solution(mesh):
    placed = (
        P("sp", "tp"),
        P("sp"),
        P(),
        P(None, "tp", None),
        P(None, "tp", None),
        P(None, "tp", None),
        P(None, "tp", None),
        P(None, "tp", None),
        P(None, "tp", None),
        P(),
    )
    return jax.shard_map(
        local, mesh=mesh, in_specs=placed, out_specs=P("sp", "tp"), check_vma=False
    )
```

```python
import functools

import jax
import jax.numpy as jnp
from jax import lax
from jax.experimental import pallas as pl
from jax.experimental.pallas import tpu as pltpu
from jax.sharding import PartitionSpec as P

D = 2048
HD = 64
BLOCK = 64
PAST_BLOCKS = 4
LAYERS = 3
PAST = 256
CLIP = 128
GROUP = 2 * BLOCK
WINDOW = PAST + GROUP
SKEW = 512
CORES = 2
DOC_ROWS = 16
HALF = GROUP // CORES
FAR = -1e30

norm_eps = 1e-06
rows_by_rows = (((1,), (1,)), ((), ()))
vmem = pl.BlockSpec(memory_space=pltpu.VMEM)
hbm = pl.BlockSpec(memory_space=pltpu.HBM)
params = pltpu.CompilerParams(vmem_limit_bytes=16 * 1024 * 1024)


def turn(vector, axis):
    size = max(vector.shape)
    diagonal = lax.broadcasted_iota(jnp.int32, (size, size), 0) == lax.broadcasted_iota(
        jnp.int32, (size, size), 1
    )
    spread = jnp.where(diagonal, jnp.broadcast_to(vector, (size, size)), jnp.zeros_like(vector))
    return jnp.sum(spread, axis=axis, keepdims=True)


def setup_body(bias_hbm, docs_hbm, *refs):
    sources, refs = refs[:6], refs[6:]
    stage_ref, pre_ref, post_ref, docs_out, mask_ref, *bands = refs[:-3]
    bias_ref, docs_ref, sems = refs[-3:]
    bias_copy = pltpu.make_async_copy(bias_hbm, bias_ref, sems.at[6])
    bias_copy.start()
    docs_copy = pltpu.make_async_copy(docs_hbm, docs_ref, sems.at[7])
    docs_copy.start()
    targets = [stage_ref.at[at] for at in range(4)] + [pre_ref, post_ref]
    copies = [
        pltpu.make_async_copy(source.at[0] if at < 4 else source, target, sems.at[at])
        for at, (source, target) in enumerate(zip(sources, targets))
    ]
    for copy in copies:
        copy.start()
    docs_copy.wait()
    docs = docs_ref[...].reshape(1, docs_ref.shape[0])
    docs_out[...] = docs
    for index in range(mask_ref.shape[0]):
        start = PAST + index * GROUP
        mask_ref[index] = doc_mask(
            docs[:, start : start + GROUP], docs[:, start - PAST : start + GROUP]
        )
    layers, heads, entries = bias_ref.shape
    row_block = lax.broadcasted_iota(jnp.int32, (GROUP, WINDOW), 0) // BLOCK
    col_block = lax.broadcasted_iota(jnp.int32, (GROUP, WINDOW), 1) // BLOCK
    allowed = (col_block >= row_block) & (col_block <= row_block + PAST_BLOCKS)
    shift = lax.broadcasted_iota(jnp.int32, (entries, SKEW), 1)
    entry = jnp.where(shift < WINDOW, jnp.minimum(PAST - shift, CLIP) + CLIP, 2 * CLIP)
    pick = (lax.broadcasted_iota(jnp.int32, (entries, SKEW), 0) == entry).astype(jnp.float32)
    bias_copy.wait()
    for layer in range(layers):
        base = lax.dot_general(
            bias_ref[layer],
            pick,
            (((1,), (0,)), ((), ())),
            precision=lax.Precision.HIGHEST,
            preferred_element_type=jnp.float32,
        )
        for head in range(heads):
            row = jnp.broadcast_to(base[head : head + 1, :], (GROUP, SKEW))
            skewed = pltpu.roll(row, 0, 1, stride=1, stride_axis=0)
            bands[layer][head] = jnp.where(allowed, skewed[:, :WINDOW], FAR)
    for copy in copies:
        copy.wait()


def doc_mask(own, seen):
    return jnp.where(turn(own, 1) == seen, 0.0, FAR)


def setup(position_bias, docs, weights, pre_gain, post_gain):
    layers, heads, _ = position_bias.shape
    rows = docs.shape[0]
    groups = (rows - PAST) // GROUP
    own = weights[0].shape[1]
    shapes = [
        jax.ShapeDtypeStruct((4, own, D), jnp.bfloat16),
        jax.ShapeDtypeStruct(pre_gain.shape, jnp.float32),
        jax.ShapeDtypeStruct(post_gain.shape, jnp.float32),
        jax.ShapeDtypeStruct((1, rows), jnp.int32),
        jax.ShapeDtypeStruct((groups, GROUP, WINDOW), jnp.float32),
        *[jax.ShapeDtypeStruct((heads, GROUP, WINDOW), jnp.float32) for _ in range(layers)],
    ]
    far = [
        pltpu.with_memory_space_constraint(a, pltpu.HBM)
        for a in (position_bias, docs, *weights, pre_gain, post_gain)
    ]
    return pl.pallas_call(
        setup_body,
        out_shape=tuple(shapes),
        in_specs=[hbm] * 8,
        out_specs=(vmem,) * len(shapes),
        scratch_shapes=[
            pltpu.VMEM(position_bias.shape, jnp.float32),
            pltpu.VMEM(docs.shape, jnp.int32),
            pltpu.SemaphoreType.DMA((8,)),
        ],
        compiler_params=params,
        name="setup",
    )(*far)


def ring_order(count):
    return [0, *range(1, count, 2), *reversed(range(2, count, 2))]


def block_columns(blocks):
    if len(blocks) == 1:
        return [(blocks[0], 0, 0)]
    core = lax.rem(lax.axis_index("tp"), CORES)
    width = blocks[0].shape[2]
    return [
        (ref, slot, pl.multiple_of((CORES * z + (core if side == 0 else 1 - core)) * width, 128))
        for side, ref in enumerate(blocks)
        for slot, z in enumerate(ring_order(ref.shape[0]))
    ]


def lane_sum(square):
    total = square[:, :128]
    for at in range(128, square.shape[1], 128):
        total = total + square[:, at : at + 128]
    return total


def core_at():
    return lax.rem(lax.axis_index("tp"), CORES)


def half_rows(mine):
    at = core_at() if mine else 1 - core_at()
    return pl.ds(pl.multiple_of(at * HALF, HALF), HALF)


def update_half(layer, placed, source, resid_ref, post_ref, pre_ref, resid_out, normed_out):
    if layer:
        total = jnp.zeros((HALF, 128), jnp.float32)
        for ref, slot, _ in placed:
            part = ref[slot, source, :].astype(jnp.float32)
            total = total + lane_sum(part * part)
        inv_out = lax.rsqrt(jnp.sum(total, axis=1, keepdims=True) / D + norm_eps)
    total = jnp.zeros((HALF, 128), jnp.float32)
    for ref, slot, col in placed:
        cols = pl.ds(col, ref.shape[2])
        new = ref[slot, source, :]
        if layer:
            part = new.astype(jnp.float32)
            old = resid_ref[:, cols].astype(jnp.float32)
            new = (old + part * inv_out * post_ref[layer - 1 : layer, cols]).astype(jnp.bfloat16)
        resid_out[:, cols] = new
        wide = new.astype(jnp.float32)
        total = total + lane_sum(wide * wide)
    inv_in = lax.rsqrt(jnp.sum(total, axis=1, keepdims=True) / D + norm_eps)
    for ref, _, col in placed:
        cols = pl.ds(col, ref.shape[2])
        wide = resid_out[:, cols].astype(jnp.float32)
        normed_out[:, cols] = (wide * inv_in * pre_ref[layer : layer + 1, cols]).astype(jnp.bfloat16)


def norm_group(blocks, offset, pre_ref, resid_half, rows_ref, normed_ref):
    placed = block_columns(blocks)
    for half in range(CORES):
        at = pl.ds(half * HALF, HALF)
        update_half(
            0,
            placed,
            pl.ds(offset + half * HALF, HALF),
            None,
            None,
            pre_ref,
            rows_ref.at[at],
            normed_ref.at[at],
        )
    resid_half[...] = rows_ref[half_rows(True), :]


def chip_columns(ref):
    width = ref.shape[2]
    return [(ref, slot, z * width) for slot, z in enumerate(ring_order(ref.shape[0]))]


def update_body(layer, groups, blocks_ref, post_ref, pre_ref, *refs):
    count = len(groups)
    olds, news, normed = [refs[at * count : (at + 1) * count] for at in range(3)]
    placed = chip_columns(blocks_ref)
    for index, group in enumerate(groups):
        update_half(
            layer,
            placed,
            pl.ds(group * HALF, HALF),
            olds[index],
            post_ref,
            pre_ref,
            news[index],
            normed[index],
        )


def update(layer, groups, blocks, post, pre, olds):
    shape = jax.ShapeDtypeStruct((HALF, D), jnp.bfloat16)
    operands = (blocks, post, pre, *olds)
    made = pl.pallas_call(
        functools.partial(update_body, layer, groups),
        out_shape=(shape,) * (2 * len(groups)),
        in_specs=[vmem] * len(operands),
        out_specs=(vmem,) * (2 * len(groups)),
        compiler_params=params,
        name="update",
    )(*operands)
    return made[: len(groups)], made[len(groups) :]


def product(rows_ref, weight):
    return lax.dot_general(
        rows_ref[...], weight, rows_by_rows, preferred_element_type=jnp.float32
    ).astype(jnp.bfloat16)


def turned_body(layer, count, *refs):
    out_ref = refs[-1]
    own = refs[0].shape[1]
    for at in range(count):
        out_ref[:, at * own : (at + 1) * own] = jnp.transpose(refs[at][layer])


def turned(layer, weights, after):
    own = weights[0].shape[1]
    return pl.pallas_call(
        functools.partial(turned_body, layer, len(weights)),
        out_shape=jax.ShapeDtypeStruct((D, len(weights) * own), weights[0].dtype),
        in_specs=[vmem] * (len(weights) + 1),
        out_specs=vmem,
        compiler_params=params,
        name="turned",
    )(*weights, after)


def columns_product(rows_ref, weight_ref):
    return jnp.dot(
        rows_ref[...], weight_ref[...], preferred_element_type=jnp.float32
    ).astype(jnp.bfloat16)


def weight_of(layer, weights, at):
    return weights[0][at] if layer == 0 else weights[at][layer]


def first_piece_body(offset, count, *refs):
    blocks, (docs_ref, pre_ref, weights_ref) = refs[:count], refs[count : count + 3]
    resid_half, normed_ref, kv_ref, rows_ref = refs[count + 3 :]
    norm_group(blocks, offset, pre_ref, resid_half, rows_ref, normed_ref)
    own = kv_ref.shape[1] // 2
    for at in range(2):
        kv_ref[:GROUP, at * own : (at + 1) * own] = product(normed_ref, weights_ref[at])
    docs = docs_ref[:, offset : offset + GROUP].astype(jnp.float32)
    kv_ref[GROUP:, :GROUP] = jnp.broadcast_to(docs, (DOC_ROWS, GROUP)).astype(jnp.bfloat16)


def first_piece(blocks, offset, docs, pre, stage):
    own = stage.shape[1]
    bf = jnp.bfloat16
    operands = (*blocks, docs, pre, stage)
    return pl.pallas_call(
        functools.partial(first_piece_body, offset, len(blocks)),
        out_shape=(
            jax.ShapeDtypeStruct((HALF, D), bf),
            jax.ShapeDtypeStruct((GROUP, D), bf),
            jax.ShapeDtypeStruct((GROUP + DOC_ROWS, 2 * own), bf),
        ),
        in_specs=[vmem] * len(operands),
        out_specs=(vmem,) * 3,
        scratch_shapes=[pltpu.VMEM((GROUP, D), bf)],
        compiler_params=params,
        name="first_piece",
    )(*operands)


def piece_body(mine_ref, other_ref, weight_ref, kv_ref, rows_ref):
    rows_ref[half_rows(True), :] = mine_ref[...]
    rows_ref[half_rows(False), :] = other_ref[...]
    kv_ref[...] = columns_product(rows_ref, weight_ref)


def project_piece(mine, other, weight):
    return pl.pallas_call(
        piece_body,
        out_shape=jax.ShapeDtypeStruct((GROUP, weight.shape[1]), jnp.bfloat16),
        in_specs=[vmem] * 3,
        out_specs=vmem,
        scratch_shapes=[pltpu.VMEM((GROUP, D), jnp.bfloat16)],
        compiler_params=params,
        name="project_piece",
    )(mine, other, weight)


def attend_group(query, gate, ext_ref, seen, band_ref, mask, own):
    span = min(own, 128)
    subs = span // HD
    lane = lax.broadcasted_iota(jnp.int32, (GROUP, span), 1) // HD
    zero = jnp.zeros((), query.dtype)
    heads = [
        (start // HD + sub, slice(start, start + span), sub)
        for start in range(0, own, span)
        for sub in range(subs)
    ]
    scores = [
        lax.dot_general(
            jnp.where(lane == sub, query[:, cols], zero),
            ext_ref[seen, cols],
            rows_by_rows,
            preferred_element_type=jnp.float32,
        )
        for _, cols, sub in heads
    ]
    scores = [part + band_ref[head] + mask for (head, _, _), part in zip(heads, scores)]
    tops = [jnp.max(part, axis=1, keepdims=True) for part in scores]
    lifted = [jnp.exp(part - top) for part, top in zip(scores, tops)]
    totals = [jnp.sum(part, axis=1, keepdims=True) for part in lifted]
    parts = [
        jnp.dot(
            part.astype(jnp.bfloat16),
            ext_ref[seen, own + cols.start : own + cols.stop],
            preferred_element_type=jnp.float32,
        )
        for (_, cols, _), part in zip(heads, lifted)
    ]
    parts = [part / total for part, total in zip(parts, totals)]
    results = []
    for at in range(0, len(parts), subs):
        result = parts[at]
        for sub in range(1, subs):
            result = jnp.where(lane == sub, parts[at + sub], result)
        wide = gate[:, heads[at][1]].astype(jnp.float32)
        results.append((result * (wide / (1.0 + jnp.exp(-wide)))).astype(jnp.bfloat16))
    return results


def store_group(mixed_ref, at, results):
    start = 0
    for result in results:
        mixed_ref[at, start : start + result.shape[1]] = result
        start = start + result.shape[1]


def local_body(layer, count, *refs):
    pieces = PAST // GROUP
    if layer == 0:
        blocks, pre_ref, refs = refs[:count], refs[count], refs[count + 1 :]
        piece_normed, refs = refs[:pieces], refs[pieces:]
    else:
        mine, other, refs = refs[:count], refs[count : 2 * count], refs[2 * count :]
    piece_kv, refs = refs[:pieces], refs[pieces:]
    band_ref, mask_ref, refs = refs[0], refs[1], refs[2:]
    if layer == 0:
        weights, refs = refs[:1], refs[1:]
        resid_half, refs = refs[0], refs[1:]
    else:
        weights, refs = refs[:4], refs[4:]
    head_ref, query_out, gate_out, mixed_ref, normed_ref, ext_ref = refs[:6]
    head_rows = head_ref.shape[0]
    head_at = pl.ds(0, head_rows)
    for index in range(pieces):
        at = pl.ds(head_rows + index * GROUP, GROUP)
        ext_ref[at] = piece_kv[index][:GROUP]
        if layer == 0:
            normed_ref[at] = piece_normed[index][...]
    if layer == 0:
        norm_group(blocks, 0, pre_ref, resid_half, refs[6], normed_ref.at[head_at])
    else:
        for group in range(count):
            rows_ref = normed_ref.at[pl.ds(group * GROUP, GROUP)]
            rows_ref[half_rows(True), :] = mine[group][...]
            rows_ref[half_rows(False), :] = other[group][...]
    rest, own = query_out.shape
    local = []
    for at in range(4):
        weight = weight_of(layer, weights, at)
        if at < 2:
            head_ref[:, at * own : (at + 1) * own] = product(normed_ref.at[head_at], weight)
            continue
        result = product(normed_ref, weight)
        if at == 2:
            result = result * jnp.bfloat16(HD ** (-0.5))
        target = query_out if at == 2 else gate_out
        target[...] = result[:rest]
        local.append(result[rest:])
    ext_ref[head_at] = head_ref[...]
    for index in range(mask_ref.shape[0]):
        at = slice(index * GROUP, (index + 1) * GROUP)
        seen = slice(index * GROUP, index * GROUP + WINDOW)
        results = attend_group(
            local[0][at], local[1][at], ext_ref, seen, band_ref, mask_ref[index], own
        )
        store_group(mixed_ref, at, results)


def project_local(layer, rows, sources, pieces, band, mask, weights):
    own = weights[0].shape[1]
    head_rows = rows - PAST
    bf = jnp.bfloat16
    operands = [*sources, *pieces, band, mask, *weights]
    count = len(sources) // 2 if layer else len(sources) - 1 - len(pieces)
    shapes = [] if layer else [(HALF, D)]
    shapes = shapes + [
        (head_rows, 2 * own),
        (PAST, own),
        (PAST, own),
        (rows - PAST, own),
    ]
    scratch = [pltpu.VMEM((rows, D), bf), pltpu.VMEM((rows, 2 * own), bf)]
    if layer == 0:
        scratch.append(pltpu.VMEM((head_rows, D), bf))
    return pl.pallas_call(
        functools.partial(local_body, layer, count),
        out_shape=tuple(jax.ShapeDtypeStruct(shape, bf) for shape in shapes),
        in_specs=[vmem] * len(operands),
        out_specs=(vmem,) * len(shapes),
        scratch_shapes=scratch,
        compiler_params=params,
        name="project_local",
    )(*operands)


def attend_body(layer, group, done, waited, *refs):
    halo_count = PAST // GROUP - group
    chunks, refs = refs[: WINDOW // GROUP], refs[WINDOW // GROUP :]
    query_ref, gate_ref, band_ref, docs_ref, refs = *refs[:4], refs[4:]
    known = halo_count if layer else halo_count - 1
    told_refs, refs = refs[:known], refs[known:]
    done_refs, refs = refs[:done], refs[done + waited :]
    keep_ref = give_ref = None
    if group == 0:
        (keep_ref, give_ref), refs = refs[:2], refs[2:]
    else:
        mixed_ref, refs = refs[0], refs[1:]
    told = [ref[...] for ref in told_refs]
    if layer == 0:
        arrived = chunks[0][GROUP : GROUP + DOC_ROWS, :GROUP].astype(jnp.float32)[:1]
        arrived = jnp.where(lax.axis_index("sp") == 0, -1, arrived.astype(jnp.int32))
        refs[0][...] = arrived
        told = [arrived, *told]
        refs = refs[1:]
    ext_ref = refs[0]
    if group == 0:
        mixed_ref = refs[1]
    for index, chunk in enumerate(chunks):
        ext_ref[index * GROUP : (index + 1) * GROUP] = chunk[:GROUP]
    at = slice(group * GROUP, (group + 1) * GROUP)
    docs = docs_ref[...]
    mask = doc_mask(docs[:, at], jnp.concatenate([*told, docs[:, : at.stop]], axis=1))
    own = query_ref.shape[1]
    results = attend_group(
        query_ref[at], gate_ref[at], ext_ref, slice(None), band_ref, mask, own
    )
    store_group(mixed_ref, slice(None), results)
    if group == 0:
        for index, ref in enumerate((mixed_ref, *done_refs)):
            at = slice(index * HALF, (index + 1) * HALF)
            keep_ref[at] = ref[half_rows(True), :]
            give_ref[at] = ref[half_rows(False), :]


def attend(layer, group, chunks, query, gate, band, docs, told, done, waited):
    own = query.shape[1]
    bf = jnp.bfloat16
    operands = (*chunks, query, gate, band, docs, *told, *done, *waited)
    shapes = [jax.ShapeDtypeStruct((GROUP, own), bf)]
    scratch = [pltpu.VMEM((WINDOW, 2 * own), bf)]
    if group == 0:
        shapes = [jax.ShapeDtypeStruct(((1 + len(done)) * HALF, own), bf)] * CORES
        scratch.append(pltpu.VMEM((GROUP, own), bf))
    if layer == 0:
        shapes.append(jax.ShapeDtypeStruct((1, GROUP), jnp.int32))
    return pl.pallas_call(
        functools.partial(attend_body, layer, group, len(done), len(waited)),
        out_shape=tuple(shapes),
        in_specs=[vmem] * len(operands),
        out_specs=(vmem,) * len(shapes),
        scratch_shapes=scratch,
        compiler_params=params,
        name="attend",
    )(*operands)


def by_core(action):
    for core in range(CORES):
        pl.when(core_at() == core)(functools.partial(action, core))


def join_body(keep_ref, got_ref, out_ref):
    own = keep_ref.shape[1]

    def place(core):
        out_ref[:, core * own : (core + 1) * own] = keep_ref[...]
        out_ref[:, (1 - core) * own : (2 - core) * own] = got_ref[...]

    by_core(place)


def join(keep, got):
    rows, own = keep.shape
    return pl.pallas_call(
        join_body,
        out_shape=jax.ShapeDtypeStruct((rows, CORES * own), keep.dtype),
        in_specs=[vmem] * 2,
        out_specs=vmem,
        compiler_params=params,
        name="join",
    )(keep, got)


def out_body(last, blocks_ref, weight_ref, *refs):
    mixed_ref = refs[-1]
    width = blocks_ref.shape[2]
    own = width // CORES
    for ref, slot, col in chip_columns(blocks_ref):
        mixed_ref[:, col : col + width] = ref[slot]
    branch = columns_product(mixed_ref, weight_ref)
    mine, other = branch[:, :own], branch[:, own:]
    if not last:
        branch_ref = refs[0]

        def place(core):
            branch_ref[:, core * own : (core + 1) * own] = mine
            branch_ref[:, (1 - core) * own : (2 - core) * own] = other

        by_core(place)
        return
    keep_ref, give_ref, square_ref = refs[:3]
    keep_ref[...] = mine
    give_ref[...] = other
    total = 0.0
    for part in (mine, other):
        wide = part.astype(jnp.float32)
        total = total + jnp.sum(wide * wide, axis=1, keepdims=True)
    empty = jnp.zeros((1, HALF), jnp.float32)
    for group in range(total.shape[0] // HALF):
        row = turn(total[group * HALF : (group + 1) * HALF], 0)

        def place(core):
            pair = (row, empty) if core == 0 else (empty, row)
            square_ref[:, group * GROUP : (group + 1) * GROUP] = jnp.concatenate(pair, axis=1)

        by_core(place)


def out_project(blocks, weight, last):
    rows, width = blocks.shape[1:]
    bf = jnp.bfloat16
    shapes = [jax.ShapeDtypeStruct((rows, width), bf)]
    if last:
        shapes = [jax.ShapeDtypeStruct((rows, width // CORES), bf)] * CORES
        shapes.append(jax.ShapeDtypeStruct((1, CORES * rows), jnp.float32))
    return pl.pallas_call(
        functools.partial(out_body, last),
        out_shape=tuple(shapes),
        in_specs=[vmem] * 2,
        out_specs=(vmem,) * len(shapes),
        scratch_shapes=[pltpu.VMEM((rows, D), bf)],
        compiler_params=params,
        name="out_project",
    )(blocks, weight)


def chip_slice(width):
    chip = lax.div(lax.axis_index("tp"), CORES)
    return pl.ds(pl.multiple_of(chip * width, 128), width)


def split_body(groups, *refs):
    keep_ref, give_ref = refs[-2:]
    own = keep_ref.shape[1]
    for group in range(groups):
        at = slice(group * HALF, (group + 1) * HALF)
        rows = refs[group][:, chip_slice(CORES * own)]

        def place(core):
            keep_ref[at] = rows[:, core * own : (core + 1) * own]
            give_ref[at] = rows[:, (1 - core) * own : (2 - core) * own]

        by_core(place)


def split(halves, own, after):
    shape = jax.ShapeDtypeStruct((len(halves) * HALF, own), jnp.bfloat16)
    return pl.pallas_call(
        functools.partial(split_body, len(halves)),
        out_shape=(shape,) * 2,
        in_specs=[vmem] * (len(halves) + 1),
        out_specs=(vmem,) * 2,
        compiler_params=params,
        name="split",
    )(*halves, after)


def finish_body(old_keep, old_got, keep_ref, got_ref, gain_ref, *refs):
    out_ref, old_ref, branch_ref = refs[-3:]
    total = refs[0][...]
    for ref in refs[1:-3]:
        total = total + ref[...]
    own = out_ref.shape[1]
    gain = gain_ref[gain_ref.shape[0] - 1 :, chip_slice(CORES * own)]
    gain = jnp.where(core_at() == 0, gain[:, :own], gain[:, own:])
    for group in range(out_ref.shape[0] // GROUP):
        at = slice(group * GROUP, (group + 1) * GROUP)
        half = slice(group * HALF, (group + 1) * HALF)
        for target, mine, other in ((old_ref, old_keep, old_got), (branch_ref, keep_ref, got_ref)):
            target[half_rows(True), :] = mine[half].astype(jnp.float32)
            target[half_rows(False), :] = other[half].astype(jnp.float32)
        inv_out = lax.rsqrt(turn(total[:, at], 1) / D + norm_eps)
        out_ref[at] = (old_ref[...] + branch_ref[...] * inv_out * gain).astype(jnp.bfloat16)


def finish(old_keep, old_got, keep, got, gain, totals):
    rows, own = keep.shape
    operands = (old_keep, old_got, keep, got, gain, *totals)
    return pl.pallas_call(
        finish_body,
        out_shape=jax.ShapeDtypeStruct((CORES * rows, own), jnp.bfloat16),
        in_specs=[vmem] * len(operands),
        out_specs=vmem,
        scratch_shapes=[pltpu.VMEM((GROUP, own), jnp.float32)] * 2,
        compiler_params=params,
        name="finish",
    )(*operands)


def partner(x):
    size = lax.axis_size("tp")
    return lax.ppermute(x, "tp", [(i, i ^ 1) for i in range(size)])


def gather_chips(x):
    order = ring_order(lax.axis_size("tp") // CORES)
    lines = [[CORES * z + core for z in order] for core in range(CORES)]
    return lax.all_gather(x, "tp", axis=0, axis_index_groups=lines)


def gather_tokens(x):
    if x.shape[1] % 128:
        return lax.all_gather(x, "tp", axis=1, tiled=True)[None]
    return gather_chips(x)


def swapped(own):
    return (own, partner(own)) if own.shape[2] < D else (own,)


def total_over_tp(square):
    size = lax.axis_size("tp")
    if size > 8:
        return (lax.psum(square, "tp"),)
    both = square + partner(square)
    return (both,) + tuple(
        lax.ppermute(both, "tp", [(i, (i + hop) % size) for i in range(size)])
        for hop in range(CORES, size, CORES)
    )


def from_behind(block):
    size = lax.axis_size("sp")
    return lax.ppermute(block, "sp", [(i, (i + 1) % size) for i in range(size)])


def local(
    tokens,
    documents,
    pre_gain,
    query_weight,
    key_weight,
    value_weight,
    gate_weight,
    out_weight,
    position_bias,
    post_gain,
):
    rows = tokens.shape[0]
    groups = rows // GROUP
    first = (rows - PAST) // GROUP
    weights = (key_weight, value_weight, query_weight, gate_weight)
    out_pair = (out_weight, partner(out_weight))
    gathered, documents = lax.optimization_barrier((gather_tokens(tokens), documents))
    blocks = swapped(gathered)
    stage, pre, post, docs, mask, *bands = setup(
        position_bias, documents, weights, pre_gain, post_gain
    )
    halves, normed, other, pieces, halos = [[None] * groups for _ in range(5)]
    behind = [None] * (PAST // GROUP)
    for layer in range(LAYERS):
        if layer:
            late = tuple(range(groups - 1))
            for batch in ((groups - 1,), late[::-1]):
                made = update(layer, batch, blocks, post, pre, [halves[at] for at in batch])
                for at, half, row in zip(batch, *made):
                    halves[at], normed[at], other[at] = half, row, partner(row)
        for group in reversed(range(first, groups)):
            if layer:
                pieces[group] = project_piece(normed[group], other[group], key_value)
            else:
                halves[group], normed[group], pieces[group] = first_piece(
                    blocks, group * GROUP, docs, pre, stage
                )
            halos[group] = from_behind(pieces[group])
        sources = (*normed, *other) if layer else (*blocks, pre, *normed[first:])
        *half, head, query, gate, local_mixed = project_local(
            layer, rows, sources, pieces[first:], bands[layer], mask, weights if layer else (stage,)
        )
        if half:
            halves[0] = half[0]
        last = layer + 1 == LAYERS
        ready = [turned(layer, out_pair, local_mixed)]
        if last:
            old_keep, old_give = split(halves, tokens.shape[1], local_mixed)
            old_got = partner(old_give)
            ready.append(old_keep)
        else:
            ready.append(turned(layer + 1, weights[:2], local_mixed))
            key_value = ready[1]
        done = [local_mixed]
        known = [*halos[first:], head, *pieces[first:]]
        for group in reversed(range(PAST // GROUP)):
            chunks = known[group : group + WINDOW // GROUP]
            told = behind[group if layer else group + 1 :]
            made = attend(
                layer,
                group,
                chunks,
                query,
                gate,
                bands[layer],
                docs,
                told,
                () if group else done,
                () if group else ready,
            )
            if layer == 0:
                *made, behind[group] = made
            if group:
                done = [made[0], *done]
        keep, give = made
        mixed = gather_chips(join(keep, partner(give)))
        result = out_project(mixed, ready[0], last)
        if not last:
            blocks = gather_chips(result[0])
    keep, give, square = result
    totals = total_over_tp(square)
    return finish(old_keep, old_got, keep, partner(give), post, totals)


def solution(mesh):
    placed = (
        P("sp", "tp"),
        P("sp"),
        P(),
        P(None, "tp", None),
        P(None, "tp", None),
        P(None, "tp", None),
        P(None, "tp", None),
        P(None, "tp", None),
        P(None, "tp", None),
        P(),
    )
    return jax.shard_map(
        local, mesh=mesh, in_specs=placed, out_specs=P("sp", "tp"), check_vma=False
    )
```

```python
import functools

import jax
import jax.numpy as jnp
from jax import lax
from jax.experimental import pallas as pl
from jax.experimental.pallas import tpu as pltpu
from jax.sharding import PartitionSpec as P

D = 2048
HD = 64
BLOCK = 64
PAST_BLOCKS = 4
LAYERS = 3
PAST = 256
CLIP = 128
GROUP = 2 * BLOCK
WINDOW = PAST + GROUP
SKEW = 512
CORES = 2
DOC_ROWS = 16
HALF = GROUP // CORES
FAR = -1e30

norm_eps = 1e-06
rows_by_rows = (((1,), (1,)), ((), ()))
vmem = pl.BlockSpec(memory_space=pltpu.VMEM)
hbm = pl.BlockSpec(memory_space=pltpu.HBM)
params = pltpu.CompilerParams(vmem_limit_bytes=16 * 1024 * 1024)


def turn(vector, axis):
    size = max(vector.shape)
    diagonal = lax.broadcasted_iota(jnp.int32, (size, size), 0) == lax.broadcasted_iota(
        jnp.int32, (size, size), 1
    )
    spread = jnp.where(diagonal, jnp.broadcast_to(vector, (size, size)), jnp.zeros_like(vector))
    return jnp.sum(spread, axis=axis, keepdims=True)


def setup_body(bias_hbm, docs_hbm, *refs):
    sources, refs = refs[:6], refs[6:]
    stage_ref, pre_ref, post_ref, docs_out, mask_ref, *bands = refs[:-3]
    bias_ref, docs_ref, sems = refs[-3:]
    bias_copy = pltpu.make_async_copy(bias_hbm, bias_ref, sems.at[6])
    bias_copy.start()
    docs_copy = pltpu.make_async_copy(docs_hbm, docs_ref, sems.at[7])
    docs_copy.start()
    targets = [stage_ref.at[at] for at in range(4)] + [pre_ref, post_ref]
    copies = [
        pltpu.make_async_copy(source.at[0] if at < 4 else source, target, sems.at[at])
        for at, (source, target) in enumerate(zip(sources, targets))
    ]
    for copy in copies:
        copy.start()
    docs_copy.wait()
    docs = docs_ref[...].reshape(1, docs_ref.shape[0])
    docs_out[...] = docs
    for index in range(mask_ref.shape[0]):
        start = PAST + index * GROUP
        mask_ref[index] = doc_mask(
            docs[:, start : start + GROUP], docs[:, start - PAST : start + GROUP]
        )
    layers, heads, entries = bias_ref.shape
    row_block = lax.broadcasted_iota(jnp.int32, (GROUP, WINDOW), 0) // BLOCK
    col_block = lax.broadcasted_iota(jnp.int32, (GROUP, WINDOW), 1) // BLOCK
    allowed = (col_block >= row_block) & (col_block <= row_block + PAST_BLOCKS)
    shift = lax.broadcasted_iota(jnp.int32, (entries, SKEW), 1)
    entry = jnp.where(shift < WINDOW, jnp.minimum(PAST - shift, CLIP) + CLIP, 2 * CLIP)
    pick = (lax.broadcasted_iota(jnp.int32, (entries, SKEW), 0) == entry).astype(jnp.float32)
    bias_copy.wait()
    for layer in range(layers):
        base = lax.dot_general(
            bias_ref[layer],
            pick,
            (((1,), (0,)), ((), ())),
            precision=lax.Precision.HIGHEST,
            preferred_element_type=jnp.float32,
        )
        for head in range(heads):
            row = jnp.broadcast_to(base[head : head + 1, :], (GROUP, SKEW))
            skewed = pltpu.roll(row, 0, 1, stride=1, stride_axis=0)
            bands[layer][head] = jnp.where(allowed, skewed[:, :WINDOW], FAR)
    for copy in copies:
        copy.wait()


def doc_mask(own, seen):
    return jnp.where(turn(own, 1) == seen, 0.0, FAR)


def setup(position_bias, docs, weights, pre_gain, post_gain):
    layers, heads, _ = position_bias.shape
    rows = docs.shape[0]
    groups = (rows - PAST) // GROUP
    own = weights[0].shape[1]
    shapes = [
        jax.ShapeDtypeStruct((4, own, D), jnp.bfloat16),
        jax.ShapeDtypeStruct(pre_gain.shape, jnp.float32),
        jax.ShapeDtypeStruct(post_gain.shape, jnp.float32),
        jax.ShapeDtypeStruct((1, rows), jnp.int32),
        jax.ShapeDtypeStruct((groups, GROUP, WINDOW), jnp.float32),
        *[jax.ShapeDtypeStruct((heads, GROUP, WINDOW), jnp.float32) for _ in range(layers)],
    ]
    far = [
        pltpu.with_memory_space_constraint(a, pltpu.HBM)
        for a in (position_bias, docs, *weights, pre_gain, post_gain)
    ]
    return pl.pallas_call(
        setup_body,
        out_shape=tuple(shapes),
        in_specs=[hbm] * 8,
        out_specs=(vmem,) * len(shapes),
        scratch_shapes=[
            pltpu.VMEM(position_bias.shape, jnp.float32),
            pltpu.VMEM(docs.shape, jnp.int32),
            pltpu.SemaphoreType.DMA((8,)),
        ],
        compiler_params=params,
        name="setup",
    )(*far)


def ring_order(count):
    return [0, *range(1, count, 2), *reversed(range(2, count, 2))]


def block_columns(blocks):
    if len(blocks) == 1:
        return [(blocks[0], 0, 0)]
    core = lax.rem(lax.axis_index("tp"), CORES)
    width = blocks[0].shape[2]
    return [
        (ref, slot, pl.multiple_of((CORES * z + (core if side == 0 else 1 - core)) * width, 128))
        for side, ref in enumerate(blocks)
        for slot, z in enumerate(ring_order(ref.shape[0]))
    ]


def lane_sum(square):
    total = square[:, :128]
    for at in range(128, square.shape[1], 128):
        total = total + square[:, at : at + 128]
    return total


def core_at():
    return lax.rem(lax.axis_index("tp"), CORES)


def half_rows(mine):
    at = core_at() if mine else 1 - core_at()
    return pl.ds(pl.multiple_of(at * HALF, HALF), HALF)


def update_half(layer, placed, source, resid_ref, post_ref, pre_ref, resid_out, normed_out):
    if layer:
        total = jnp.zeros((HALF, 128), jnp.float32)
        for ref, slot, _ in placed:
            part = ref[slot, source, :].astype(jnp.float32)
            total = total + lane_sum(part * part)
        inv_out = lax.rsqrt(jnp.sum(total, axis=1, keepdims=True) / D + norm_eps)
    total = jnp.zeros((HALF, 128), jnp.float32)
    for ref, slot, col in placed:
        cols = pl.ds(col, ref.shape[2])
        new = ref[slot, source, :]
        if layer:
            part = new.astype(jnp.float32)
            old = resid_ref[:, cols].astype(jnp.float32)
            new = (old + part * inv_out * post_ref[layer - 1 : layer, cols]).astype(jnp.bfloat16)
        resid_out[:, cols] = new
        wide = new.astype(jnp.float32)
        total = total + lane_sum(wide * wide)
    inv_in = lax.rsqrt(jnp.sum(total, axis=1, keepdims=True) / D + norm_eps)
    for ref, _, col in placed:
        cols = pl.ds(col, ref.shape[2])
        wide = resid_out[:, cols].astype(jnp.float32)
        normed_out[:, cols] = (wide * inv_in * pre_ref[layer : layer + 1, cols]).astype(jnp.bfloat16)


def norm_group(blocks, offset, pre_ref, resid_half, rows_ref, normed_ref):
    placed = block_columns(blocks)
    for half in range(CORES):
        at = pl.ds(half * HALF, HALF)
        update_half(
            0,
            placed,
            pl.ds(offset + half * HALF, HALF),
            None,
            None,
            pre_ref,
            rows_ref.at[at],
            normed_ref.at[at],
        )
    resid_half[...] = rows_ref[half_rows(True), :]


def chip_columns(ref):
    width = ref.shape[2]
    return [(ref, slot, z * width) for slot, z in enumerate(ring_order(ref.shape[0]))]


def update_body(layer, groups, waited, blocks_ref, post_ref, pre_ref, *refs):
    count = len(groups)
    refs = refs[waited:]
    olds, news, normed = [refs[at * count : (at + 1) * count] for at in range(3)]
    placed = chip_columns(blocks_ref)
    for index, group in enumerate(groups):
        update_half(
            layer,
            placed,
            pl.ds(group * HALF, HALF),
            olds[index],
            post_ref,
            pre_ref,
            news[index],
            normed[index],
        )


def update(layer, groups, blocks, post, pre, olds, waited):
    shape = jax.ShapeDtypeStruct((HALF, D), jnp.bfloat16)
    operands = (blocks, post, pre, *waited, *olds)
    made = pl.pallas_call(
        functools.partial(update_body, layer, groups, len(waited)),
        out_shape=(shape,) * (2 * len(groups)),
        in_specs=[vmem] * len(operands),
        out_specs=(vmem,) * (2 * len(groups)),
        compiler_params=params,
        name="update",
    )(*operands)
    return made[: len(groups)], made[len(groups) :]


def product(rows_ref, weight):
    return lax.dot_general(
        rows_ref[...], weight, rows_by_rows, preferred_element_type=jnp.float32
    ).astype(jnp.bfloat16)


def turned_body(layer, count, *refs):
    out_ref = refs[-1]
    own = refs[0].shape[1]
    for at in range(count):
        out_ref[:, at * own : (at + 1) * own] = jnp.transpose(refs[at][layer])


def turned(layer, weights, after):
    own = weights[0].shape[1]
    return pl.pallas_call(
        functools.partial(turned_body, layer, len(weights)),
        out_shape=jax.ShapeDtypeStruct((D, len(weights) * own), weights[0].dtype),
        in_specs=[vmem] * (len(weights) + 1),
        out_specs=vmem,
        compiler_params=params,
        name="turned",
    )(*weights, after)


def columns_product(rows_ref, weight_ref):
    return jnp.dot(
        rows_ref[...], weight_ref[...], preferred_element_type=jnp.float32
    ).astype(jnp.bfloat16)


def weight_of(layer, weights, at):
    return weights[0][at] if layer == 0 else weights[at][layer]


def first_piece_body(offset, count, *refs):
    blocks, (docs_ref, pre_ref, weights_ref) = refs[:count], refs[count : count + 3]
    resid_half, normed_ref, kv_ref, rows_ref = refs[count + 3 :]
    norm_group(blocks, offset, pre_ref, resid_half, rows_ref, normed_ref)
    own = kv_ref.shape[1] // 2
    for at in range(2):
        kv_ref[:GROUP, at * own : (at + 1) * own] = product(normed_ref, weights_ref[at])
    docs = docs_ref[:, offset : offset + GROUP].astype(jnp.float32)
    kv_ref[GROUP:, :GROUP] = jnp.broadcast_to(docs, (DOC_ROWS, GROUP)).astype(jnp.bfloat16)


def first_piece(blocks, offset, docs, pre, stage):
    own = stage.shape[1]
    bf = jnp.bfloat16
    operands = (*blocks, docs, pre, stage)
    return pl.pallas_call(
        functools.partial(first_piece_body, offset, len(blocks)),
        out_shape=(
            jax.ShapeDtypeStruct((HALF, D), bf),
            jax.ShapeDtypeStruct((GROUP, D), bf),
            jax.ShapeDtypeStruct((GROUP + DOC_ROWS, 2 * own), bf),
        ),
        in_specs=[vmem] * len(operands),
        out_specs=(vmem,) * 3,
        scratch_shapes=[pltpu.VMEM((GROUP, D), bf)],
        compiler_params=params,
        name="first_piece",
    )(*operands)


def piece_body(mine_ref, other_ref, weight_ref, kv_ref, rows_ref):
    rows_ref[half_rows(True), :] = mine_ref[...]
    rows_ref[half_rows(False), :] = other_ref[...]
    kv_ref[...] = columns_product(rows_ref, weight_ref)


def project_piece(mine, other, weight):
    return pl.pallas_call(
        piece_body,
        out_shape=jax.ShapeDtypeStruct((GROUP, weight.shape[1]), jnp.bfloat16),
        in_specs=[vmem] * 3,
        out_specs=vmem,
        scratch_shapes=[pltpu.VMEM((GROUP, D), jnp.bfloat16)],
        compiler_params=params,
        name="project_piece",
    )(mine, other, weight)


def attend_group(query, gate, ext_ref, seen, band_ref, mask, own):
    span = min(own, 128)
    subs = span // HD
    lane = lax.broadcasted_iota(jnp.int32, (GROUP, span), 1) // HD
    zero = jnp.zeros((), query.dtype)
    heads = [
        (start // HD + sub, slice(start, start + span), sub)
        for start in range(0, own, span)
        for sub in range(subs)
    ]
    scores = [
        lax.dot_general(
            jnp.where(lane == sub, query[:, cols], zero),
            ext_ref[seen, cols],
            rows_by_rows,
            preferred_element_type=jnp.float32,
        )
        for _, cols, sub in heads
    ]
    scores = [part + band_ref[head] + mask for (head, _, _), part in zip(heads, scores)]
    tops = [jnp.max(part, axis=1, keepdims=True) for part in scores]
    lifted = [jnp.exp(part - top) for part, top in zip(scores, tops)]
    totals = [jnp.sum(part, axis=1, keepdims=True) for part in lifted]
    parts = [
        jnp.dot(
            part.astype(jnp.bfloat16),
            ext_ref[seen, own + cols.start : own + cols.stop],
            preferred_element_type=jnp.float32,
        )
        for (_, cols, _), part in zip(heads, lifted)
    ]
    parts = [part / total for part, total in zip(parts, totals)]
    results = []
    for at in range(0, len(parts), subs):
        result = parts[at]
        for sub in range(1, subs):
            result = jnp.where(lane == sub, parts[at + sub], result)
        wide = gate[:, heads[at][1]].astype(jnp.float32)
        results.append((result * (wide / (1.0 + jnp.exp(-wide)))).astype(jnp.bfloat16))
    return results


def store_group(mixed_ref, at, results):
    start = 0
    for result in results:
        mixed_ref[at, start : start + result.shape[1]] = result
        start = start + result.shape[1]


def local_body(layer, count, *refs):
    pieces = PAST // GROUP
    if layer == 0:
        blocks, pre_ref, refs = refs[:count], refs[count], refs[count + 1 :]
        piece_normed, refs = refs[:pieces], refs[pieces:]
    else:
        mine, other, refs = refs[:count], refs[count : 2 * count], refs[2 * count :]
    piece_kv, refs = refs[:pieces], refs[pieces:]
    band_ref, mask_ref, refs = refs[0], refs[1], refs[2:]
    if layer == 0:
        weights, refs = refs[:1], refs[1:]
        resid_half, refs = refs[0], refs[1:]
    else:
        weights, refs = refs[:4], refs[4:]
    head_ref, query_out, gate_out, mixed_ref, normed_ref, ext_ref = refs[:6]
    head_rows = head_ref.shape[0]
    head_at = pl.ds(0, head_rows)
    for index in range(pieces):
        at = pl.ds(head_rows + index * GROUP, GROUP)
        ext_ref[at] = piece_kv[index][:GROUP]
        if layer == 0:
            normed_ref[at] = piece_normed[index][...]
    if layer == 0:
        norm_group(blocks, 0, pre_ref, resid_half, refs[6], normed_ref.at[head_at])
    else:
        for group in range(count):
            rows_ref = normed_ref.at[pl.ds(group * GROUP, GROUP)]
            rows_ref[half_rows(True), :] = mine[group][...]
            rows_ref[half_rows(False), :] = other[group][...]
    rest, own = query_out.shape
    local = []
    for at in range(4):
        weight = weight_of(layer, weights, at)
        if at < 2:
            head_ref[:, at * own : (at + 1) * own] = product(normed_ref.at[head_at], weight)
            continue
        result = product(normed_ref, weight)
        if at == 2:
            result = result * jnp.bfloat16(HD ** (-0.5))
        target = query_out if at == 2 else gate_out
        target[...] = result[:rest]
        local.append(result[rest:])
    ext_ref[head_at] = head_ref[...]
    for index in range(mask_ref.shape[0]):
        at = slice(index * GROUP, (index + 1) * GROUP)
        seen = slice(index * GROUP, index * GROUP + WINDOW)
        results = attend_group(
            local[0][at], local[1][at], ext_ref, seen, band_ref, mask_ref[index], own
        )
        store_group(mixed_ref, at, results)


def project_local(layer, rows, sources, pieces, band, mask, weights):
    own = weights[0].shape[1]
    head_rows = rows - PAST
    bf = jnp.bfloat16
    operands = [*sources, *pieces, band, mask, *weights]
    count = len(sources) // 2 if layer else len(sources) - 1 - len(pieces)
    shapes = [] if layer else [(HALF, D)]
    shapes = shapes + [
        (head_rows, 2 * own),
        (PAST, own),
        (PAST, own),
        (rows - PAST, own),
    ]
    scratch = [pltpu.VMEM((rows, D), bf), pltpu.VMEM((rows, 2 * own), bf)]
    if layer == 0:
        scratch.append(pltpu.VMEM((head_rows, D), bf))
    return pl.pallas_call(
        functools.partial(local_body, layer, count),
        out_shape=tuple(jax.ShapeDtypeStruct(shape, bf) for shape in shapes),
        in_specs=[vmem] * len(operands),
        out_specs=(vmem,) * len(shapes),
        scratch_shapes=scratch,
        compiler_params=params,
        name="project_local",
    )(*operands)


def attend_body(layer, group, done, waited, *refs):
    halo_count = PAST // GROUP - group
    chunks, refs = refs[: WINDOW // GROUP], refs[WINDOW // GROUP :]
    query_ref, gate_ref, band_ref, docs_ref, refs = *refs[:4], refs[4:]
    known = halo_count if layer else halo_count - 1
    told_refs, refs = refs[:known], refs[known:]
    done_refs, refs = refs[:done], refs[done + waited :]
    keep_ref = give_ref = None
    if group == 0:
        (keep_ref, give_ref), refs = refs[:2], refs[2:]
    else:
        mixed_ref, refs = refs[0], refs[1:]
    told = [ref[...] for ref in told_refs]
    if layer == 0:
        arrived = chunks[0][GROUP : GROUP + DOC_ROWS, :GROUP].astype(jnp.float32)[:1]
        arrived = jnp.where(lax.axis_index("sp") == 0, -1, arrived.astype(jnp.int32))
        refs[0][...] = arrived
        told = [arrived, *told]
        refs = refs[1:]
    ext_ref = refs[0]
    if group == 0:
        mixed_ref = refs[1]
    for index, chunk in enumerate(chunks):
        ext_ref[index * GROUP : (index + 1) * GROUP] = chunk[:GROUP]
    at = slice(group * GROUP, (group + 1) * GROUP)
    docs = docs_ref[...]
    mask = doc_mask(docs[:, at], jnp.concatenate([*told, docs[:, : at.stop]], axis=1))
    own = query_ref.shape[1]
    results = attend_group(
        query_ref[at], gate_ref[at], ext_ref, slice(None), band_ref, mask, own
    )
    store_group(mixed_ref, slice(None), results)
    if group == 0:
        for index, ref in enumerate((mixed_ref, *done_refs)):
            at = slice(index * HALF, (index + 1) * HALF)
            keep_ref[at] = ref[half_rows(True), :]
            give_ref[at] = ref[half_rows(False), :]


def attend(layer, group, chunks, query, gate, band, docs, told, done, waited):
    own = query.shape[1]
    bf = jnp.bfloat16
    operands = (*chunks, query, gate, band, docs, *told, *done, *waited)
    shapes = [jax.ShapeDtypeStruct((GROUP, own), bf)]
    scratch = [pltpu.VMEM((WINDOW, 2 * own), bf)]
    if group == 0:
        shapes = [jax.ShapeDtypeStruct(((1 + len(done)) * HALF, own), bf)] * CORES
        scratch.append(pltpu.VMEM((GROUP, own), bf))
    if layer == 0:
        shapes.append(jax.ShapeDtypeStruct((1, GROUP), jnp.int32))
    return pl.pallas_call(
        functools.partial(attend_body, layer, group, len(done), len(waited)),
        out_shape=tuple(shapes),
        in_specs=[vmem] * len(operands),
        out_specs=(vmem,) * len(shapes),
        scratch_shapes=scratch,
        compiler_params=params,
        name="attend",
    )(*operands)


def by_core(action):
    for core in range(CORES):
        pl.when(core_at() == core)(functools.partial(action, core))


def join_body(keep_ref, got_ref, out_ref):
    own = keep_ref.shape[1]

    def place(core):
        out_ref[:, core * own : (core + 1) * own] = keep_ref[...]
        out_ref[:, (1 - core) * own : (2 - core) * own] = got_ref[...]

    by_core(place)


def join(keep, got):
    rows, own = keep.shape
    return pl.pallas_call(
        join_body,
        out_shape=jax.ShapeDtypeStruct((rows, CORES * own), keep.dtype),
        in_specs=[vmem] * 2,
        out_specs=vmem,
        compiler_params=params,
        name="join",
    )(keep, got)


def out_body(last, blocks_ref, weight_ref, *refs):
    refs = refs[1:] if last else refs
    mixed_ref = refs[-1]
    width = blocks_ref.shape[2]
    own = width // CORES
    for ref, slot, col in chip_columns(blocks_ref):
        mixed_ref[:, col : col + width] = ref[slot]
    branch = columns_product(mixed_ref, weight_ref)
    mine, other = branch[:, :own], branch[:, own:]
    if not last:
        branch_ref = refs[0]

        def place(core):
            branch_ref[:, core * own : (core + 1) * own] = mine
            branch_ref[:, (1 - core) * own : (2 - core) * own] = other

        by_core(place)
        return
    keep_ref, give_ref, square_ref = refs[:3]
    keep_ref[...] = mine
    give_ref[...] = other
    total = 0.0
    for part in (mine, other):
        wide = part.astype(jnp.float32)
        total = total + jnp.sum(wide * wide, axis=1, keepdims=True)
    empty = jnp.zeros((1, HALF), jnp.float32)
    for group in range(total.shape[0] // HALF):
        row = turn(total[group * HALF : (group + 1) * HALF], 0)

        def place(core):
            pair = (row, empty) if core == 0 else (empty, row)
            square_ref[:, group * GROUP : (group + 1) * GROUP] = jnp.concatenate(pair, axis=1)

        by_core(place)


def out_project(blocks, weight, last, waited):
    rows, width = blocks.shape[1:]
    bf = jnp.bfloat16
    shapes = [jax.ShapeDtypeStruct((rows, width), bf)]
    if last:
        shapes = [jax.ShapeDtypeStruct((rows, width // CORES), bf)] * CORES
        shapes.append(jax.ShapeDtypeStruct((1, CORES * rows), jnp.float32))
    return pl.pallas_call(
        functools.partial(out_body, last),
        out_shape=tuple(shapes),
        in_specs=[vmem] * (2 + len(waited)),
        out_specs=(vmem,) * len(shapes),
        scratch_shapes=[pltpu.VMEM((rows, D), bf)],
        compiler_params=params,
        name="out_project",
    )(blocks, weight, *waited)


def chip_slice(width):
    chip = lax.div(lax.axis_index("tp"), CORES)
    return pl.ds(pl.multiple_of(chip * width, 128), width)


def split_body(groups, *refs):
    keep_ref, give_ref = refs[-2:]
    own = keep_ref.shape[1]
    for group in range(groups):
        at = slice(group * HALF, (group + 1) * HALF)
        rows = refs[group][:, chip_slice(CORES * own)]

        def place(core):
            keep_ref[at] = rows[:, core * own : (core + 1) * own]
            give_ref[at] = rows[:, (1 - core) * own : (2 - core) * own]

        by_core(place)


def split(halves, own, after):
    shape = jax.ShapeDtypeStruct((len(halves) * HALF, own), jnp.bfloat16)
    return pl.pallas_call(
        functools.partial(split_body, len(halves)),
        out_shape=(shape,) * 2,
        in_specs=[vmem] * (len(halves) + 1),
        out_specs=(vmem,) * 2,
        compiler_params=params,
        name="split",
    )(*halves, after)


def finish_body(old_keep, old_got, keep_ref, got_ref, gain_ref, *refs):
    out_ref, old_ref, branch_ref = refs[-3:]
    total = refs[0][...]
    for ref in refs[1:-3]:
        total = total + ref[...]
    own = out_ref.shape[1]
    gain = gain_ref[gain_ref.shape[0] - 1 :, chip_slice(CORES * own)]
    gain = jnp.where(core_at() == 0, gain[:, :own], gain[:, own:])
    for group in range(out_ref.shape[0] // GROUP):
        at = slice(group * GROUP, (group + 1) * GROUP)
        half = slice(group * HALF, (group + 1) * HALF)
        for target, mine, other in ((old_ref, old_keep, old_got), (branch_ref, keep_ref, got_ref)):
            target[half_rows(True), :] = mine[half].astype(jnp.float32)
            target[half_rows(False), :] = other[half].astype(jnp.float32)
        inv_out = lax.rsqrt(turn(total[:, at], 1) / D + norm_eps)
        out_ref[at] = (old_ref[...] + branch_ref[...] * inv_out * gain).astype(jnp.bfloat16)


def finish(old_keep, old_got, keep, got, gain, totals):
    rows, own = keep.shape
    operands = (old_keep, old_got, keep, got, gain, *totals)
    return pl.pallas_call(
        finish_body,
        out_shape=jax.ShapeDtypeStruct((CORES * rows, own), jnp.bfloat16),
        in_specs=[vmem] * len(operands),
        out_specs=vmem,
        scratch_shapes=[pltpu.VMEM((GROUP, own), jnp.float32)] * 2,
        compiler_params=params,
        name="finish",
    )(*operands)


def partner(x):
    size = lax.axis_size("tp")
    return lax.ppermute(x, "tp", [(i, i ^ 1) for i in range(size)])


def gather_chips(x):
    order = ring_order(lax.axis_size("tp") // CORES)
    lines = [[CORES * z + core for z in order] for core in range(CORES)]
    return lax.all_gather(x, "tp", axis=0, axis_index_groups=lines)


def gather_tokens(x):
    if x.shape[1] % 128:
        return lax.all_gather(x, "tp", axis=1, tiled=True)[None]
    return gather_chips(x)


def swapped(own):
    return (own, partner(own)) if own.shape[2] < D else (own,)


def total_over_tp(square, give):
    size = lax.axis_size("tp")
    if size > 8:
        return (lax.psum(square, "tp"),), give
    both, give = lax.optimization_barrier((square + partner(square), give))
    return (both,) + tuple(
        lax.ppermute(both, "tp", [(i, (i + hop) % size) for i in range(size)])
        for hop in range(CORES, size, CORES)
    ), give


def from_behind(block):
    size = lax.axis_size("sp")
    return lax.ppermute(block, "sp", [(i, (i + 1) % size) for i in range(size)])


def local(
    tokens,
    documents,
    pre_gain,
    query_weight,
    key_weight,
    value_weight,
    gate_weight,
    out_weight,
    position_bias,
    post_gain,
):
    rows = tokens.shape[0]
    groups = rows // GROUP
    first = (rows - PAST) // GROUP
    weights = (key_weight, value_weight, query_weight, gate_weight)
    out_pair = (out_weight, partner(out_weight))
    gathered, documents = lax.optimization_barrier((gather_tokens(tokens), documents))
    blocks = swapped(gathered)
    stage, pre, post, docs, mask, *bands = setup(
        position_bias, documents, weights, pre_gain, post_gain
    )
    halves, normed, other, pieces, halos = [[None] * groups for _ in range(5)]
    behind = [None] * (PAST // GROUP)
    for layer in range(LAYERS):
        if layer:
            late = tuple(range(groups - 1))
            for batch in ((groups - 1,), late[::-1]):
                olds = [halves[at] for at in batch]
                waited = normed[groups - 1 :] if batch == late[::-1] else ()
                made = update(layer, batch, blocks, post, pre, olds, waited)
                for at, half, row in zip(batch, *made):
                    halves[at], normed[at], other[at] = half, row, partner(row)
        for group in reversed(range(first, groups)):
            if layer:
                pieces[group] = project_piece(normed[group], other[group], key_value)
            else:
                halves[group], normed[group], pieces[group] = first_piece(
                    blocks, group * GROUP, docs, pre, stage
                )
            halos[group] = from_behind(pieces[group])
        sources = (*normed, *other) if layer else (*blocks, pre, *normed[first:])
        *half, head, query, gate, local_mixed = project_local(
            layer, rows, sources, pieces[first:], bands[layer], mask, weights if layer else (stage,)
        )
        if half:
            halves[0] = half[0]
        last = layer + 1 == LAYERS
        ready = [turned(layer, out_pair, local_mixed)]
        if last:
            old_keep, old_give = split(halves, tokens.shape[1], local_mixed)
            old_got = partner(old_give)
            ready.append(old_keep)
        else:
            ready.append(turned(layer + 1, weights[:2], local_mixed))
            key_value = ready[1]
        done = [local_mixed]
        known = [*halos[first:], head, *pieces[first:]]
        for group in reversed(range(PAST // GROUP)):
            chunks = known[group : group + WINDOW // GROUP]
            told = behind[group if layer else group + 1 :]
            made = attend(
                layer,
                group,
                chunks,
                query,
                gate,
                bands[layer],
                docs,
                told,
                () if group else done,
                () if group else ready,
            )
            if layer == 0:
                *made, behind[group] = made
            if group:
                done = [made[0], *done]
        keep, give = made
        mixed = gather_chips(join(keep, partner(give)))
        result = out_project(mixed, ready[0], last, (old_got,) if last else ())
        if not last:
            blocks = gather_chips(result[0])
    keep, give, square = result
    totals, give = total_over_tp(square, give)
    return finish(old_keep, old_got, keep, partner(give), post, totals)


def solution(mesh):
    placed = (
        P("sp", "tp"),
        P("sp"),
        P(),
        P(None, "tp", None),
        P(None, "tp", None),
        P(None, "tp", None),
        P(None, "tp", None),
        P(None, "tp", None),
        P(None, "tp", None),
        P(),
    )
    return jax.shard_map(
        local, mesh=mesh, in_specs=placed, out_specs=P("sp", "tp"), check_vma=False
    )
```

```python
import functools

import jax
import jax.numpy as jnp
from jax import lax
from jax.experimental import pallas as pl
from jax.experimental.pallas import tpu as pltpu
from jax.sharding import PartitionSpec as P

D = 2048
HD = 64
BLOCK = 64
PAST_BLOCKS = 4
LAYERS = 3
PAST = 256
CLIP = 128
GROUP = 2 * BLOCK
WINDOW = PAST + GROUP
SKEW = 512
CORES = 2
DOC_ROWS = 16
HALF = GROUP // CORES
FAR = -1e30

norm_eps = 1e-06
rows_by_rows = (((1,), (1,)), ((), ()))
vmem = pl.BlockSpec(memory_space=pltpu.VMEM)
hbm = pl.BlockSpec(memory_space=pltpu.HBM)
params = pltpu.CompilerParams(vmem_limit_bytes=16 * 1024 * 1024)


def turn(vector, axis):
    size = max(vector.shape)
    diagonal = lax.broadcasted_iota(jnp.int32, (size, size), 0) == lax.broadcasted_iota(
        jnp.int32, (size, size), 1
    )
    spread = jnp.where(diagonal, jnp.broadcast_to(vector, (size, size)), jnp.zeros_like(vector))
    return jnp.sum(spread, axis=axis, keepdims=True)


def setup_body(bias_hbm, docs_hbm, *refs):
    sources, refs = refs[:6], refs[6:]
    stage_ref, pre_ref, post_ref, docs_out, mask_ref, *bands = refs[:-3]
    bias_ref, docs_ref, sems = refs[-3:]
    bias_copy = pltpu.make_async_copy(bias_hbm, bias_ref, sems.at[6])
    bias_copy.start()
    docs_copy = pltpu.make_async_copy(docs_hbm, docs_ref, sems.at[7])
    docs_copy.start()
    targets = [stage_ref.at[at] for at in range(4)] + [pre_ref, post_ref]
    copies = [
        pltpu.make_async_copy(source.at[0] if at < 4 else source, target, sems.at[at])
        for at, (source, target) in enumerate(zip(sources, targets))
    ]
    for copy in copies:
        copy.start()
    docs_copy.wait()
    docs = docs_ref[...].reshape(1, docs_ref.shape[0])
    docs_out[...] = docs
    for index in range(mask_ref.shape[0]):
        start = PAST + index * GROUP
        mask_ref[index] = doc_mask(
            docs[:, start : start + GROUP], docs[:, start - PAST : start + GROUP]
        )
    layers, heads, entries = bias_ref.shape
    row_block = lax.broadcasted_iota(jnp.int32, (GROUP, WINDOW), 0) // BLOCK
    col_block = lax.broadcasted_iota(jnp.int32, (GROUP, WINDOW), 1) // BLOCK
    allowed = (col_block >= row_block) & (col_block <= row_block + PAST_BLOCKS)
    shift = lax.broadcasted_iota(jnp.int32, (entries, SKEW), 1)
    entry = jnp.where(shift < WINDOW, jnp.minimum(PAST - shift, CLIP) + CLIP, 2 * CLIP)
    pick = (lax.broadcasted_iota(jnp.int32, (entries, SKEW), 0) == entry).astype(jnp.float32)
    bias_copy.wait()
    for layer in range(layers):
        base = lax.dot_general(
            bias_ref[layer],
            pick,
            (((1,), (0,)), ((), ())),
            precision=lax.Precision.HIGHEST,
            preferred_element_type=jnp.float32,
        )
        for head in range(heads):
            row = jnp.broadcast_to(base[head : head + 1, :], (GROUP, SKEW))
            skewed = pltpu.roll(row, 0, 1, stride=1, stride_axis=0)
            bands[layer][head] = jnp.where(allowed, skewed[:, :WINDOW], FAR)
    for copy in copies:
        copy.wait()


def doc_mask(own, seen):
    return jnp.where(turn(own, 1) == seen, 0.0, FAR)


def setup(position_bias, docs, weights, pre_gain, post_gain):
    layers, heads, _ = position_bias.shape
    rows = docs.shape[0]
    groups = (rows - PAST) // GROUP
    own = weights[0].shape[1]
    shapes = [
        jax.ShapeDtypeStruct((4, own, D), jnp.bfloat16),
        jax.ShapeDtypeStruct(pre_gain.shape, jnp.float32),
        jax.ShapeDtypeStruct(post_gain.shape, jnp.float32),
        jax.ShapeDtypeStruct((1, rows), jnp.int32),
        jax.ShapeDtypeStruct((groups, GROUP, WINDOW), jnp.float32),
        *[jax.ShapeDtypeStruct((heads, GROUP, WINDOW), jnp.float32) for _ in range(layers)],
    ]
    far = [
        pltpu.with_memory_space_constraint(a, pltpu.HBM)
        for a in (position_bias, docs, *weights, pre_gain, post_gain)
    ]
    return pl.pallas_call(
        setup_body,
        out_shape=tuple(shapes),
        in_specs=[hbm] * 8,
        out_specs=(vmem,) * len(shapes),
        scratch_shapes=[
            pltpu.VMEM(position_bias.shape, jnp.float32),
            pltpu.VMEM(docs.shape, jnp.int32),
            pltpu.SemaphoreType.DMA((8,)),
        ],
        compiler_params=params,
        name="setup",
    )(*far)


def ring_order(count):
    return [0, *range(1, count, 2), *reversed(range(2, count, 2))]


def block_columns(blocks):
    if len(blocks) == 1:
        return [(blocks[0], 0, 0)]
    core = lax.rem(lax.axis_index("tp"), CORES)
    width = blocks[0].shape[2]
    return [
        (ref, slot, pl.multiple_of((CORES * z + (core if side == 0 else 1 - core)) * width, 128))
        for side, ref in enumerate(blocks)
        for slot, z in enumerate(ring_order(ref.shape[0]))
    ]


def lane_sum(square):
    total = square[:, :128]
    for at in range(128, square.shape[1], 128):
        total = total + square[:, at : at + 128]
    return total


def core_at():
    return lax.rem(lax.axis_index("tp"), CORES)


def half_rows(mine):
    at = core_at() if mine else 1 - core_at()
    return pl.ds(pl.multiple_of(at * HALF, HALF), HALF)


def update_half(layer, placed, source, resid_ref, post_ref, pre_ref, resid_out, normed_out):
    if layer:
        total = jnp.zeros((HALF, 128), jnp.float32)
        for ref, slot, _ in placed:
            part = ref[slot, source, :].astype(jnp.float32)
            total = total + lane_sum(part * part)
        inv_out = lax.rsqrt(jnp.sum(total, axis=1, keepdims=True) / D + norm_eps)
    total = jnp.zeros((HALF, 128), jnp.float32)
    for ref, slot, col in placed:
        cols = pl.ds(col, ref.shape[2])
        new = ref[slot, source, :]
        if layer:
            part = new.astype(jnp.float32)
            old = resid_ref[:, cols].astype(jnp.float32)
            new = (old + part * inv_out * post_ref[layer - 1 : layer, cols]).astype(jnp.bfloat16)
        resid_out[:, cols] = new
        wide = new.astype(jnp.float32)
        total = total + lane_sum(wide * wide)
    inv_in = lax.rsqrt(jnp.sum(total, axis=1, keepdims=True) / D + norm_eps)
    for ref, _, col in placed:
        cols = pl.ds(col, ref.shape[2])
        wide = resid_out[:, cols].astype(jnp.float32)
        normed_out[:, cols] = (wide * inv_in * pre_ref[layer : layer + 1, cols]).astype(jnp.bfloat16)


def norm_group(blocks, offset, pre_ref, resid_half, rows_ref, normed_ref):
    placed = block_columns(blocks)
    for half in range(CORES):
        at = pl.ds(half * HALF, HALF)
        update_half(
            0,
            placed,
            pl.ds(offset + half * HALF, HALF),
            None,
            None,
            pre_ref,
            rows_ref.at[at],
            normed_ref.at[at],
        )
    resid_half[...] = rows_ref[half_rows(True), :]


def chip_columns(ref):
    width = ref.shape[2]
    return [(ref, slot, z * width) for slot, z in enumerate(ring_order(ref.shape[0]))]


def update_body(layer, groups, blocks_ref, post_ref, pre_ref, *refs):
    count = len(groups)
    olds, news, normed = [refs[at * count : (at + 1) * count] for at in range(3)]
    placed = chip_columns(blocks_ref)
    for index, group in enumerate(groups):
        update_half(
            layer,
            placed,
            pl.ds(group * HALF, HALF),
            olds[index],
            post_ref,
            pre_ref,
            news[index],
            normed[index],
        )


def update(layer, groups, blocks, post, pre, olds):
    shape = jax.ShapeDtypeStruct((HALF, D), jnp.bfloat16)
    operands = (blocks, post, pre, *olds)
    made = pl.pallas_call(
        functools.partial(update_body, layer, groups),
        out_shape=(shape,) * (2 * len(groups)),
        in_specs=[vmem] * len(operands),
        out_specs=(vmem,) * (2 * len(groups)),
        compiler_params=params,
        name="update",
    )(*operands)
    return made[: len(groups)], made[len(groups) :]


def product(rows_ref, weight):
    return lax.dot_general(
        rows_ref[...], weight, rows_by_rows, preferred_element_type=jnp.float32
    ).astype(jnp.bfloat16)


def turned_body(layer, count, *refs):
    out_ref = refs[-1]
    own = refs[0].shape[1]
    for at in range(count):
        out_ref[:, at * own : (at + 1) * own] = jnp.transpose(refs[at][layer])


def turned(layer, weights, after):
    own = weights[0].shape[1]
    return pl.pallas_call(
        functools.partial(turned_body, layer, len(weights)),
        out_shape=jax.ShapeDtypeStruct((D, len(weights) * own), weights[0].dtype),
        in_specs=[vmem] * (len(weights) + 1),
        out_specs=vmem,
        compiler_params=params,
        name="turned",
    )(*weights, after)


def columns_product(rows_ref, weight_ref):
    return jnp.dot(
        rows_ref[...], weight_ref[...], preferred_element_type=jnp.float32
    ).astype(jnp.bfloat16)


def weight_of(layer, weights, at):
    return weights[0][at] if layer == 0 else weights[at][layer]


def first_piece_body(offset, count, *refs):
    blocks, (docs_ref, pre_ref, weights_ref) = refs[:count], refs[count : count + 3]
    resid_half, normed_ref, kv_ref, rows_ref = refs[count + 3 :]
    norm_group(blocks, offset, pre_ref, resid_half, rows_ref, normed_ref)
    own = kv_ref.shape[1] // 2
    for at in range(2):
        kv_ref[:GROUP, at * own : (at + 1) * own] = product(normed_ref, weights_ref[at])
    docs = docs_ref[:, offset : offset + GROUP].astype(jnp.float32)
    kv_ref[GROUP:, :GROUP] = jnp.broadcast_to(docs, (DOC_ROWS, GROUP)).astype(jnp.bfloat16)


def first_piece(blocks, offset, docs, pre, stage):
    own = stage.shape[1]
    bf = jnp.bfloat16
    operands = (*blocks, docs, pre, stage)
    return pl.pallas_call(
        functools.partial(first_piece_body, offset, len(blocks)),
        out_shape=(
            jax.ShapeDtypeStruct((HALF, D), bf),
            jax.ShapeDtypeStruct((GROUP, D), bf),
            jax.ShapeDtypeStruct((GROUP + DOC_ROWS, 2 * own), bf),
        ),
        in_specs=[vmem] * len(operands),
        out_specs=(vmem,) * 3,
        scratch_shapes=[pltpu.VMEM((GROUP, D), bf)],
        compiler_params=params,
        name="first_piece",
    )(*operands)


def piece_body(mine_ref, other_ref, weight_ref, kv_ref, rows_ref):
    rows_ref[half_rows(True), :] = mine_ref[...]
    rows_ref[half_rows(False), :] = other_ref[...]
    kv_ref[...] = columns_product(rows_ref, weight_ref)


def project_piece(mine, other, weight):
    return pl.pallas_call(
        piece_body,
        out_shape=jax.ShapeDtypeStruct((GROUP, weight.shape[1]), jnp.bfloat16),
        in_specs=[vmem] * 3,
        out_specs=vmem,
        scratch_shapes=[pltpu.VMEM((GROUP, D), jnp.bfloat16)],
        compiler_params=params,
        name="project_piece",
    )(mine, other, weight)


def attend_group(query, gate, ext_ref, seen, band_ref, mask, own):
    span = min(own, 128)
    subs = span // HD
    lane = lax.broadcasted_iota(jnp.int32, (GROUP, span), 1) // HD
    zero = jnp.zeros((), query.dtype)
    heads = [
        (start // HD + sub, slice(start, start + span), sub)
        for start in range(0, own, span)
        for sub in range(subs)
    ]
    scores = [
        lax.dot_general(
            jnp.where(lane == sub, query[:, cols], zero),
            ext_ref[seen, cols],
            rows_by_rows,
            preferred_element_type=jnp.float32,
        )
        for _, cols, sub in heads
    ]
    scores = [part + band_ref[head] + mask for (head, _, _), part in zip(heads, scores)]
    tops = [jnp.max(part, axis=1, keepdims=True) for part in scores]
    lifted = [jnp.exp(part - top) for part, top in zip(scores, tops)]
    totals = [jnp.sum(part, axis=1, keepdims=True) for part in lifted]
    parts = [
        jnp.dot(
            part.astype(jnp.bfloat16),
            ext_ref[seen, own + cols.start : own + cols.stop],
            preferred_element_type=jnp.float32,
        )
        for (_, cols, _), part in zip(heads, lifted)
    ]
    parts = [part / total for part, total in zip(parts, totals)]
    results = []
    for at in range(0, len(parts), subs):
        result = parts[at]
        for sub in range(1, subs):
            result = jnp.where(lane == sub, parts[at + sub], result)
        wide = gate[:, heads[at][1]].astype(jnp.float32)
        results.append((result * (wide / (1.0 + jnp.exp(-wide)))).astype(jnp.bfloat16))
    return results


def store_group(mixed_ref, at, results):
    start = 0
    for result in results:
        mixed_ref[at, start : start + result.shape[1]] = result
        start = start + result.shape[1]


def local_body(layer, count, *refs):
    pieces = PAST // GROUP
    if layer == 0:
        blocks, pre_ref, refs = refs[:count], refs[count], refs[count + 1 :]
        piece_normed, refs = refs[:pieces], refs[pieces:]
    else:
        mine, other, refs = refs[:count], refs[count : 2 * count], refs[2 * count :]
    piece_kv, refs = refs[:pieces], refs[pieces:]
    band_ref, mask_ref, refs = refs[0], refs[1], refs[2:]
    if layer == 0:
        weights, refs = refs[:1], refs[1:]
        resid_half, refs = refs[0], refs[1:]
    else:
        weights, refs = refs[:4], refs[4:]
    head_ref, query_out, gate_out, mixed_ref, normed_ref, ext_ref = refs[:6]
    head_rows = head_ref.shape[0]
    head_at = pl.ds(0, head_rows)
    for index in range(pieces):
        at = pl.ds(head_rows + index * GROUP, GROUP)
        ext_ref[at] = piece_kv[index][:GROUP]
        if layer == 0:
            normed_ref[at] = piece_normed[index][...]
    if layer == 0:
        norm_group(blocks, 0, pre_ref, resid_half, refs[6], normed_ref.at[head_at])
    else:
        for group in range(count):
            rows_ref = normed_ref.at[pl.ds(group * GROUP, GROUP)]
            rows_ref[half_rows(True), :] = mine[group][...]
            rows_ref[half_rows(False), :] = other[group][...]
    rest, own = query_out.shape
    local = []
    for at in range(4):
        weight = weight_of(layer, weights, at)
        if at < 2:
            head_ref[:, at * own : (at + 1) * own] = product(normed_ref.at[head_at], weight)
            continue
        result = product(normed_ref, weight)
        if at == 2:
            result = result * jnp.bfloat16(HD ** (-0.5))
        target = query_out if at == 2 else gate_out
        target[...] = result[:rest]
        local.append(result[rest:])
    ext_ref[head_at] = head_ref[...]
    for index in range(mask_ref.shape[0]):
        at = slice(index * GROUP, (index + 1) * GROUP)
        seen = slice(index * GROUP, index * GROUP + WINDOW)
        results = attend_group(
            local[0][at], local[1][at], ext_ref, seen, band_ref, mask_ref[index], own
        )
        store_group(mixed_ref, at, results)


def project_local(layer, rows, sources, pieces, band, mask, weights):
    own = weights[0].shape[1]
    head_rows = rows - PAST
    bf = jnp.bfloat16
    operands = [*sources, *pieces, band, mask, *weights]
    count = len(sources) // 2 if layer else len(sources) - 1 - len(pieces)
    shapes = [] if layer else [(HALF, D)]
    shapes = shapes + [
        (head_rows, 2 * own),
        (PAST, own),
        (PAST, own),
        (rows - PAST, own),
    ]
    scratch = [pltpu.VMEM((rows, D), bf), pltpu.VMEM((rows, 2 * own), bf)]
    if layer == 0:
        scratch.append(pltpu.VMEM((head_rows, D), bf))
    return pl.pallas_call(
        functools.partial(local_body, layer, count),
        out_shape=tuple(jax.ShapeDtypeStruct(shape, bf) for shape in shapes),
        in_specs=[vmem] * len(operands),
        out_specs=(vmem,) * len(shapes),
        scratch_shapes=scratch,
        compiler_params=params,
        name="project_local",
    )(*operands)


def attend_body(layer, group, done, waited, *refs):
    halo_count = PAST // GROUP - group
    chunks, refs = refs[: WINDOW // GROUP], refs[WINDOW // GROUP :]
    query_ref, gate_ref, band_ref, docs_ref, refs = *refs[:4], refs[4:]
    known = halo_count if layer else halo_count - 1
    told_refs, refs = refs[:known], refs[known:]
    done_refs, refs = refs[:done], refs[done + waited :]
    keep_ref = give_ref = None
    if group == 0:
        (keep_ref, give_ref), refs = refs[:2], refs[2:]
    else:
        mixed_ref, refs = refs[0], refs[1:]
    told = [ref[...] for ref in told_refs]
    if layer == 0:
        arrived = chunks[0][GROUP : GROUP + DOC_ROWS, :GROUP].astype(jnp.float32)[:1]
        arrived = jnp.where(lax.axis_index("sp") == 0, -1, arrived.astype(jnp.int32))
        refs[0][...] = arrived
        told = [arrived, *told]
        refs = refs[1:]
    ext_ref = refs[0]
    if group == 0:
        mixed_ref = refs[1]
    for index, chunk in enumerate(chunks):
        ext_ref[index * GROUP : (index + 1) * GROUP] = chunk[:GROUP]
    at = slice(group * GROUP, (group + 1) * GROUP)
    docs = docs_ref[...]
    mask = doc_mask(docs[:, at], jnp.concatenate([*told, docs[:, : at.stop]], axis=1))
    own = query_ref.shape[1]
    results = attend_group(
        query_ref[at], gate_ref[at], ext_ref, slice(None), band_ref, mask, own
    )
    store_group(mixed_ref, slice(None), results)
    if group == 0:
        for index, ref in enumerate((mixed_ref, *done_refs)):
            at = slice(index * HALF, (index + 1) * HALF)
            keep_ref[at] = ref[half_rows(True), :]
            give_ref[at] = ref[half_rows(False), :]


def attend(layer, group, chunks, query, gate, band, docs, told, done, waited):
    own = query.shape[1]
    bf = jnp.bfloat16
    operands = (*chunks, query, gate, band, docs, *told, *done, *waited)
    shapes = [jax.ShapeDtypeStruct((GROUP, own), bf)]
    scratch = [pltpu.VMEM((WINDOW, 2 * own), bf)]
    if group == 0:
        shapes = [jax.ShapeDtypeStruct(((1 + len(done)) * HALF, own), bf)] * CORES
        scratch.append(pltpu.VMEM((GROUP, own), bf))
    if layer == 0:
        shapes.append(jax.ShapeDtypeStruct((1, GROUP), jnp.int32))
    return pl.pallas_call(
        functools.partial(attend_body, layer, group, len(done), len(waited)),
        out_shape=tuple(shapes),
        in_specs=[vmem] * len(operands),
        out_specs=(vmem,) * len(shapes),
        scratch_shapes=scratch,
        compiler_params=params,
        name="attend",
    )(*operands)


def by_core(action):
    for core in range(CORES):
        pl.when(core_at() == core)(functools.partial(action, core))


def join_body(keep_ref, got_ref, out_ref):
    own = keep_ref.shape[1]

    def place(core):
        out_ref[:, core * own : (core + 1) * own] = keep_ref[...]
        out_ref[:, (1 - core) * own : (2 - core) * own] = got_ref[...]

    by_core(place)


def join(keep, got):
    rows, own = keep.shape
    return pl.pallas_call(
        join_body,
        out_shape=jax.ShapeDtypeStruct((rows, CORES * own), keep.dtype),
        in_specs=[vmem] * 2,
        out_specs=vmem,
        compiler_params=params,
        name="join",
    )(keep, got)


def out_body(last, blocks_ref, weight_ref, *refs):
    mixed_ref = refs[-1]
    width = blocks_ref.shape[2]
    own = width // CORES
    for ref, slot, col in chip_columns(blocks_ref):
        mixed_ref[:, col : col + width] = ref[slot]
    branch = columns_product(mixed_ref, weight_ref)
    mine, other = branch[:, :own], branch[:, own:]
    if not last:
        branch_ref = refs[0]

        def place(core):
            branch_ref[:, core * own : (core + 1) * own] = mine
            branch_ref[:, (1 - core) * own : (2 - core) * own] = other

        by_core(place)
        return
    keep_ref, give_ref, square_ref = refs[:3]
    keep_ref[...] = mine
    give_ref[...] = other
    total = 0.0
    for part in (mine, other):
        wide = part.astype(jnp.float32)
        total = total + jnp.sum(wide * wide, axis=1, keepdims=True)
    empty = jnp.zeros((1, HALF), jnp.float32)
    for group in range(total.shape[0] // HALF):
        row = turn(total[group * HALF : (group + 1) * HALF], 0)

        def place(core):
            pair = (row, empty) if core == 0 else (empty, row)
            square_ref[:, group * GROUP : (group + 1) * GROUP] = jnp.concatenate(pair, axis=1)

        by_core(place)


def out_project(blocks, weight, last):
    rows, width = blocks.shape[1:]
    bf = jnp.bfloat16
    shapes = [jax.ShapeDtypeStruct((rows, width), bf)]
    if last:
        shapes = [jax.ShapeDtypeStruct((rows, width // CORES), bf)] * CORES
        shapes.append(jax.ShapeDtypeStruct((1, CORES * rows), jnp.float32))
    return pl.pallas_call(
        functools.partial(out_body, last),
        out_shape=tuple(shapes),
        in_specs=[vmem] * 2,
        out_specs=(vmem,) * len(shapes),
        scratch_shapes=[pltpu.VMEM((rows, D), bf)],
        compiler_params=params,
        name="out_project",
    )(blocks, weight)


def chip_slice(width):
    chip = lax.div(lax.axis_index("tp"), CORES)
    return pl.ds(pl.multiple_of(chip * width, 128), width)


def split_body(groups, *refs):
    keep_ref, give_ref = refs[-2:]
    own = keep_ref.shape[1]
    for group in range(groups):
        at = slice(group * HALF, (group + 1) * HALF)
        rows = refs[group][:, chip_slice(CORES * own)]

        def place(core):
            keep_ref[at] = rows[:, core * own : (core + 1) * own]
            give_ref[at] = rows[:, (1 - core) * own : (2 - core) * own]

        by_core(place)


def split(halves, own, after):
    shape = jax.ShapeDtypeStruct((len(halves) * HALF, own), jnp.bfloat16)
    return pl.pallas_call(
        functools.partial(split_body, len(halves)),
        out_shape=(shape,) * 2,
        in_specs=[vmem] * (len(halves) + 1),
        out_specs=(vmem,) * 2,
        compiler_params=params,
        name="split",
    )(*halves, after)


def finish_body(old_keep, old_got, keep_ref, got_ref, gain_ref, *refs):
    out_ref = refs[-1]
    total = refs[0][...]
    for ref in refs[1:-1]:
        total = total + ref[...]
    own = out_ref.shape[1]
    gain = gain_ref[gain_ref.shape[0] - 1 :, chip_slice(CORES * own)]
    gain = jnp.where(core_at() == 0, gain[:, :own], gain[:, own:])
    for group in range(out_ref.shape[0] // GROUP):
        at = slice(group * GROUP, (group + 1) * GROUP)
        half = slice(group * HALF, (group + 1) * HALF)
        old, branch = [
            jnp.where(
                core_at() == 0,
                jnp.concatenate([mine[half], other[half]]),
                jnp.concatenate([other[half], mine[half]]),
            ).astype(jnp.float32)
            for mine, other in ((old_keep, old_got), (keep_ref, got_ref))
        ]
        inv_out = lax.rsqrt(turn(total[:, at], 1) / D + norm_eps)
        out_ref[at] = (old + branch * inv_out * gain).astype(jnp.bfloat16)


def finish(old_keep, old_got, keep, got, gain, totals):
    rows, own = keep.shape
    operands = (old_keep, old_got, keep, got, gain, *totals)
    return pl.pallas_call(
        finish_body,
        out_shape=jax.ShapeDtypeStruct((CORES * rows, own), jnp.bfloat16),
        in_specs=[vmem] * len(operands),
        out_specs=vmem,
        compiler_params=params,
        name="finish",
    )(*operands)


def partner(x):
    size = lax.axis_size("tp")
    return lax.ppermute(x, "tp", [(i, i ^ 1) for i in range(size)])


def gather_chips(x):
    order = ring_order(lax.axis_size("tp") // CORES)
    lines = [[CORES * z + core for z in order] for core in range(CORES)]
    return lax.all_gather(x, "tp", axis=0, axis_index_groups=lines)


def gather_tokens(x):
    if x.shape[1] % 128:
        return lax.all_gather(x, "tp", axis=1, tiled=True)[None]
    return gather_chips(x)


def swapped(own):
    return (own, partner(own)) if own.shape[2] < D else (own,)


def total_over_tp(square):
    size = lax.axis_size("tp")
    if size > 8:
        return (lax.psum(square, "tp"),)
    both = square + partner(square)
    return (both,) + tuple(
        lax.ppermute(both, "tp", [(i, (i + hop) % size) for i in range(size)])
        for hop in range(CORES, size, CORES)
    )


def from_behind(block):
    size = lax.axis_size("sp")
    return lax.ppermute(block, "sp", [(i, (i + 1) % size) for i in range(size)])


def local(
    tokens,
    documents,
    pre_gain,
    query_weight,
    key_weight,
    value_weight,
    gate_weight,
    out_weight,
    position_bias,
    post_gain,
):
    rows = tokens.shape[0]
    groups = rows // GROUP
    first = (rows - PAST) // GROUP
    weights = (key_weight, value_weight, query_weight, gate_weight)
    out_pair = (out_weight, partner(out_weight))
    gathered, documents = lax.optimization_barrier((gather_tokens(tokens), documents))
    blocks = swapped(gathered)
    stage, pre, post, docs, mask, *bands = setup(
        position_bias, documents, weights, pre_gain, post_gain
    )
    halves, normed, other, pieces, halos = [[None] * groups for _ in range(5)]
    behind = [None] * (PAST // GROUP)
    for layer in range(LAYERS):
        if layer:
            late = tuple(range(groups - 1))
            for batch in ((groups - 1,), late[::-1]):
                made = update(layer, batch, blocks, post, pre, [halves[at] for at in batch])
                for at, half, row in zip(batch, *made):
                    halves[at], normed[at], other[at] = half, row, partner(row)
        for group in reversed(range(first, groups)):
            if layer:
                pieces[group] = project_piece(normed[group], other[group], key_value)
            else:
                halves[group], normed[group], pieces[group] = first_piece(
                    blocks, group * GROUP, docs, pre, stage
                )
            halos[group] = from_behind(pieces[group])
        sources = (*normed, *other) if layer else (*blocks, pre, *normed[first:])
        *half, head, query, gate, local_mixed = project_local(
            layer, rows, sources, pieces[first:], bands[layer], mask, weights if layer else (stage,)
        )
        if half:
            halves[0] = half[0]
        last = layer + 1 == LAYERS
        ready = [turned(layer, out_pair, local_mixed)]
        if last:
            old_keep, old_give = split(halves, tokens.shape[1], local_mixed)
            old_got = partner(old_give)
            ready.append(old_keep)
        else:
            ready.append(turned(layer + 1, weights[:2], local_mixed))
            key_value = ready[1]
        done = [local_mixed]
        known = [*halos[first:], head, *pieces[first:]]
        for group in reversed(range(PAST // GROUP)):
            chunks = known[group : group + WINDOW // GROUP]
            told = behind[group if layer else group + 1 :]
            made = attend(
                layer,
                group,
                chunks,
                query,
                gate,
                bands[layer],
                docs,
                told,
                () if group else done,
                () if group else ready,
            )
            if layer == 0:
                *made, behind[group] = made
            if group:
                done = [made[0], *done]
        keep, give = made
        mixed = gather_chips(join(keep, partner(give)))
        result = out_project(mixed, ready[0], last)
        if not last:
            blocks = gather_chips(result[0])
    keep, give, square = result
    totals = total_over_tp(square)
    return finish(old_keep, old_got, keep, partner(give), post, totals)


def solution(mesh):
    placed = (
        P("sp", "tp"),
        P("sp"),
        P(),
        P(None, "tp", None),
        P(None, "tp", None),
        P(None, "tp", None),
        P(None, "tp", None),
        P(None, "tp", None),
        P(None, "tp", None),
        P(),
    )
    return jax.shard_map(
        local, mesh=mesh, in_specs=placed, out_specs=P("sp", "tp"), check_vma=False
    )
```
